256 devices in a mesh: sp: 16 (over y, x), tp: 16 (over z, core).
Axes of the slice: x: 4, y: 4, z: 8, core: 2. Of those that a mesh axis runs over, the one named last changes fastest.
Arguments:
- queries: bfloat16 [6144, 2048], P('sp', 'tp'), may hold values from -6 to 6
- keys: bfloat16 [6144, 2048], P('sp', 'tp'), may hold values from -6 to 6
- values: bfloat16 [6144, 2048], P('sp', 'tp'), may hold values from -6 to 6
- key_bias: bfloat16 [6144, 32], P('sp', 'tp'), may hold values from -16 to 0
- head_gain: float32 [32, 64], P('tp'), may hold values from 0.1 to 1.9
- out_weight: bfloat16 [2048, 2048], P('tp'), may hold values from -0.125 to 0.125
- residual: bfloat16 [6144, 2048], P(('sp', 'tp')), may hold values from -6 to 6
- norm_gain: float32 [2048], replicated, may hold values from 0.1 to 1.9
- gate_proj: bfloat16 [16, 2048, 7168], P('sp', None, 'tp'), may hold values from -0.125 to 0.125
- up_proj: bfloat16 [16, 2048, 7168], P('sp', None, 'tp'), may hold values from -0.125 to 0.125
- down_proj: bfloat16 [16, 7168, 2048], P('sp', 'tp'), may hold values from -0.0625 to 0.0625
- expert_choice: int32 [6144, 2], P(('sp', 'tp')), may hold values from 0 to 15, all different within a row; in each aligned block of 24 rows (0 to 23, 24 to 47, ...) at most 6 rows name the same one
- expert_weights: float32 [6144, 2], P(('sp', 'tp')), may hold values from 0.2 to 1
Outputs:
- layer_out: bfloat16 [6144, 2048], P(('sp', 'tp'))
The draws below stay inside these ranges and needn't reach their ends.
Inputs may be any that keep to these rules, and one draw needn't show every extreme that they name: `expert_choice`: in each aligned block of 24 rows (the rows of one device), no expert is named more than 6 times; the two experts of a row differ.
All inputs are finite; a program needn't handle non-finite values.
Results may differ from the reference program's by a relative error of at most 0.019.
Values may be sent and summed in bfloat16 or wider, within the bound.
A program may use at most 128 MiB of HBM per device.

```python
import math
import jax
import jax.numpy as jnp
import numpy as np
from jax import lax

D = 2048
HEADS = 32
HEAD_DIM = 64
FFE = 7168
TOK_DEV = 384
TOKENS = 6144
EXPERTS = 16
ROWS_DEV = 24
CAP = 6
N_TP = 16


def draw_key_bias(key, part):
    streams = jax.random.split(jax.random.fold_in(key, 11), 7)
    chance = 0.5
    slow_heads = jax.random.uniform(streams[0], (HEADS,)) < chance
    fast_base = jax.random.uniform(streams[1], (HEADS,), minval=-5.0, maxval=-3.8)
    slow_base = -jnp.log(jnp.float32(TOKENS)) - 0.5 + jax.random.uniform(streams[2], (HEADS,), minval=-0.5, maxval=0.5)
    blocks = TOKENS // TOK_DEV
    device_factor = jax.random.uniform(streams[3], (blocks, 1, HEADS), minval=-0.7, maxval=0.7)
    device_factor = jnp.broadcast_to(device_factor, (blocks, TOK_DEV, HEADS)).reshape(TOKENS, HEADS)
    jitter = 0.3 * jax.random.normal(streams[4], (TOKENS, HEADS))
    base = jnp.where(slow_heads[None, :], slow_base[None, :], fast_base[None, :]) + device_factor + jitter
    spots = jax.random.randint(streams[5], (2,), 0, TOKENS)
    levels = jax.random.uniform(streams[6], (2, HEADS), minval=-1.4, maxval=0.0)
    position = jnp.arange(TOKENS)
    first_hit = (position == spots[0])[:, None] & slow_heads[None, :]
    second_hit = (position == spots[1])[:, None] & slow_heads[None, :]
    base = jnp.where(first_hit, levels[0][None, :], base)
    base = jnp.where(second_hit, levels[1][None, :], base)
    return jnp.clip(base, -16.0, 0.0).astype(jnp.bfloat16)


def block_levels(stream_key, extent, pieces, smallest, top_value):
    factor_of, own = 1.0, jax.random.fold_in(stream_key, 6)
    for dim, blocks in pieces:
        heights = jnp.exp(jax.random.uniform(jax.random.fold_in(own, dim), (blocks,), jnp.float32, smallest / len(pieces), top_value / len(pieces)))
        factor_of = factor_of * jnp.repeat(heights, extent[dim] // blocks).reshape([-1 if axis == dim else 1 for axis in range(len(extent))])
    return factor_of


def assign_block(key, own, number, rows, count, top, bound, skew):
    sequence = jax.random.permutation(key, count)
    heavy_load, ordinary = shares(count, rows * top, bound, skew, True), shares(count, rows * top, bound, skew, False)
    places = jnp.arange(count)

    def named(tallies, rotation):
        used = int((tallies > 0).sum())
        fixed = max(1, used // 4)
        shifted = fixed + (places - fixed + rotation * (used - fixed)) % max(1, count - fixed)
        return jnp.zeros((count,), jnp.int32).at[sequence[jnp.where(places < fixed, places, shifted)]].set(jnp.asarray(tallies, jnp.int32))

    tallies = jnp.where(number % 4 == 0, named(heavy_load, number // 4), named(ordinary, number - number // 4 - 1))
    mixed = jax.random.permutation(jax.random.fold_in(own, 3), count)
    giver, taker = mixed[0:count // 2 * 2:2], mixed[1:count // 2 * 2:2]
    margin = jnp.minimum(tallies[giver] - 1, bound - tallies[taker]) // 2
    margin = jnp.where((giver == sequence[0]) | (taker == sequence[0]) | (tallies[taker] == 0), 0, jnp.maximum(margin, 0))
    shifted = jax.random.randint(jax.random.fold_in(own, 4), (count // 2,), 0, 1 << 20) % (margin + 1)
    tallies = tallies.at[giver].add(-shifted).at[taker].add(shifted)
    items = jnp.searchsorted(jnp.cumsum(tallies), jnp.arange(rows * top), side="right").astype(jnp.int32)
    table = items.reshape(top, rows).T
    table = table[jax.random.permutation(jax.random.fold_in(own, 1), rows)]
    rotation = jax.random.randint(jax.random.fold_in(own, 2), (rows, 1), 0, top)
    return jnp.take_along_axis(table, (jnp.arange(top)[None, :] + rotation) % top, axis=1)


def shares(count, total, limit, slope, full):
    weights = [(1 << 20) // math.isqrt(standing ** slope) + 1 for standing in range(1, count + 1)]
    largest = limit if full else min(limit, max(-(-total // count), total * weights[0] // sum(weights)))
    least = 1 if total - largest >= count - 1 else 0
    counts, spare = [largest] + [least] * (count - 1), total - largest - least * (count - 1)
    while spare > 0:
        movable = [i for i in range(1, count) if counts[i] < largest] or [i for i in range(1, count) if counts[i] < limit]
        whole, remaining = sum([weights[i] for i in movable]), spare
        for i in movable:
            addition = min(limit - counts[i], max(1, remaining * weights[i] // whole), spare)
            counts[i] = counts[i] + addition
            spare = spare - addition
    return np.array(counts)


def scatter_about(key, shape, spread, reach, shards=(), held_as=jnp.bfloat16):
    gain = block_levels(key, shape, shards, -0.22, 0.18) if shards else 1.0
    values = jax.random.normal(key, shape, jnp.float32) * spread * gain
    return jnp.minimum(jnp.maximum(values, -reach), reach).astype(held_as)


def setup_inputs(seed: int = 0) -> dict:
    key_of = jax.random.split(jax.random.key(seed), 14)
    queries = scatter_about(key_of[0], (TOKENS, HEADS * HEAD_DIM), 1.0, 6.0, ((0, 16), (1, 16)))
    keys = scatter_about(key_of[1], (TOKENS, HEADS * HEAD_DIM), 1.0, 6.0, ((0, 16), (1, 16)))
    values = scatter_about(key_of[2], (TOKENS, HEADS * HEAD_DIM), 1.0, 6.0, ((0, 16), (1, 16)))
    key_bias = draw_key_bias(jax.random.fold_in(key_of[13], 71), 0)
    head_gain = jnp.clip(1.0 + 0.18 * jax.random.normal(key_of[4], (HEADS, HEAD_DIM), jnp.float32), 0.1, 1.9)
    out_weight = scatter_about(key_of[5], (HEADS * HEAD_DIM, D), (HEADS * HEAD_DIM) ** -0.5, 0.125, ((0, 16),))
    residual = scatter_about(key_of[6], (TOKENS, D), 1.0, 6.0, ((0, 256),))
    norm_gain = jnp.clip(1.0 + 0.18 * jax.random.normal(key_of[7], (D,), jnp.float32), 0.1, 1.9)
    gate_proj = scatter_about(key_of[8], (EXPERTS, D, FFE), D ** -0.5, 0.125, ((0, 16), (2, 16)))
    up_proj = scatter_about(key_of[9], (EXPERTS, D, FFE), D ** -0.5, 0.125, ((0, 16), (2, 16)))
    down_proj = scatter_about(key_of[10], (EXPERTS, FFE, D), FFE ** -0.5, 0.0625, ((0, 16), (1, 16)))
    expert_choice_keys = jax.random.split(jax.random.fold_in(key_of[11], 1), TOKENS // ROWS_DEV)
    expert_choice_turns = jax.random.permutation(jax.random.fold_in(key_of[11], 3), TOKENS // ROWS_DEV)
    expert_choice = jax.vmap(lambda own, number: assign_block(jax.random.fold_in(key_of[11], 2), own, number, ROWS_DEV, EXPERTS, 2, CAP, 1))(expert_choice_keys, expert_choice_turns).reshape((TOKENS, 2))
    expert_weights = jnp.clip(0.2 + 0.8 * jax.random.uniform(key_of[12], (TOKENS, 2), jnp.float32) ** block_levels(key_of[12], (TOKENS, 2), ((0, 256),), -0.2, 0.2), 0.2, 1.0)
    return {"queries": queries, "keys": keys, "values": values, "key_bias": key_bias, "head_gain": head_gain, "out_weight": out_weight, "residual": residual, "norm_gain": norm_gain, "gate_proj": gate_proj, "up_proj": up_proj, "down_proj": down_proj, "expert_choice": expert_choice, "expert_weights": expert_weights}


epsilon = 1e-06

def rms_scaled(values_in):
    return values_in * lax.rsqrt(lax.optimization_barrier(jnp.mean(values_in * values_in, axis=-1, keepdims=True)) + epsilon)

def head_mixture(operands):
    query_head, key_head, value_head, bias_head = operands
    length = query_head.shape[0]
    blocks = length // TOK_DEV
    scores = jnp.dot(query_head, key_head.T, preferred_element_type=jnp.float32) * HEAD_DIM ** (-0.5)
    scores = scores + bias_head.astype(jnp.float32)[None, :]
    position = jnp.arange(length, dtype=jnp.int32)
    earlier = (position[None, :] < position[:, None]).reshape(length, blocks, TOK_DEV)
    scores = scores.reshape(length, blocks, TOK_DEV)
    log_drops = jnp.where(earlier, jax.nn.log_sigmoid(-scores), 0.0)
    suffix = lax.cumsum(log_drops, axis=2, reverse=True) - log_drops
    within = jnp.where(earlier, jnp.exp(jax.nn.log_sigmoid(scores) + suffix), 0.0).astype(jnp.bfloat16)
    value_blocks = value_head.reshape(blocks, TOK_DEV, HEAD_DIM).astype(jnp.float32)
    block_sums = jnp.einsum('tms,msd->tmd', within.astype(jnp.float32), value_blocks)
    totals = lax.optimization_barrier(jnp.sum(log_drops, axis=2))
    carried = lax.optimization_barrier(jnp.sum(totals, axis=1, keepdims=True)) - jnp.cumsum(totals, axis=1)
    return lax.optimization_barrier(jnp.sum(jnp.exp(carried)[:, :, None] * block_sums, axis=1))

def reference(queries, keys, values, key_bias, head_gain, out_weight, residual, norm_gain, gate_proj, up_proj, down_proj, expert_choice, expert_weights):

    def split_heads(array):
        return array.reshape(TOKENS, HEADS, HEAD_DIM).transpose(1, 0, 2)
    mixture = lax.map(head_mixture, (split_heads(queries), split_heads(keys), split_heads(values), key_bias.T))
    attended = (rms_scaled(mixture) * head_gain[:, None, :]).astype(jnp.bfloat16)
    attended = attended.transpose(1, 0, 2).reshape(TOKENS, HEADS * HEAD_DIM)
    projected = jnp.dot(attended, out_weight, preferred_element_type=jnp.float32)
    stream = (residual.astype(jnp.float32) + projected).astype(jnp.bfloat16)
    normed = (rms_scaled(stream.astype(jnp.float32)) * norm_gain).astype(jnp.bfloat16)
    device_blocks = TOKENS // ROWS_DEV
    flat_expert = expert_choice.reshape(-1).astype(jnp.int32)
    flat_token = jnp.arange(2 * TOKENS, dtype=jnp.int32) // 2
    onehot = (flat_expert[:, None] == jnp.arange(EXPERTS, dtype=jnp.int32)[None, :]).astype(jnp.int32)
    grouped = onehot.reshape(device_blocks, 2 * ROWS_DEV, EXPERTS)
    before = (jnp.cumsum(grouped, axis=1) - grouped).reshape(2 * TOKENS, EXPERTS)
    slot_rank = lax.optimization_barrier(jnp.sum(before * onehot, axis=1)).astype(jnp.int32)
    slot_index = (flat_token // ROWS_DEV * CAP + slot_rank).astype(jnp.int32)
    slot_table = jnp.full((EXPERTS, device_blocks * CAP), TOKENS, jnp.int32).at[flat_expert, slot_index].set(flat_token)
    padded = jnp.concatenate([normed, jnp.zeros((1, D), jnp.bfloat16)], axis=0)
    group_size = FFE // N_TP

    def one_expert(operands):
        rows_index, gate_matrix, up_matrix, down_matrix = operands
        row_block = padded[rows_index]
        gate_part = jnp.dot(row_block, gate_matrix, preferred_element_type=jnp.float32)
        up_part = jnp.dot(row_block, up_matrix, preferred_element_type=jnp.float32)
        hidden = (jax.nn.silu(gate_part) * up_part).astype(jnp.bfloat16)
        hidden_groups = hidden.reshape(row_block.shape[0], N_TP, group_size).transpose(1, 0, 2)
        down_groups = down_matrix.reshape(N_TP, group_size, D)

        def add_group(running, group_pair):
            rounded = jnp.dot(group_pair[0], group_pair[1], preferred_element_type=jnp.float32).astype(jnp.bfloat16)
            rounded = lax.optimization_barrier(rounded)
            return (running + rounded.astype(jnp.float32), None)
        running, unused = lax.scan(add_group, jnp.zeros((row_block.shape[0], D), jnp.float32), (hidden_groups, down_groups))
        return running.astype(jnp.bfloat16)
    expert_out = lax.map(one_expert, (slot_table, gate_proj, up_proj, down_proj))
    picked = expert_out[flat_expert, slot_index].astype(jnp.float32).reshape(TOKENS, 2, D)
    combined = lax.optimization_barrier(jnp.sum(expert_weights[:, :, None] * picked, axis=1))
    return (stream.astype(jnp.float32) + combined).astype(jnp.bfloat16)
```

```python
import functools

import jax
import jax.numpy as jnp
from jax import lax
from jax.experimental import pallas as pl
from jax.experimental.pallas import tpu as pltpu
from jax.sharding import PartitionSpec as P

epsilon = 1e-06
CHUNK = 256


def in_one_piece(arrays, axis, dim, along):
    ends, at = ([], 0)
    for a in arrays[:-1]:
        at += a.shape[along]
        ends.append(at)
    both = jnp.concatenate(arrays, axis=along)
    return tuple(jnp.split(lax.all_gather(both, axis, axis=dim, tiled=True), ends, axis=along))


def rms_scaled(values_in):
    return values_in * lax.rsqrt(jnp.mean(values_in * values_in, axis=-1, keepdims=True) + epsilon)


def attention_kernel(heads, head_size, q_ref, k_ref, v_ref, b_ref, gain_ref, out_ref, acc, carry):
    rows = q_ref.shape[0]
    own = lax.axis_index("sp")
    acc[...] = jnp.zeros_like(acc)
    carry[...] = jnp.zeros_like(carry)
    row = lax.broadcasted_iota(jnp.int32, (CHUNK, CHUNK), 0)
    col = lax.broadcasted_iota(jnp.int32, (CHUNK, CHUNK), 1)
    after = (row > col).astype(jnp.bfloat16)

    def chunk(start, masked, query_offset):
        for h in range(heads):
            lanes = slice(h * head_size, (h + 1) * head_size)
            q_neg = q_ref[:, lanes] * jnp.bfloat16(-(head_size ** -0.5))
            k_part = k_ref[pl.ds(start, CHUNK), lanes]
            minus = lax.dot_general(
                q_neg, k_part, (((1,), (1,)), ((), ())), preferred_element_type=jnp.float32
            ) - b_ref[pl.ds(h, 1), pl.ds(start, CHUNK)]
            log_part = jnp.log(1.0 + jnp.exp(-jnp.abs(minus)))
            drop = jnp.minimum(minus, 0.0) - log_part
            own_log = drop - minus
            if masked:
                q_at = lax.broadcasted_iota(jnp.int32, (rows, CHUNK), 0) + query_offset
                k_at = lax.broadcasted_iota(jnp.int32, (rows, CHUNK), 1)
                earlier = k_at < q_at
                drop = jnp.where(earlier, drop, 0.0)
            suffix = jnp.dot(drop.astype(jnp.bfloat16), after, preferred_element_type=jnp.float32)
            within = jnp.exp(own_log + suffix)
            if masked:
                within = jnp.where(earlier, within, 0.0)
            part = jnp.dot(
                within.astype(jnp.bfloat16), v_ref[pl.ds(start, CHUNK), lanes], preferred_element_type=jnp.float32
            )
            now = carry[h]
            acc[h] += jnp.exp(now) * part
            carry[h] = now + (suffix[:, :1] + drop[:, :1])

    def pair(index, masked):
        base = pl.multiple_of((own - 2 * index) * rows, 128)
        for c in reversed(range(2 * rows // CHUNK)):
            chunk(base + c * CHUNK, masked, rows - c * CHUNK)

    pair(0, True)

    def body(index, none):
        pair(index, False)
        return none

    lax.fori_loop(1, (own + 2) // 2, body, 0)
    for h in range(heads):
        mixture = acc[h]
        scaled = mixture * lax.rsqrt(jnp.mean(mixture * mixture, axis=-1, keepdims=True) + epsilon)
        out_ref[:, h * head_size : (h + 1) * head_size] = (scaled * gain_ref[pl.ds(h, 1), :]).astype(jnp.bfloat16)


def attention(queries, keys, values, bias, gain):
    rows = queries.shape[0]
    heads, head_size = gain.shape
    keys = jnp.pad(keys, ((rows, 0), (0, 0)))
    values = jnp.pad(values, ((rows, 0), (0, 0)))
    bias = jnp.pad(bias.astype(jnp.float32).T, ((0, 0), (rows, 0)), constant_values=-30000.0)
    vmem = pl.BlockSpec(memory_space=pltpu.VMEM)
    return pl.pallas_call(
        functools.partial(attention_kernel, heads, head_size),
        out_shape=jax.ShapeDtypeStruct(queries.shape, jnp.bfloat16),
        in_specs=[vmem] * 5,
        out_specs=vmem,
        scratch_shapes=[
            pltpu.VMEM((heads, rows, head_size), jnp.float32),
            pltpu.VMEM((heads, rows, 1), jnp.float32),
        ],
        compiler_params=pltpu.CompilerParams(vmem_limit_bytes=32 << 20),
        name="attention",
    )(queries, keys, values, bias, gain)


def expert_partial(row_block, gate_matrix, up_matrix, down_matrix):
    gate_part = jnp.dot(row_block, gate_matrix, preferred_element_type=jnp.float32)
    up_part = jnp.dot(row_block, up_matrix, preferred_element_type=jnp.float32)
    hidden = (jax.nn.silu(gate_part) * up_part).astype(jnp.bfloat16)
    return jnp.dot(hidden, down_matrix, preferred_element_type=jnp.float32)


def choice_ranks(routes, experts_all):
    flat_routes = routes.reshape(routes.shape[:-2] + (-1,))
    onehot = (flat_routes[..., None] == jnp.arange(experts_all, dtype=jnp.int32)).astype(jnp.int32)
    before = jnp.cumsum(onehot, axis=-2) - onehot
    return jnp.sum(before * onehot, axis=-1).reshape(routes.shape)


def slot_tokens(slot_index, targets, missing):
    flat_slots = slot_index.reshape(-1)
    owners = jnp.arange(flat_slots.shape[0], dtype=jnp.int32) // 2
    matches = flat_slots[None, :] == jnp.arange(targets, dtype=jnp.int32)[:, None]
    owner_found = jnp.sum(jnp.where(matches, owners[None, :], 0), axis=1)
    return jnp.where(jnp.any(matches, axis=1), owner_found, missing)


def on_device(
    queries,
    keys,
    values,
    key_bias,
    head_gain,
    out_weight,
    residual,
    norm_gain,
    gate_proj,
    up_proj,
    down_proj,
    expert_choice,
    expert_weights,
):
    rows_own = queries.shape[0]
    model_width = out_weight.shape[1]
    seq_devices = lax.axis_size("sp")
    head_devices = lax.axis_size("tp")
    key_piece, value_piece, bias_piece = in_one_piece((keys, values, key_bias), "sp", 0, 1)
    attended = attention(queries, key_piece, value_piece, bias_piece, head_gain)
    row_share = rows_own // head_devices
    merged = lax.all_to_all(attended, "tp", split_axis=0, concat_axis=1, tiled=True)
    projected = jnp.dot(
        merged,
        lax.all_gather(out_weight, "tp", axis=0, tiled=True),
        preferred_element_type=jnp.float32,
    )
    stream = (residual.astype(jnp.float32) + projected).astype(jnp.bfloat16)
    normed = (rms_scaled(stream.astype(jnp.float32)) * norm_gain).astype(jnp.bfloat16)
    local_experts = gate_proj.shape[0]
    experts_all = local_experts * seq_devices
    capacity = 4 * rows_own // (head_devices * experts_all)
    own_slots = expert_choice * capacity + choice_ranks(expert_choice, experts_all)
    wanted = slot_tokens(own_slots, experts_all * capacity, row_share)
    outgoing = jnp.take(normed, wanted, axis=0, mode="fill", fill_value=0)
    arrived = lax.all_to_all(
        outgoing.reshape(seq_devices, local_experts, capacity, model_width),
        "sp",
        split_axis=0,
        concat_axis=0,
        tiled=True,
    )
    row_piece = lax.all_gather(arrived, "tp", axis=0, tiled=True)
    count_rows = row_piece.shape[0]
    partials = jnp.stack(
        [
            expert_partial(
                row_piece[:, 0].reshape(-1, model_width), gate_proj[0], up_proj[0], down_proj[0]
            ).reshape(count_rows, capacity, model_width)
        ],
        axis=1,
    )
    summed = lax.psum_scatter(partials.astype(jnp.bfloat16), "tp", scatter_dimension=0, tiled=True)
    returned = lax.all_to_all(summed, "sp", split_axis=0, concat_axis=0, tiled=True).reshape(
        experts_all * capacity, model_width
    )
    picked = jnp.take(returned, own_slots, axis=0).astype(jnp.float32)
    combined = jnp.sum(expert_weights[:, :, None] * picked, axis=1)
    return (stream.astype(jnp.float32) + combined).astype(jnp.bfloat16)


def solution(mesh):
    placed = (
        P("sp", "tp"),
        P("sp", "tp"),
        P("sp", "tp"),
        P("sp", "tp"),
        P("tp", None),
        P("tp", None),
        P(("sp", "tp"), None),
        P(),
        P("sp", None, "tp"),
        P("sp", None, "tp"),
        P("sp", "tp", None),
        P(("sp", "tp"), None),
        P(("sp", "tp"), None),
    )
    return jax.shard_map(
        on_device, mesh=mesh, in_specs=placed, out_specs=P(("sp", "tp"), None), check_vma=False
    )
```

```python
import functools

import jax
import jax.numpy as jnp
from jax import lax
from jax.experimental import pallas as pl
from jax.experimental.pallas import tpu as pltpu
from jax.sharding import PartitionSpec as P

epsilon = 1e-06
CHUNK = 256


def in_one_piece(arrays, axis, dim, along):
    ends, at = ([], 0)
    for a in arrays[:-1]:
        at += a.shape[along]
        ends.append(at)
    both = jnp.concatenate(arrays, axis=along)
    return tuple(jnp.split(lax.all_gather(both, axis, axis=dim, tiled=True), ends, axis=along))


def rms_scaled(values_in):
    return values_in * lax.rsqrt(jnp.mean(values_in * values_in, axis=-1, keepdims=True) + epsilon)


def attention_kernel(heads, head_size, q_ref, k_ref, v_ref, b_ref, gain_ref, out_ref, acc, carry):
    rows = q_ref.shape[0]
    own = lax.axis_index("sp")
    acc[...] = jnp.zeros_like(acc)
    carry[...] = jnp.zeros_like(carry)
    row = lax.broadcasted_iota(jnp.int32, (CHUNK, CHUNK), 0)
    col = lax.broadcasted_iota(jnp.int32, (CHUNK, CHUNK), 1)
    after = (row > col).astype(jnp.bfloat16)

    def chunk(start, masked, query_offset):
        for h in range(heads):
            lanes = slice(h * head_size, (h + 1) * head_size)
            q_neg = q_ref[:, lanes] * jnp.bfloat16(-(head_size ** -0.5))
            k_part = k_ref[pl.ds(start, CHUNK), lanes]
            minus = lax.dot_general(
                q_neg, k_part, (((1,), (1,)), ((), ())), preferred_element_type=jnp.float32
            ) - b_ref[pl.ds(h, 1), pl.ds(start, CHUNK)]
            log_part = jnp.log(1.0 + jnp.exp(-jnp.abs(minus)))
            drop = jnp.minimum(minus, 0.0) - log_part
            own_log = drop - minus
            if masked:
                q_at = lax.broadcasted_iota(jnp.int32, (rows, CHUNK), 0) + query_offset
                k_at = lax.broadcasted_iota(jnp.int32, (rows, CHUNK), 1)
                earlier = k_at < q_at
                drop = jnp.where(earlier, drop, 0.0)
            suffix = jnp.dot(drop.astype(jnp.bfloat16), after, preferred_element_type=jnp.float32)
            within = jnp.exp(own_log + suffix)
            if masked:
                within = jnp.where(earlier, within, 0.0)
            part = jnp.dot(
                within.astype(jnp.bfloat16), v_ref[pl.ds(start, CHUNK), lanes], preferred_element_type=jnp.float32
            )
            now = carry[h]
            acc[h] += jnp.exp(now) * part
            carry[h] = now + (suffix[:, :1] + drop[:, :1])

    def pair(index, masked):
        base = pl.multiple_of((own - 2 * index) * rows, 128)
        for c in reversed(range(2 * rows // CHUNK)):
            chunk(base + c * CHUNK, masked, rows - c * CHUNK)

    pair(0, True)

    def body(index, none):
        pair(index, False)
        return none

    lax.fori_loop(1, (own + 2) // 2, body, 0)
    for h in range(heads):
        mixture = acc[h]
        scaled = mixture * lax.rsqrt(jnp.mean(mixture * mixture, axis=-1, keepdims=True) + epsilon)
        out_ref[:, h * head_size : (h + 1) * head_size] = (scaled * gain_ref[pl.ds(h, 1), :]).astype(jnp.bfloat16)


def attention(queries, keys, values, bias, gain):
    rows = queries.shape[0]
    heads, head_size = gain.shape
    keys = jnp.pad(keys, ((rows, 0), (0, 0)))
    values = jnp.pad(values, ((rows, 0), (0, 0)))
    bias = jnp.pad(bias.astype(jnp.float32).T, ((0, 0), (rows, 0)), constant_values=-30000.0)
    vmem = pl.BlockSpec(memory_space=pltpu.VMEM)
    return pl.pallas_call(
        functools.partial(attention_kernel, heads, head_size),
        out_shape=jax.ShapeDtypeStruct(queries.shape, jnp.bfloat16),
        in_specs=[vmem] * 5,
        out_specs=vmem,
        scratch_shapes=[
            pltpu.VMEM((heads, rows, head_size), jnp.float32),
            pltpu.VMEM((heads, rows, 1), jnp.float32),
        ],
        compiler_params=pltpu.CompilerParams(vmem_limit_bytes=32 << 20),
        name="attention",
    )(queries, keys, values, bias, gain)


def choice_ranks(routes, experts_all):
    flat_routes = routes.reshape(routes.shape[:-2] + (-1,))
    onehot = (flat_routes[..., None] == jnp.arange(experts_all, dtype=jnp.int32)).astype(jnp.int32)
    before = jnp.cumsum(onehot, axis=-2) - onehot
    return jnp.sum(before * onehot, axis=-1).reshape(routes.shape)


MESH = pl.DeviceIdType.MESH
SLOT_ROWS = 8


def remote(src, dst, send_sem, recv_sem, device):
    return pltpu.make_async_remote_copy(
        src_ref=src, dst_ref=dst, send_sem=send_sem, recv_sem=recv_sem, device_id=device, device_id_type=MESH
    )


def expert_kernel(
    cap, stream_ref, normed_ref, select_ref, weight_ref, gate_hbm, up_hbm, down_hbm, out_ref,
    outgoing, arrived, rows, part, partner_part, ring_sum, back, returned, gate_w, up_w, down_w,
    load_sem, go_send, go_recv, ag_send, ag_recv, pair_send, pair_recv, pin_send, pin_recv,
    rs_send, rs_recv, back_send, back_recv,
):
    experts, _, width = outgoing.shape
    chunks, chips, _, block, _ = rows.shape
    far, half, per = chips // 2, width // 2, experts // chunks
    me, t = lax.axis_index("sp"), lax.axis_index("tp")
    z, c = t // 2, t % 2
    partner = (me, 2 * z + (1 - c))
    ahead = ((me, 2 * ((z + 1) % chips) + c), (me, 2 * ((z + chips - 1) % chips) + c))
    piece = (pl.ds(0, half), pl.ds(half, half))

    barrier = pltpu.get_barrier_semaphore()
    for device in (partner, *ahead):
        pl.semaphore_signal(barrier, inc=1, device_id=device, device_id_type=MESH)

    def greet(j, none):
        pl.semaphore_signal(barrier, inc=1, device_id=((me + j) % experts, t), device_id_type=MESH)
        return none

    lax.fori_loop(1, experts, greet, 0)
    loads = [
        pltpu.make_async_copy(src.at[0], dst, load_sem.at[i])
        for i, (src, dst) in enumerate(((gate_hbm, gate_w), (up_hbm, up_w), (down_hbm, down_w)))
    ]
    for load in loads:
        load.start()
    chosen = jnp.dot(select_ref[...], normed_ref[...], preferred_element_type=jnp.float32)
    outgoing[...] = chosen.reshape(experts, SLOT_ROWS, width).astype(jnp.bfloat16)
    for k in range(chunks):
        for d in range(2):
            ring_sum[k, d, 0, :, piece[1 - d]] = jnp.zeros((block, half), jnp.bfloat16)
    pl.semaphore_wait(barrier, experts + 2)

    def go(src, dst, source_id, device):
        return remote(src, dst, go_send.at[source_id], go_recv.at[source_id], device)

    def send_go(j, none):
        e = (me + j) % experts
        remote(outgoing.at[e], arrived.at[me], go_send.at[e], go_recv.at[me], (e, t)).start()
        return none

    lax.fori_loop(1, experts, send_go, 0)
    own = pltpu.make_async_copy(outgoing.at[me], arrived.at[me], go_recv.at[me])
    own.start()

    def take_arrived(k):
        def wait_one(j, none):
            s = k * per + j

            @pl.when(s == me)
            def _():
                own.wait()

            @pl.when(s != me)
            def _():
                remote(outgoing.at[s], arrived.at[s], go_send.at[s], go_recv.at[s], (s, t)).wait_recv()

            return none

        lax.fori_loop(0, per, wait_one, 0)
        row = lax.broadcasted_iota(jnp.int32, (block, per * SLOT_ROWS), 0)
        col = lax.broadcasted_iota(jnp.int32, (block, per * SLOT_ROWS), 1)
        pick = (col == row // cap * SLOT_ROWS + row % cap).astype(jnp.bfloat16)
        padded = arrived[pl.ds(k * per, per)].astype(jnp.float32).reshape(per * SLOT_ROWS, width)
        rows[k, z, c] = jnp.dot(
            pick, padded.astype(jnp.bfloat16), preferred_element_type=jnp.float32
        ).astype(jnp.bfloat16)

    def ring_rows(k, d, i, p, device):
        at = (z - i if d == 0 else z + i) % chips if isinstance(i, int) else lax.rem((z - i if d == 0 else z + i) + chips, chips)
        ref = rows.at[k, at, c, :, piece[p]]
        return remote(ref, ref, ag_send.at[k, d, i, p], ag_recv.at[k, d, i, p], device)

    def to_partner(k, at, p):
        ref = rows.at[k, at, c, :, piece[p]]
        return remote(ref, ref, pair_send.at[k, at, p], pair_recv.at[k, at, p], partner)

    def start_own(k):
        for p in range(2):
            for d in range(2):
                ring_rows(k, d, 0, p if d == 0 else 1 - p, ahead[d]).start()
        for p in range(2):
            to_partner(k, z, p).start()

    def from_ring(k, d, i, p):
        at = lax.rem((z - i - 1 if d == 0 else z + i + 1) + chips, chips)
        ref = rows.at[k, at, c, :, piece[p]]
        return at, remote(ref, ref, ag_send.at[k, d, i, p], ag_recv.at[k, d, i, p], ahead[d])

    def gather_step(k, i):
        for order in range(2):
            for d in range(2):
                p = d if order == 0 else 1 - d

                def handle(d=d, p=p, last=(order == 1)):
                    at, copy = from_ring(k, d, i, p)
                    copy.wait_recv()

                    @pl.when(i + 1 < (far - 1 if last else far))
                    def _():
                        ref = rows.at[k, at, c, :, piece[p]]
                        remote(ref, ref, ag_send.at[k, d, i + 1, p], ag_recv.at[k, d, i + 1, p], ahead[d]).start()

                    to_partner(k, at, p).start()

                if order == 0:
                    handle()
                else:
                    pl.when(i < far - 1)(handle)

    def wait_partner_rows(k):
        def wait_one(at, none):
            for p in range(2):
                ref = rows.at[k, at, 1 - c, :, piece[p]]
                remote(ref, ref, pair_send.at[k, at, p], pair_recv.at[k, at, p], partner).wait_recv()
            return none

        lax.fori_loop(0, chips, wait_one, 0)

    group = chips // far

    def experts_on(k, i):
        at = pl.ds(i * group, group)
        x = rows[k, at].reshape(group * 2 * block, width)
        gate = jnp.dot(x, gate_w[...], preferred_element_type=jnp.float32)
        up = jnp.dot(x, up_w[...], preferred_element_type=jnp.float32)
        hidden = (gate / (1.0 + jnp.exp(-gate)) * up).astype(jnp.bfloat16)
        product = jnp.dot(hidden, down_w[...], preferred_element_type=jnp.float32)
        part[k, at] = product.astype(jnp.bfloat16).reshape(group, 2, block, width)
        for j in range(group):
            pin(k, i * group + j).start()

    def pin(k, at):
        return remote(
            part.at[k, at, 1 - c], partner_part.at[k, at], pin_send.at[k, at], pin_recv.at[k, at], partner
        )

    def wait_pins(k):
        def wait_one(at, none):
            pin(k, at).wait_recv()
            return none

        lax.fori_loop(0, chips, wait_one, 0)

    def ring_step(k, i):
        for order in range(2):
            for d in range(2):
                p = d if order == 0 else 1 - d

                def handle(d=d, p=p, first=(order == 0)):
                    at = lax.rem((z + (far - i) if d == 0 else z - (far - i)) + chips, chips)
                    own_sum = part[k, at, c, :, piece[p]].astype(jnp.float32) + partner_part[
                        k, at, :, piece[p]
                    ].astype(jnp.float32)

                    @pl.when(i == 0)
                    def _():
                        part[k, at, c, :, piece[p]] = own_sum.astype(jnp.bfloat16)

                    @pl.when(i > 0)
                    def _():
                        before = jnp.maximum(i - 1, 0)
                        if first:
                            from_sum(k, d, before, p).wait_recv()
                        else:
                            pl.when(i > 1)(lambda: from_sum(k, d, before, p).wait_recv())
                        total = own_sum + ring_sum[k, d, before, :, piece[p]].astype(jnp.float32)
                        part[k, at, c, :, piece[p]] = total.astype(jnp.bfloat16)

                    remote(
                        part.at[k, at, c, :, piece[p]],
                        ring_sum.at[k, d, i, :, piece[p]],
                        rs_send.at[k, d, i, p],
                        rs_recv.at[k, d, i, p],
                        ahead[d],
                    ).start()

                if order == 0:
                    handle()
                else:
                    pl.when(i > 0)(handle)

    def from_sum(k, d, i, p):
        ref = ring_sum.at[k, d, i, :, piece[p]]
        return remote(ref, ref, rs_send.at[k, d, i, p], rs_recv.at[k, d, i, p], ahead[d])

    def send_back(k):
        for p in range(2):
            for d in range(2):
                from_sum(k, d, far - 1, p).wait_recv()
        total = (
            part[k, z, c].astype(jnp.float32)
            + partner_part[k, z].astype(jnp.float32)
            + ring_sum[k, 0, far - 1].astype(jnp.float32)
            + ring_sum[k, 1, far - 1].astype(jnp.float32)
        ).astype(jnp.bfloat16)
        row = lax.broadcasted_iota(jnp.int32, (per * SLOT_ROWS, block), 0)
        col = lax.broadcasted_iota(jnp.int32, (per * SLOT_ROWS, block), 1)
        spread = ((row % SLOT_ROWS < cap) & (col == row // SLOT_ROWS * cap + row % SLOT_ROWS)).astype(jnp.bfloat16)
        back[pl.ds(k * per, per)] = (
            jnp.dot(spread, total, preferred_element_type=jnp.float32)
            .reshape(per, SLOT_ROWS, width)
            .astype(jnp.bfloat16)
        )

        def send_one(j, none):
            s = k * per + j

            @pl.when(s != me)
            def _():
                remote(back.at[s], returned.at[me], back_send.at[s], back_recv.at[me], (s, t)).start()

            @pl.when(s == me)
            def _():
                pltpu.make_async_copy(back.at[s], returned.at[me], back_recv.at[me]).start()

            return none

        lax.fori_loop(0, per, send_one, 0)

    def steps(body):
        def one(i, none):
            body(i)
            return none

        lax.fori_loop(0, far, one, 0)

    take_arrived(0)
    start_own(0)
    take_arrived(1)
    steps(lambda i: gather_step(0, i))
    start_own(1)
    for load in loads:
        load.wait()
    wait_partner_rows(0)

    def gather_and_compute(i):
        gather_step(1, i)
        experts_on(0, i)

    steps(gather_and_compute)
    wait_partner_rows(1)
    wait_pins(0)

    def sum_and_compute(i):
        ring_step(0, i)
        experts_on(1, i)

    steps(sum_and_compute)
    wait_pins(1)
    steps(lambda i: (pl.when(i == 1)(lambda: send_back(0)), ring_step(1, i)))
    send_back(1)

    def wait_back(e, none):
        @pl.when(e == me)
        def _():
            pltpu.make_async_copy(back.at[e], returned.at[e], back_recv.at[e]).wait()

        @pl.when(e != me)
        def _():
            remote(back.at[e], returned.at[e], back_send.at[e], back_recv.at[e], (e, t)).wait_recv()

        return none

    lax.fori_loop(0, experts, wait_back, 0)
    weights = weight_ref[...]
    high = weights.astype(jnp.bfloat16)
    rest = weights - high.astype(jnp.float32)
    middle = rest.astype(jnp.bfloat16)
    low = (rest - middle.astype(jnp.float32)).astype(jnp.bfloat16)
    picked = returned[...].astype(jnp.float32).reshape(experts * SLOT_ROWS, width).astype(jnp.bfloat16)
    combined = stream_ref[...].astype(jnp.float32)
    for share in (low, middle, high):
        combined = combined + jnp.dot(share, picked, preferred_element_type=jnp.float32)
    out_ref[...] = combined.astype(jnp.bfloat16)

    def drain_sp(j, none):
        e = (me + j) % experts
        remote(outgoing.at[e], arrived.at[me], go_send.at[e], go_recv.at[me], (e, t)).wait_send()
        remote(back.at[e], returned.at[me], back_send.at[e], back_recv.at[me], (e, t)).wait_send()
        return none

    lax.fori_loop(1, experts, drain_sp, 0)

    def drain_pair(at, none):
        for k in range(chunks):
            for p in range(2):
                to_partner(k, at, p).wait_send()
            pin(k, at).wait_send()
        return none

    lax.fori_loop(0, chips, drain_pair, 0)

    def drain_ring(i, none):
        for k in range(chunks):
            for d in range(2):
                for p in range(2):

                    def sent(k=k, d=d, p=p):
                        ref = rows.at[k, 0, c, :, piece[p]]
                        remote(ref, ref, ag_send.at[k, d, i, p], ag_recv.at[k, d, i, p], ahead[d]).wait_send()

                    def summed(k=k, d=d, p=p):
                        ref = rows.at[k, 0, c, :, piece[p]]
                        remote(ref, ref, rs_send.at[k, d, i, p], rs_recv.at[k, d, i, p], ahead[d]).wait_send()

                    if p == d:
                        sent()
                        summed()
                    else:
                        pl.when(i < far - 1)(sent)
                        pl.when(i > 0)(summed)
        return none

    lax.fori_loop(0, far, drain_ring, 0)


def expert_layer(stream, normed, choice, choice_weights, gate_proj, up_proj, down_proj, seq_devices, head_devices, cap):
    own_rows, width = stream.shape
    hidden = gate_proj.shape[2]
    experts, chips, chunks = seq_devices, head_devices // 2, 2
    far, block = chips // 2, seq_devices // chunks * cap
    slots = choice * SLOT_ROWS + choice_ranks(choice, experts)
    targets = jnp.arange(experts * SLOT_ROWS, dtype=jnp.int32)
    match = slots[:, :, None] == targets[None, None, :]
    select = jnp.any(match, axis=1).T.astype(jnp.bfloat16)
    weights = jnp.sum(jnp.where(match, choice_weights[:, :, None], 0.0), axis=1)
    vmem, hbm = pl.BlockSpec(memory_space=pltpu.VMEM), pl.BlockSpec(memory_space=pl.ANY)
    bf16, dma = jnp.bfloat16, pltpu.SemaphoreType.DMA
    return pl.pallas_call(
        functools.partial(expert_kernel, cap),
        out_shape=jax.ShapeDtypeStruct(stream.shape, bf16),
        in_specs=[vmem] * 4 + [hbm] * 3,
        out_specs=vmem,
        scratch_shapes=[
            pltpu.VMEM((experts, SLOT_ROWS, width), bf16),
            pltpu.VMEM((experts, SLOT_ROWS, width), bf16),
            pltpu.VMEM((chunks, chips, 2, block, width), bf16),
            pltpu.VMEM((chunks, chips, 2, block, width), bf16),
            pltpu.VMEM((chunks, chips, block, width), bf16),
            pltpu.VMEM((chunks, 2, far, block, width), bf16),
            pltpu.VMEM((experts, SLOT_ROWS, width), bf16),
            pltpu.VMEM((experts, SLOT_ROWS, width), bf16),
            pltpu.VMEM((width, hidden), bf16),
            pltpu.VMEM((width, hidden), bf16),
            pltpu.VMEM((hidden, width), bf16),
            dma((3,)),
            dma((experts,)),
            dma((experts,)),
            dma((chunks, 2, far, 2)),
            dma((chunks, 2, far, 2)),
            dma((chunks, chips, 2)),
            dma((chunks, chips, 2)),
            dma((chunks, chips)),
            dma((chunks, chips)),
            dma((chunks, 2, far, 2)),
            dma((chunks, 2, far, 2)),
            dma((experts,)),
            dma((experts,)),
        ],
        compiler_params=pltpu.CompilerParams(
            collective_id=1, has_side_effects=True, vmem_limit_bytes=56 << 20
        ),
        name="experts",
    )(stream, normed, select, weights, gate_proj, up_proj, down_proj)


def on_device(
    queries,
    keys,
    values,
    key_bias,
    head_gain,
    out_weight,
    residual,
    norm_gain,
    gate_proj,
    up_proj,
    down_proj,
    expert_choice,
    expert_weights,
):
    rows_own = queries.shape[0]
    model_width = out_weight.shape[1]
    seq_devices = lax.axis_size("sp")
    head_devices = lax.axis_size("tp")
    key_piece, value_piece, bias_piece = in_one_piece((keys, values, key_bias), "sp", 0, 1)
    attended = attention(queries, key_piece, value_piece, bias_piece, head_gain)
    row_share = rows_own // head_devices
    merged = lax.all_to_all(attended, "tp", split_axis=0, concat_axis=1, tiled=True)
    projected = jnp.dot(
        merged,
        lax.all_gather(out_weight, "tp", axis=0, tiled=True),
        preferred_element_type=jnp.float32,
    )
    stream = (residual.astype(jnp.float32) + projected).astype(jnp.bfloat16)
    normed = (rms_scaled(stream.astype(jnp.float32)) * norm_gain).astype(jnp.bfloat16)
    cap = 4 * rows_own // (head_devices * seq_devices)
    return expert_layer(
        stream, normed, expert_choice, expert_weights, gate_proj, up_proj, down_proj, seq_devices, head_devices, cap
    )


def solution(mesh):
    placed = (
        P("sp", "tp"),
        P("sp", "tp"),
        P("sp", "tp"),
        P("sp", "tp"),
        P("tp", None),
        P("tp", None),
        P(("sp", "tp"), None),
        P(),
        P("sp", None, "tp"),
        P("sp", None, "tp"),
        P("sp", "tp", None),
        P(("sp", "tp"), None),
        P(("sp", "tp"), None),
    )
    return jax.shard_map(
        on_device, mesh=mesh, in_specs=placed, out_specs=P(("sp", "tp"), None), check_vma=False
    )
```

```python
import functools

import jax
import jax.numpy as jnp
from jax import lax
from jax.experimental import pallas as pl
from jax.experimental.pallas import tpu as pltpu
from jax.sharding import PartitionSpec as P

epsilon = 1e-06
CHUNK = 256
MESH = pl.DeviceIdType.MESH
SLOT_ROWS = 8


def remote(src, dst, send_sem, recv_sem, device):
    return pltpu.make_async_remote_copy(
        src_ref=src, dst_ref=dst, send_sem=send_sem, recv_sem=recv_sem, device_id=device, device_id_type=MESH
    )


def choice_ranks(routes, experts_all):
    flat_routes = routes.reshape(routes.shape[:-2] + (-1,))
    onehot = (flat_routes[..., None] == jnp.arange(experts_all, dtype=jnp.int32)).astype(jnp.int32)
    before = jnp.cumsum(onehot, axis=-2) - onehot
    return jnp.sum(before * onehot, axis=-1).reshape(routes.shape)


def attention_kernel(
    chips_y, q_ref, k_ref, v_ref, bias_ref, gain_ref, w_ref, residual_ref, norm_ref, stream_ref, normed_ref,
    kv_out, q_out, kv, q_in, gains, weights, acc, carry, att_out, att_in, part, part_out, ring_sum,
    kv_send, kv_recv, q_send, q_recv, x_send, x_recv, pair_send, pair_recv, w_send, w_recv, g_send, g_recv,
    att_send, att_recv, rs_send, rs_recv,
):
    rows, packed = q_ref.shape
    size = packed // 2
    chips_x = lax.axis_size("sp") // chips_y
    chips = lax.axis_size("tp") // 2
    width = w_ref.shape[1]
    far, half = chips // 2, width // 2
    piece = (pl.ds(0, half), pl.ds(half, half))
    me, t = lax.axis_index("sp"), lax.axis_index("tp")
    y, x, z, c = me // chips_x, me % chips_x, t // 2, t % 2

    def device(yy, xx, zz, cc):
        return (yy * chips_x + xx, 2 * zz + cc)

    def query_core(yy):
        return ((yy + 1) // 2) % 2

    partner = device(y, x, z, 1 - c)
    beside = (device(y, (x + 1) % chips_x, z, c), device(y, (x + chips_x - 1) % chips_x, z, c))
    ahead = (device(y, x, (z + 1) % chips, c), device(y, x, (z + chips - 1) % chips, c))
    ring = [
        device((y + dy) % chips_y, x, z, (c + dc) % 2) for dy in range(chips_y) for dc in range(2) if (dy, dc) != (0, 0)
    ]
    barrier = pltpu.get_barrier_semaphore()
    met = [*ring, *beside, *ahead]
    for other in met:
        pl.semaphore_signal(barrier, inc=1, device_id=other, device_id_type=MESH)

    empty = jnp.zeros((rows, size), jnp.bfloat16)
    for h in range(2):
        lanes = slice(h * size, (h + 1) * size)
        kv_out[h, pl.ds(0, rows)] = jnp.concatenate([k_ref[:, lanes], v_ref[:, lanes]], axis=1)
        kv_out[h, pl.ds(rows, 16)] = bias_ref[h]
        q_out[h] = jnp.concatenate([q_ref[:, lanes] * jnp.bfloat16(-(size ** -0.5)), empty], axis=1)
    kv[0, pl.ds(0, rows)] = jnp.zeros((rows, packed), jnp.bfloat16)
    kv[0, pl.ds(rows, 16)] = jnp.full((16, packed), -30000.0, jnp.bfloat16)
    weights[c] = w_ref[...]
    gains[c] = gain_ref[...]
    pl.semaphore_wait(barrier, len(met))

    at_home = (y // 2 == c) & (y % 2 == c)
    asks_self = (y // 2 == c) & (query_core(y) == c)
    for h in range(2):
        j = 2 * c + h

        def kv_remote(h=h, j=j):
            return remote(kv_out.at[h], kv.at[me + 1], kv_send.at[h], kv_recv.at[y // 2], device(j, x, z, y % 2))

        def q_remote(h=h, j=j):
            return remote(q_out.at[h], q_in.at[y // 2], q_send.at[h], q_recv.at[y // 2], device(j, x, z, query_core(y)))

        here = at_home & (j == y)
        asks = asks_self & (j == y)
        pl.when(jnp.logical_not(here))(lambda f=kv_remote: f().start())
        pl.when(jnp.logical_not(asks))(lambda f=q_remote: f().start())

        @pl.when(here)
        def _(h=h):
            pltpu.make_async_copy(kv_out.at[h], kv.at[me + 1], kv_recv.at[y // 2]).start()

        @pl.when(asks)
        def _(h=h):
            pltpu.make_async_copy(q_out.at[h], q_in.at[y // 2], q_recv.at[y // 2]).start()

    to_w = remote(w_ref, weights.at[c], w_send.at[0], w_recv.at[0], partner)
    to_g = remote(gain_ref, gains.at[c], g_send.at[0], g_recv.at[0], partner)
    to_g.start()

    def block_at(k, xx):
        return kv.at[(c + 2 * k) * chips_x + xx + 1]

    def to_partner(k, xx):
        ref = block_at(k, xx)
        return remote(ref, ref, pair_send.at[k, xx], pair_recv.at[k, xx], partner)

    def along(d, n, k, xx):
        ref = block_at(k, xx)
        return remote(ref, ref, x_send.at[d, n], x_recv.at[d, n], beside[d])

    back_x = ((x + chips_x - 1) % chips_x, (x + 1) % chips_x)
    across = (x + 2) % chips_x
    for k in range(2):
        kept = at_home & (c + 2 * k == y)

        @pl.when(kept)
        def _(k=k):
            pltpu.make_async_copy(kv_out.at[0], block_at(k, x), kv_recv.at[k]).wait()

        @pl.when(jnp.logical_not(kept))
        def _(k=k):
            remote(kv_out.at[0], block_at(k, x), kv_send.at[0], kv_recv.at[k], partner).wait_recv()

        for d in range(2):
            along(d, k, k, x).start()
        to_partner(k, x).start()
    to_w.start()
    for d in range(2):
        along(d, d, d, back_x[d]).wait_recv()
        along(d, 2, d, back_x[d]).start()
        to_partner(d, back_x[d]).start()
    for d in range(2):
        along(d, 1 - d, 1 - d, back_x[d]).wait_recv()
        to_partner(1 - d, back_x[d]).start()
    for d in range(2):
        along(d, 2, d, across).wait_recv()
        to_partner(d, across).start()
    to_g.wait_recv()

    def wait_pair(n, none):
        k, xx = n // chips_x, n % chips_x
        ref = kv.at[(1 - c + 2 * k) * chips_x + xx + 1]
        remote(ref, ref, pair_send.at[k, xx], pair_recv.at[k, xx], partner).wait_recv()
        return none

    lax.fori_loop(0, 2 * chips_x, wait_pair, 0)

    row = lax.broadcasted_iota(jnp.int32, (CHUNK, CHUNK), 0)
    col = lax.broadcasted_iota(jnp.int32, (CHUNK, CHUNK), 1)
    after = (row > col).astype(jnp.bfloat16)

    def attend(slot):
        from_y = c if slot == 0 else 3 - c
        block = from_y * chips_x + x
        asked = asks_self & (from_y == y)

        @pl.when(asked)
        def _():
            pltpu.make_async_copy(q_out.at[0], q_in.at[slot], q_recv.at[slot]).wait()

        @pl.when(jnp.logical_not(asked))
        def _():
            remote(q_out.at[0], q_in.at[slot], q_send.at[0], q_recv.at[slot], partner).wait_recv()

        acc[...] = jnp.zeros_like(acc)
        carry[...] = jnp.zeros_like(carry)

        def pair(index, masked):
            older = block - 2 * index

            def part_of(place, first, length):
                return kv[older + place, pl.ds(first, length)], kv[older + place, pl.ds(rows, 16)], first // 128, length // 128

            def chunk(sources, place):
                kv_part = jnp.concatenate([s[0] for s in sources], axis=0)
                offset = jnp.concatenate(
                    [s[1][s[2] + n : s[2] + n + 1, :].astype(jnp.float32) for s in sources for n in range(s[3])], axis=1
                )
                minus = (
                    lax.dot_general(
                        q_in[slot], kv_part, (((1,), (1,)), ((), ())), preferred_element_type=jnp.float32
                    )
                    - offset
                )
                log_part = jnp.log(1.0 + jnp.exp(-jnp.abs(minus)))
                drop = jnp.minimum(minus, 0.0) - log_part
                own_log = drop - minus
                if masked:
                    q_at = lax.broadcasted_iota(jnp.int32, (rows, CHUNK), 0) + (rows - place)
                    earlier = lax.broadcasted_iota(jnp.int32, (rows, CHUNK), 1) < q_at
                    drop = jnp.where(earlier, drop, 0.0)
                suffix = jnp.dot(drop.astype(jnp.bfloat16), after, preferred_element_type=jnp.float32)
                within = jnp.exp(own_log + suffix)
                if masked:
                    within = jnp.where(earlier, within, 0.0)
                product = jnp.dot(within.astype(jnp.bfloat16), kv_part, preferred_element_type=jnp.float32)
                now = carry[...]
                acc[...] += jnp.exp(now) * product
                carry[...] = now + (suffix[:, :1] + drop[:, :1])

            chunk([part_of(1, 128, 256)], 512)
            chunk([part_of(0, 256, 128), part_of(1, 0, 128)], 256)
            chunk([part_of(0, 0, 256)], 0)

        pair(0, True)

        def body(index, none):
            pair(index, False)
            return none

        lax.fori_loop(1, (block + 2) // 2, body, 0)
        mixture = acc[...][:, size:]
        scaled = mixture * lax.rsqrt(jnp.mean(mixture * mixture, axis=-1, keepdims=True) + epsilon)
        scaled = scaled * gains[y // 2, pl.ds(y % 2, 1), :]
        by_owner = scaled.reshape(chips, 2, rows // (2 * chips), size)
        for p in range(2):
            att_out[slot, p] = by_owner[:, p].astype(jnp.bfloat16)
            stays = (from_y == y) & (p == c)

            @pl.when(stays)
            def _(p=p):
                pltpu.make_async_copy(att_out.at[slot, p], att_in.at[y], att_recv.at[y]).start()

            @pl.when(jnp.logical_not(stays))
            def _(p=p):
                send_att(slot, p, from_y).start()

    def send_att(slot, p, from_y):
        return remote(
            att_out.at[slot, p], att_in.at[y], att_send.at[slot, p], att_recv.at[y], device(from_y, x, z, p)
        )

    attend(1)
    attend(0)

    for j in range(chips_y):
        stayed = (j == y) & (query_core(y) == c)

        @pl.when(stayed)
        def _(j=j):
            pltpu.make_async_copy(att_out.at[0, 0], att_in.at[j], att_recv.at[j]).wait()

        @pl.when(jnp.logical_not(stayed))
        def _(j=j):
            remote(att_out.at[0, 0], att_in.at[j], att_send.at[0, 0], att_recv.at[j], partner).wait_recv()

    to_w.wait_recv()
    heads = [att_in[j].astype(jnp.float32).reshape(rows // 2, size) for j in range(chips_y)]
    merged = jnp.concatenate(heads, axis=1).astype(jnp.bfloat16)
    share = jnp.dot(merged, weights[...].reshape(2 * packed, width), preferred_element_type=jnp.float32)
    part[...] = share.reshape(part.shape)

    def from_sum(d, i, p):
        ref = ring_sum.at[d, i, :, piece[p]]
        return remote(ref, ref, rs_send.at[d, i, p], rs_recv.at[d, i, p], ahead[d])

    for i in range(far):
        for order in range(2):
            for d in range(2):
                p = d if order == 0 else 1 - d
                if i == 0 and p != d:
                    continue
                at = ((z + (far - i)) if d == 0 else (z - (far - i) + chips)) % chips
                total = part[at, :, piece[p]]
                if i > 1 or (i == 1 and p == d):
                    from_sum(d, i - 1, p).wait_recv()
                    total = total + ring_sum[d, i - 1, :, piece[p]].astype(jnp.float32)
                part_out[d, i, :, piece[p]] = total.astype(jnp.bfloat16)
                remote(
                    part_out.at[d, i, :, piece[p]],
                    ring_sum.at[d, i, :, piece[p]],
                    rs_send.at[d, i, p],
                    rs_recv.at[d, i, p],
                    ahead[d],
                ).start()
    for d in range(2):
        for p in range(2):
            from_sum(d, far - 1, p).wait_recv()
    projected = part[z] + ring_sum[0, far - 1].astype(jnp.float32) + ring_sum[1, far - 1].astype(jnp.float32)
    stream = (residual_ref[...].astype(jnp.float32) + projected).astype(jnp.bfloat16)
    stream_ref[...] = stream
    wide = stream.astype(jnp.float32)
    normed_ref[...] = (
        wide * lax.rsqrt(jnp.mean(wide * wide, axis=-1, keepdims=True) + epsilon) * norm_ref[...]
    ).astype(jnp.bfloat16)

    for h in range(2):
        j = 2 * c + h

        @pl.when(jnp.logical_not(at_home & (j == y)))
        def _(h=h):
            remote(kv_out.at[h], kv.at[0], kv_send.at[h], kv_recv.at[0], partner).wait_send()

        @pl.when(jnp.logical_not(asks_self & (j == y)))
        def _(h=h):
            remote(q_out.at[h], q_in.at[0], q_send.at[h], q_recv.at[0], partner).wait_send()

    to_w.wait_send()
    to_g.wait_send()
    for d in range(2):
        for n in range(3):
            along(d, n, 0, x).wait_send()

    def drain_pair(n, none):
        to_partner(n // chips_x, n % chips_x).wait_send()
        return none

    lax.fori_loop(0, 2 * chips_x, drain_pair, 0)
    for slot in range(2):
        from_y = c if slot == 0 else 3 - c
        for p in range(2):

            @pl.when(jnp.logical_not((from_y == y) & (p == c)))
            def _(slot=slot, p=p, from_y=from_y):
                send_att(slot, p, from_y).wait_send()

    for d in range(2):
        for i in range(far):
            for p in range(2):
                if i > 0 or p == d:
                    from_sum(d, i, p).wait_send()


def attention_layer(queries, keys, values, key_bias, head_gain, out_weight, residual, norm_gain):
    rows, packed = queries.shape
    size, width = head_gain.shape[1], out_weight.shape[1]
    blocks, chips, chips_y = lax.axis_size("sp"), lax.axis_size("tp") // 2, 4
    chips_x, far, own = blocks // chips_y, chips // 2, residual.shape[0]
    bias = jnp.pad(key_bias.T.reshape(2, rows // 128, 128), ((0, 0), (0, 16 - rows // 128), (0, 0)))
    vmem = pl.BlockSpec(memory_space=pltpu.VMEM)
    bf16, f32, dma = jnp.bfloat16, jnp.float32, pltpu.SemaphoreType.DMA
    return pl.pallas_call(
        functools.partial(attention_kernel, chips_y),
        out_shape=[jax.ShapeDtypeStruct(residual.shape, bf16)] * 2,
        in_specs=[vmem] * 8,
        out_specs=[vmem] * 2,
        scratch_shapes=[
            pltpu.VMEM((2, rows + 16, packed), bf16),
            pltpu.VMEM((2, rows, packed), bf16),
            pltpu.VMEM((blocks + 1, rows + 16, packed), bf16),
            pltpu.VMEM((2, rows, packed), bf16),
            pltpu.VMEM((2, 2, size), f32),
            pltpu.VMEM((2, packed, width), bf16),
            pltpu.VMEM((rows, packed), f32),
            pltpu.VMEM((rows, 1), f32),
            pltpu.VMEM((2, 2, chips, own, size), bf16),
            pltpu.VMEM((chips_y, chips, own, size), bf16),
            pltpu.VMEM((chips, own, width), f32),
            pltpu.VMEM((2, far, own, width), bf16),
            pltpu.VMEM((2, far, own, width), bf16),
            dma((2,)),
            dma((2,)),
            dma((2,)),
            dma((2,)),
            dma((2, 3)),
            dma((2, 3)),
            dma((2, chips_x)),
            dma((2, chips_x)),
            dma((1,)),
            dma((1,)),
            dma((1,)),
            dma((1,)),
            dma((2, 2)),
            dma((chips_y,)),
            dma((2, far, 2)),
            dma((2, far, 2)),
        ],
        compiler_params=pltpu.CompilerParams(collective_id=2, has_side_effects=True, vmem_limit_bytes=40 << 20),
        name="attention",
    )(queries, keys, values, bias, head_gain, out_weight, residual, norm_gain.reshape(1, -1))


def expert_kernel(
    cap, stream_ref, normed_ref, select_ref, weight_ref, gate_hbm, up_hbm, down_hbm, out_ref,
    outgoing, arrived, rows, part, partner_part, ring_sum, back, returned, gate_w, up_w, down_w,
    load_sem, go_send, go_recv, ag_send, ag_recv, pair_send, pair_recv, pin_send, pin_recv,
    rs_send, rs_recv, back_send, back_recv,
):
    experts, _, width = outgoing.shape
    chunks, chips, _, block, _ = rows.shape
    far, half, per = chips // 2, width // 2, experts // chunks
    me, t = lax.axis_index("sp"), lax.axis_index("tp")
    z, c = t // 2, t % 2
    partner = (me, 2 * z + (1 - c))
    ahead = ((me, 2 * ((z + 1) % chips) + c), (me, 2 * ((z + chips - 1) % chips) + c))
    piece = (pl.ds(0, half), pl.ds(half, half))

    barrier = pltpu.get_barrier_semaphore()
    for device in (partner, *ahead):
        pl.semaphore_signal(barrier, inc=1, device_id=device, device_id_type=MESH)

    def greet(j, none):
        pl.semaphore_signal(barrier, inc=1, device_id=((me + j) % experts, t), device_id_type=MESH)
        return none

    lax.fori_loop(1, experts, greet, 0)
    loads = [
        pltpu.make_async_copy(src.at[0], dst, load_sem.at[i])
        for i, (src, dst) in enumerate(((gate_hbm, gate_w), (up_hbm, up_w), (down_hbm, down_w)))
    ]
    for load in loads:
        load.start()
    chosen = jnp.dot(select_ref[...], normed_ref[...], preferred_element_type=jnp.float32)
    outgoing[...] = chosen.reshape(experts, SLOT_ROWS, width).astype(jnp.bfloat16)
    for k in range(chunks):
        for d in range(2):
            ring_sum[k, d, 0, :, piece[1 - d]] = jnp.zeros((block, half), jnp.bfloat16)
    pl.semaphore_wait(barrier, experts + 2)

    def go(src, dst, source_id, device):
        return remote(src, dst, go_send.at[source_id], go_recv.at[source_id], device)

    def send_go(j, none):
        e = (me + j) % experts
        remote(outgoing.at[e], arrived.at[me], go_send.at[e], go_recv.at[me], (e, t)).start()
        return none

    lax.fori_loop(1, experts, send_go, 0)
    own = pltpu.make_async_copy(outgoing.at[me], arrived.at[me], go_recv.at[me])
    own.start()

    def take_arrived(k):
        def wait_one(j, none):
            s = k * per + j

            @pl.when(s == me)
            def _():
                own.wait()

            @pl.when(s != me)
            def _():
                remote(outgoing.at[s], arrived.at[s], go_send.at[s], go_recv.at[s], (s, t)).wait_recv()

            return none

        lax.fori_loop(0, per, wait_one, 0)
        row = lax.broadcasted_iota(jnp.int32, (block, per * SLOT_ROWS), 0)
        col = lax.broadcasted_iota(jnp.int32, (block, per * SLOT_ROWS), 1)
        pick = (col == row // cap * SLOT_ROWS + row % cap).astype(jnp.bfloat16)
        padded = arrived[pl.ds(k * per, per)].astype(jnp.float32).reshape(per * SLOT_ROWS, width)
        rows[k, z, c] = jnp.dot(
            pick, padded.astype(jnp.bfloat16), preferred_element_type=jnp.float32
        ).astype(jnp.bfloat16)

    def ring_rows(k, d, i, p, device):
        at = (z - i if d == 0 else z + i) % chips if isinstance(i, int) else lax.rem((z - i if d == 0 else z + i) + chips, chips)
        ref = rows.at[k, at, c, :, piece[p]]
        return remote(ref, ref, ag_send.at[k, d, i, p], ag_recv.at[k, d, i, p], device)

    def to_partner(k, at, p):
        ref = rows.at[k, at, c, :, piece[p]]
        return remote(ref, ref, pair_send.at[k, at, p], pair_recv.at[k, at, p], partner)

    def start_own(k):
        for p in range(2):
            for d in range(2):
                ring_rows(k, d, 0, p if d == 0 else 1 - p, ahead[d]).start()
        for p in range(2):
            to_partner(k, z, p).start()

    def from_ring(k, d, i, p):
        at = lax.rem((z - i - 1 if d == 0 else z + i + 1) + chips, chips)
        ref = rows.at[k, at, c, :, piece[p]]
        return at, remote(ref, ref, ag_send.at[k, d, i, p], ag_recv.at[k, d, i, p], ahead[d])

    def gather_step(k, i):
        for order in range(2):
            for d in range(2):
                p = d if order == 0 else 1 - d

                def handle(d=d, p=p, last=(order == 1)):
                    at, copy = from_ring(k, d, i, p)
                    copy.wait_recv()

                    @pl.when(i + 1 < (far - 1 if last else far))
                    def _():
                        ref = rows.at[k, at, c, :, piece[p]]
                        remote(ref, ref, ag_send.at[k, d, i + 1, p], ag_recv.at[k, d, i + 1, p], ahead[d]).start()

                    to_partner(k, at, p).start()

                if order == 0:
                    handle()
                else:
                    pl.when(i < far - 1)(handle)

    def wait_partner_rows(k):
        def wait_one(at, none):
            for p in range(2):
                ref = rows.at[k, at, 1 - c, :, piece[p]]
                remote(ref, ref, pair_send.at[k, at, p], pair_recv.at[k, at, p], partner).wait_recv()
            return none

        lax.fori_loop(0, chips, wait_one, 0)

    group = chips // far

    def experts_on(k, i):
        at = pl.ds(i * group, group)
        x = rows[k, at].reshape(group * 2 * block, width)
        gate = jnp.dot(x, gate_w[...], preferred_element_type=jnp.float32)
        up = jnp.dot(x, up_w[...], preferred_element_type=jnp.float32)
        hidden = (gate / (1.0 + jnp.exp(-gate)) * up).astype(jnp.bfloat16)
        product = jnp.dot(hidden, down_w[...], preferred_element_type=jnp.float32)
        part[k, at] = product.astype(jnp.bfloat16).reshape(group, 2, block, width)
        for j in range(group):
            pin(k, i * group + j).start()

    def pin(k, at):
        return remote(
            part.at[k, at, 1 - c], partner_part.at[k, at], pin_send.at[k, at], pin_recv.at[k, at], partner
        )

    def wait_pins(k):
        def wait_one(at, none):
            pin(k, at).wait_recv()
            return none

        lax.fori_loop(0, chips, wait_one, 0)

    def ring_step(k, i):
        for order in range(2):
            for d in range(2):
                p = d if order == 0 else 1 - d

                def handle(d=d, p=p, first=(order == 0)):
                    at = lax.rem((z + (far - i) if d == 0 else z - (far - i)) + chips, chips)
                    own_sum = part[k, at, c, :, piece[p]].astype(jnp.float32) + partner_part[
                        k, at, :, piece[p]
                    ].astype(jnp.float32)

                    @pl.when(i == 0)
                    def _():
                        part[k, at, c, :, piece[p]] = own_sum.astype(jnp.bfloat16)

                    @pl.when(i > 0)
                    def _():
                        before = jnp.maximum(i - 1, 0)
                        if first:
                            from_sum(k, d, before, p).wait_recv()
                        else:
                            pl.when(i > 1)(lambda: from_sum(k, d, before, p).wait_recv())
                        total = own_sum + ring_sum[k, d, before, :, piece[p]].astype(jnp.float32)
                        part[k, at, c, :, piece[p]] = total.astype(jnp.bfloat16)

                    remote(
                        part.at[k, at, c, :, piece[p]],
                        ring_sum.at[k, d, i, :, piece[p]],
                        rs_send.at[k, d, i, p],
                        rs_recv.at[k, d, i, p],
                        ahead[d],
                    ).start()

                if order == 0:
                    handle()
                else:
                    pl.when(i > 0)(handle)

    def from_sum(k, d, i, p):
        ref = ring_sum.at[k, d, i, :, piece[p]]
        return remote(ref, ref, rs_send.at[k, d, i, p], rs_recv.at[k, d, i, p], ahead[d])

    def send_back(k):
        for p in range(2):
            for d in range(2):
                from_sum(k, d, far - 1, p).wait_recv()
        total = (
            part[k, z, c].astype(jnp.float32)
            + partner_part[k, z].astype(jnp.float32)
            + ring_sum[k, 0, far - 1].astype(jnp.float32)
            + ring_sum[k, 1, far - 1].astype(jnp.float32)
        ).astype(jnp.bfloat16)
        row = lax.broadcasted_iota(jnp.int32, (per * SLOT_ROWS, block), 0)
        col = lax.broadcasted_iota(jnp.int32, (per * SLOT_ROWS, block), 1)
        spread = ((row % SLOT_ROWS < cap) & (col == row // SLOT_ROWS * cap + row % SLOT_ROWS)).astype(jnp.bfloat16)
        back[pl.ds(k * per, per)] = (
            jnp.dot(spread, total, preferred_element_type=jnp.float32)
            .reshape(per, SLOT_ROWS, width)
            .astype(jnp.bfloat16)
        )

        def send_one(j, none):
            s = k * per + j

            @pl.when(s != me)
            def _():
                remote(back.at[s], returned.at[me], back_send.at[s], back_recv.at[me], (s, t)).start()

            @pl.when(s == me)
            def _():
                pltpu.make_async_copy(back.at[s], returned.at[me], back_recv.at[me]).start()

            return none

        lax.fori_loop(0, per, send_one, 0)

    def steps(body):
        def one(i, none):
            body(i)
            return none

        lax.fori_loop(0, far, one, 0)

    take_arrived(0)
    start_own(0)
    take_arrived(1)
    steps(lambda i: gather_step(0, i))
    start_own(1)
    for load in loads:
        load.wait()
    wait_partner_rows(0)

    def gather_and_compute(i):
        gather_step(1, i)
        experts_on(0, i)

    steps(gather_and_compute)
    wait_partner_rows(1)
    wait_pins(0)

    def sum_and_compute(i):
        ring_step(0, i)
        experts_on(1, i)

    steps(sum_and_compute)
    wait_pins(1)
    steps(lambda i: (pl.when(i == 1)(lambda: send_back(0)), ring_step(1, i)))
    send_back(1)

    def wait_back(e, none):
        @pl.when(e == me)
        def _():
            pltpu.make_async_copy(back.at[e], returned.at[e], back_recv.at[e]).wait()

        @pl.when(e != me)
        def _():
            remote(back.at[e], returned.at[e], back_send.at[e], back_recv.at[e], (e, t)).wait_recv()

        return none

    lax.fori_loop(0, experts, wait_back, 0)
    weights = weight_ref[...]
    high = weights.astype(jnp.bfloat16)
    rest = weights - high.astype(jnp.float32)
    middle = rest.astype(jnp.bfloat16)
    low = (rest - middle.astype(jnp.float32)).astype(jnp.bfloat16)
    picked = returned[...].astype(jnp.float32).reshape(experts * SLOT_ROWS, width).astype(jnp.bfloat16)
    combined = stream_ref[...].astype(jnp.float32)
    for share in (low, middle, high):
        combined = combined + jnp.dot(share, picked, preferred_element_type=jnp.float32)
    out_ref[...] = combined.astype(jnp.bfloat16)

    def drain_sp(j, none):
        e = (me + j) % experts
        remote(outgoing.at[e], arrived.at[me], go_send.at[e], go_recv.at[me], (e, t)).wait_send()
        remote(back.at[e], returned.at[me], back_send.at[e], back_recv.at[me], (e, t)).wait_send()
        return none

    lax.fori_loop(1, experts, drain_sp, 0)

    def drain_pair(at, none):
        for k in range(chunks):
            for p in range(2):
                to_partner(k, at, p).wait_send()
            pin(k, at).wait_send()
        return none

    lax.fori_loop(0, chips, drain_pair, 0)

    def drain_ring(i, none):
        for k in range(chunks):
            for d in range(2):
                for p in range(2):

                    def sent(k=k, d=d, p=p):
                        ref = rows.at[k, 0, c, :, piece[p]]
                        remote(ref, ref, ag_send.at[k, d, i, p], ag_recv.at[k, d, i, p], ahead[d]).wait_send()

                    def summed(k=k, d=d, p=p):
                        ref = rows.at[k, 0, c, :, piece[p]]
                        remote(ref, ref, rs_send.at[k, d, i, p], rs_recv.at[k, d, i, p], ahead[d]).wait_send()

                    if p == d:
                        sent()
                        summed()
                    else:
                        pl.when(i < far - 1)(sent)
                        pl.when(i > 0)(summed)
        return none

    lax.fori_loop(0, far, drain_ring, 0)


def expert_layer(stream, normed, choice, choice_weights, gate_proj, up_proj, down_proj, seq_devices, head_devices, cap):
    own_rows, width = stream.shape
    hidden = gate_proj.shape[2]
    experts, chips, chunks = seq_devices, head_devices // 2, 2
    far, block = chips // 2, seq_devices // chunks * cap
    slots = choice * SLOT_ROWS + choice_ranks(choice, experts)
    targets = jnp.arange(experts * SLOT_ROWS, dtype=jnp.int32)
    match = slots[:, :, None] == targets[None, None, :]
    select = jnp.any(match, axis=1).T.astype(jnp.bfloat16)
    weights = jnp.sum(jnp.where(match, choice_weights[:, :, None], 0.0), axis=1)
    vmem, hbm = pl.BlockSpec(memory_space=pltpu.VMEM), pl.BlockSpec(memory_space=pl.ANY)
    bf16, dma = jnp.bfloat16, pltpu.SemaphoreType.DMA
    return pl.pallas_call(
        functools.partial(expert_kernel, cap),
        out_shape=jax.ShapeDtypeStruct(stream.shape, bf16),
        in_specs=[vmem] * 4 + [hbm] * 3,
        out_specs=vmem,
        scratch_shapes=[
            pltpu.VMEM((experts, SLOT_ROWS, width), bf16),
            pltpu.VMEM((experts, SLOT_ROWS, width), bf16),
            pltpu.VMEM((chunks, chips, 2, block, width), bf16),
            pltpu.VMEM((chunks, chips, 2, block, width), bf16),
            pltpu.VMEM((chunks, chips, block, width), bf16),
            pltpu.VMEM((chunks, 2, far, block, width), bf16),
            pltpu.VMEM((experts, SLOT_ROWS, width), bf16),
            pltpu.VMEM((experts, SLOT_ROWS, width), bf16),
            pltpu.VMEM((width, hidden), bf16),
            pltpu.VMEM((width, hidden), bf16),
            pltpu.VMEM((hidden, width), bf16),
            dma((3,)),
            dma((experts,)),
            dma((experts,)),
            dma((chunks, 2, far, 2)),
            dma((chunks, 2, far, 2)),
            dma((chunks, chips, 2)),
            dma((chunks, chips, 2)),
            dma((chunks, chips)),
            dma((chunks, chips)),
            dma((chunks, 2, far, 2)),
            dma((chunks, 2, far, 2)),
            dma((experts,)),
            dma((experts,)),
        ],
        compiler_params=pltpu.CompilerParams(
            collective_id=1, has_side_effects=True, vmem_limit_bytes=56 << 20
        ),
        name="experts",
    )(stream, normed, select, weights, gate_proj, up_proj, down_proj)


def on_device(
    queries,
    keys,
    values,
    key_bias,
    head_gain,
    out_weight,
    residual,
    norm_gain,
    gate_proj,
    up_proj,
    down_proj,
    expert_choice,
    expert_weights,
):
    seq_devices, head_devices = lax.axis_size("sp"), lax.axis_size("tp")
    stream, normed = attention_layer(
        queries, keys, values, key_bias, head_gain, out_weight, residual, norm_gain
    )
    cap = 4 * queries.shape[0] // (head_devices * seq_devices)
    return expert_layer(
        stream, normed, expert_choice, expert_weights, gate_proj, up_proj, down_proj, seq_devices, head_devices, cap
    )


def solution(mesh):
    placed = (
        P("sp", "tp"),
        P("sp", "tp"),
        P("sp", "tp"),
        P("sp", "tp"),
        P("tp", None),
        P("tp", None),
        P(("sp", "tp"), None),
        P(),
        P("sp", None, "tp"),
        P("sp", None, "tp"),
        P("sp", "tp", None),
        P(("sp", "tp"), None),
        P(("sp", "tp"), None),
    )
    return jax.shard_map(
        on_device, mesh=mesh, in_specs=placed, out_specs=P(("sp", "tp"), None), check_vma=False
    )
```

```python
import functools

import jax
import jax.numpy as jnp
from jax import lax
from jax.experimental import pallas as pl
from jax.experimental.pallas import tpu as pltpu
from jax.sharding import PartitionSpec as P

epsilon = 1e-06
CHUNK = 256
MESH = pl.DeviceIdType.MESH
SLOT_ROWS = 8


def remote(src, dst, send_sem, recv_sem, device):
    return pltpu.make_async_remote_copy(
        src_ref=src, dst_ref=dst, send_sem=send_sem, recv_sem=recv_sem, device_id=device, device_id_type=MESH
    )


def attention_part(
    chips_y, loads, route, q_ref, k_ref, v_ref, bias_ref, gain_ref, w_ref, residual_ref, norm_ref, stream_ref, normed_ref,
    kv_out, q_out, kv, q_in, q_wide, gains, weights, acc, carry, att_out, att_in, part, part_out, ring_sum,
    kv_send, kv_recv, q_send, q_recv, x_send, x_recv, pair_send, pair_recv, w_send, w_recv, g_send, g_recv,
    att_send, att_recv, rs_send, rs_recv,
):
    rows, packed = q_ref.shape
    size = packed // 2
    chips_x = lax.axis_size("sp") // chips_y
    chips = lax.axis_size("tp") // 2
    width = w_ref.shape[1]
    far, half = chips // 2, width // 2
    piece = (pl.ds(0, half), pl.ds(half, half))
    me, t = lax.axis_index("sp"), lax.axis_index("tp")
    y, x, z, c = me // chips_x, me % chips_x, t // 2, t % 2

    def device(yy, xx, zz, cc):
        return (yy * chips_x + xx, 2 * zz + cc)

    def query_core(yy):
        return ((yy + 1) // 2) % 2

    partner = device(y, x, z, 1 - c)
    beside = (device(y, (x + 1) % chips_x, z, c), device(y, (x + chips_x - 1) % chips_x, z, c))
    ahead = (device(y, x, (z + 1) % chips, c), device(y, x, (z + chips - 1) % chips, c))
    barrier = pltpu.get_barrier_semaphore()
    sources = lax.axis_size("sp")

    def greet(n, none):
        pl.semaphore_signal(barrier, inc=1, device_id=((me + n) % sources, t), device_id_type=MESH)
        return none

    lax.fori_loop(1, sources, greet, 0)
    others = [device((y + dy) % chips_y, x, z, 1 - c) for dy in range(chips_y)] + list(ahead)
    for other in others:
        pl.semaphore_signal(barrier, inc=1, device_id=other, device_id_type=MESH)
    for load in loads[:5]:
        load.wait()

    offsets = bias_ref[...].astype(jnp.float32)
    for h in range(2):
        lanes = slice(h * size, (h + 1) * size)
        kv_out[h, pl.ds(0, rows)] = jnp.concatenate([k_ref[:, lanes], v_ref[:, lanes]], axis=1)
        by_row = [offsets[h : h + 1, n * packed : (n + 1) * packed] for n in range(rows // packed)]
        by_row.append(jnp.zeros((16 - rows // packed, packed), jnp.float32))
        kv_out[h, pl.ds(rows, 16)] = jnp.concatenate(by_row, axis=0).astype(jnp.bfloat16)
        q_neg = q_ref[:, lanes] * jnp.bfloat16(-(size ** -0.5))
        q_out[h] = jnp.concatenate([q_neg[: rows // 2], q_neg[rows // 2 :]], axis=1)
    kv[0, pl.ds(0, rows)] = jnp.zeros((rows, packed), jnp.bfloat16)
    kv[0, pl.ds(rows, 16)] = jnp.full((16, packed), -30000.0, jnp.bfloat16)
    gains[c] = gain_ref[...]
    pl.semaphore_wait(barrier, sources - 1 + len(others))

    at_home = (y // 2 == c) & (y % 2 == c)
    asks_self = (y // 2 == c) & (query_core(y) == c)
    for h in range(2):
        j = 2 * c + h

        @pl.when(jnp.logical_not(at_home & (j == y)))
        def _(h=h, j=j):
            remote(kv_out.at[h], kv.at[me + 1], kv_send.at[h], kv_recv.at[y // 2], device(j, x, z, y % 2)).start()

        @pl.when(at_home & (j == y))
        def _(h=h):
            pltpu.make_async_copy(kv_out.at[h], kv.at[me + 1], kv_recv.at[y // 2]).start()

    for h in range(2):
        j = 2 * c + h

        @pl.when(jnp.logical_not(asks_self & (j == y)))
        def _(h=h, j=j):
            remote(q_out.at[h], q_in.at[y // 2], q_send.at[h], q_recv.at[y // 2], device(j, x, z, query_core(y))).start()

        @pl.when(asks_self & (j == y))
        def _(h=h):
            pltpu.make_async_copy(q_out.at[h], q_in.at[y // 2], q_recv.at[y // 2]).start()

    to_w = remote(w_ref, weights.at[c], w_send.at[0], w_recv.at[0], partner)
    to_g = remote(gain_ref, gains.at[c], g_send.at[0], g_recv.at[0], partner)
    to_g.start()
    route()

    def block_at(k, xx):
        return kv.at[(c + 2 * k) * chips_x + xx + 1]

    def to_partner(k, xx):
        ref = block_at(k, xx)
        return remote(ref, ref, pair_send.at[k, xx], pair_recv.at[k, xx], partner)

    def along(d, n, k, xx):
        ref = block_at(k, xx)
        return remote(ref, ref, x_send.at[d, n], x_recv.at[d, n], beside[d])

    back_x = ((x + chips_x - 1) % chips_x, (x + 1) % chips_x)
    across = (x + 2) % chips_x
    for k in range(2):
        kept = at_home & (c + 2 * k == y)

        @pl.when(kept)
        def _(k=k):
            pltpu.make_async_copy(kv_out.at[0], block_at(k, x), kv_recv.at[k]).wait()

        @pl.when(jnp.logical_not(kept))
        def _(k=k):
            remote(kv_out.at[0], block_at(k, x), kv_send.at[0], kv_recv.at[k], partner).wait_recv()

        for d in range(2):
            along(d, k, k, x).start()
        to_partner(k, x).start()
    for load in loads[5:]:
        load.wait()
    to_w.start()
    weights[c] = w_ref[...]
    for d in range(2):
        along(d, d, d, back_x[d]).wait_recv()
        along(d, 2, d, back_x[d]).start()
        to_partner(d, back_x[d]).start()
    for d in range(2):
        along(d, 1 - d, 1 - d, back_x[d]).wait_recv()
        to_partner(1 - d, back_x[d]).start()
    for d in range(2):
        along(d, 2, d, across).wait_recv()
        to_partner(d, across).start()
    to_g.wait_recv()

    def wait_pair(n, none):
        k, xx = n // chips_x, n % chips_x
        ref = kv.at[(1 - c + 2 * k) * chips_x + xx + 1]
        remote(ref, ref, pair_send.at[k, xx], pair_recv.at[k, xx], partner).wait_recv()
        return none

    lax.fori_loop(0, 2 * chips_x, wait_pair, 0)

    row = lax.broadcasted_iota(jnp.int32, (CHUNK, CHUNK), 0)
    col = lax.broadcasted_iota(jnp.int32, (CHUNK, CHUNK), 1)
    after = (row > col).astype(jnp.bfloat16)

    def attend(slot):
        from_y = c if slot == 0 else 3 - c
        block = from_y * chips_x + x
        asked = asks_self & (from_y == y)

        @pl.when(asked)
        def _():
            pltpu.make_async_copy(q_out.at[0], q_in.at[slot], q_recv.at[slot]).wait()

        @pl.when(jnp.logical_not(asked))
        def _():
            remote(q_out.at[0], q_in.at[slot], q_send.at[0], q_recv.at[slot], partner).wait_recv()

        folded = q_in[slot]
        q_here = jnp.concatenate([folded[:, :size], folded[:, size:]], axis=0)
        q_wide[...] = jnp.concatenate([q_here, jnp.zeros_like(q_here)], axis=1)
        acc[...] = jnp.zeros_like(acc)
        carry[...] = jnp.zeros_like(carry)

        def pair(index, masked):
            older = block - 2 * index

            def part_of(place, first, length):
                return kv[older + place, pl.ds(first, length)], kv[older + place, pl.ds(rows, 16)], first // 128, length // 128

            def chunk(sources, place):
                kv_part = jnp.concatenate([s[0] for s in sources], axis=0)
                offset = jnp.concatenate(
                    [s[1][s[2] + n : s[2] + n + 1, :].astype(jnp.float32) for s in sources for n in range(s[3])], axis=1
                )
                minus = (
                    lax.dot_general(
                        q_wide[...], kv_part, (((1,), (1,)), ((), ())), preferred_element_type=jnp.float32
                    )
                    - offset
                )
                log_part = jnp.log(1.0 + jnp.exp(-jnp.abs(minus)))
                drop = jnp.minimum(minus, 0.0) - log_part
                own_log = drop - minus
                if masked:
                    q_at = lax.broadcasted_iota(jnp.int32, (rows, CHUNK), 0) + (rows - place)
                    earlier = lax.broadcasted_iota(jnp.int32, (rows, CHUNK), 1) < q_at
                    drop = jnp.where(earlier, drop, 0.0)
                suffix = jnp.dot(drop.astype(jnp.bfloat16), after, preferred_element_type=jnp.float32)
                within = jnp.exp(own_log + suffix)
                if masked:
                    within = jnp.where(earlier, within, 0.0)
                product = jnp.dot(within.astype(jnp.bfloat16), kv_part, preferred_element_type=jnp.float32)
                now = carry[...]
                acc[...] += jnp.exp(now) * product
                carry[...] = now + (suffix[:, :1] + drop[:, :1])

            chunk([part_of(1, 128, 256)], 512)
            chunk([part_of(0, 256, 128), part_of(1, 0, 128)], 256)
            chunk([part_of(0, 0, 256)], 0)

        pair(0, True)

        def body(index, none):
            pair(index, False)
            return none

        lax.fori_loop(1, (block + 2) // 2, body, 0)
        mixture = acc[...][:, size:]
        scaled = mixture * lax.rsqrt(jnp.mean(mixture * mixture, axis=-1, keepdims=True) + epsilon)
        scaled = scaled * gains[y // 2, pl.ds(y % 2, 1), :]
        by_owner = scaled.reshape(chips, 2, rows // (2 * chips), size)
        for p in range(2):
            att_out[slot, p] = by_owner[:, p].astype(jnp.bfloat16)
            stays = (from_y == y) & (p == c)

            @pl.when(stays)
            def _(p=p):
                pltpu.make_async_copy(att_out.at[slot, p], att_in.at[y], att_recv.at[y]).start()

            @pl.when(jnp.logical_not(stays))
            def _(p=p):
                send_att(slot, p, from_y).start()

    def send_att(slot, p, from_y):
        return remote(
            att_out.at[slot, p], att_in.at[y], att_send.at[slot, p], att_recv.at[y], device(from_y, x, z, p)
        )

    attend(1)
    attend(0)

    for j in range(chips_y):
        stayed = (j == y) & (query_core(y) == c)

        @pl.when(stayed)
        def _(j=j):
            pltpu.make_async_copy(att_out.at[0, 0], att_in.at[j], att_recv.at[j]).wait()

        @pl.when(jnp.logical_not(stayed))
        def _(j=j):
            remote(att_out.at[0, 0], att_in.at[j], att_send.at[0, 0], att_recv.at[j], partner).wait_recv()

    to_w.wait_recv()
    heads = [att_in[j].astype(jnp.float32).reshape(rows // 2, size) for j in range(chips_y)]
    merged = jnp.concatenate(heads, axis=1).astype(jnp.bfloat16)
    share = jnp.dot(merged, weights[...].reshape(2 * packed, width), preferred_element_type=jnp.float32)
    part[...] = share.reshape(part.shape)

    def from_sum(d, i, p):
        ref = ring_sum.at[d, i, :, piece[p]]
        return remote(ref, ref, rs_send.at[d, i, p], rs_recv.at[d, i, p], ahead[d])

    for i in range(far):
        for order in range(2):
            for d in range(2):
                p = d if order == 0 else 1 - d
                if i == 0 and p != d:
                    continue
                at = ((z + (far - i)) if d == 0 else (z - (far - i) + chips)) % chips
                total = part[at, :, piece[p]]
                if i > 1 or (i == 1 and p == d):
                    from_sum(d, i - 1, p).wait_recv()
                    total = total + ring_sum[d, i - 1, :, piece[p]].astype(jnp.float32)
                part_out[d, i, :, piece[p]] = total.astype(jnp.bfloat16)
                remote(
                    part_out.at[d, i, :, piece[p]],
                    ring_sum.at[d, i, :, piece[p]],
                    rs_send.at[d, i, p],
                    rs_recv.at[d, i, p],
                    ahead[d],
                ).start()
    for d in range(2):
        for p in range(2):
            from_sum(d, far - 1, p).wait_recv()
    projected = part[z] + ring_sum[0, far - 1].astype(jnp.float32) + ring_sum[1, far - 1].astype(jnp.float32)
    stream = (residual_ref[...].astype(jnp.float32) + projected).astype(jnp.bfloat16)
    stream_ref[...] = stream
    wide = stream.astype(jnp.float32)
    normed_ref[...] = (
        wide * lax.rsqrt(jnp.mean(wide * wide, axis=-1, keepdims=True) + epsilon) * norm_ref[...]
    ).astype(jnp.bfloat16)

    for h in range(2):
        j = 2 * c + h

        @pl.when(jnp.logical_not(at_home & (j == y)))
        def _(h=h):
            remote(kv_out.at[h], kv.at[0], kv_send.at[h], kv_recv.at[0], partner).wait_send()

        @pl.when(jnp.logical_not(asks_self & (j == y)))
        def _(h=h):
            remote(q_out.at[h], q_in.at[0], q_send.at[h], q_recv.at[0], partner).wait_send()

    to_w.wait_send()
    to_g.wait_send()
    for d in range(2):
        for n in range(3):
            along(d, n, 0, x).wait_send()

    def drain_pair(n, none):
        to_partner(n // chips_x, n % chips_x).wait_send()
        return none

    lax.fori_loop(0, 2 * chips_x, drain_pair, 0)
    for slot in range(2):
        from_y = c if slot == 0 else 3 - c
        for p in range(2):

            @pl.when(jnp.logical_not((from_y == y) & (p == c)))
            def _(slot=slot, p=p, from_y=from_y):
                send_att(slot, p, from_y).wait_send()

    for d in range(2):
        for i in range(far):
            for p in range(2):
                if i > 0 or p == d:
                    from_sum(d, i, p).wait_send()


def expert_part(
    cap, loads, gate_w, up_w, down_w, stream_ref, normed_ref, select_ref, weight_ref, out_ref,
    outgoing, arrived, rows, part, partner_part, ring_sum, back, returned,
    go_send, go_recv, ag_send, ag_recv, pair_send, pair_recv, pin_send, pin_recv,
    rs_send, rs_recv, back_send, back_recv,
):
    experts, _, width = outgoing.shape
    chunks, chips, _, block, _ = rows.shape
    far, half, per = chips // 2, width // 2, experts // chunks
    me, t = lax.axis_index("sp"), lax.axis_index("tp")
    z, c = t // 2, t % 2
    partner = (me, 2 * z + (1 - c))
    ahead = ((me, 2 * ((z + 1) % chips) + c), (me, 2 * ((z + chips - 1) % chips) + c))
    piece = (pl.ds(0, half), pl.ds(half, half))

    chosen = jnp.dot(select_ref[...], normed_ref[...], preferred_element_type=jnp.float32)
    outgoing[...] = chosen.reshape(experts, SLOT_ROWS, width).astype(jnp.bfloat16)
    for k in range(chunks):
        for d in range(2):
            ring_sum[k, d, 0, :, piece[1 - d]] = jnp.zeros((block, half), jnp.bfloat16)

    def go(src, dst, source_id, device):
        return remote(src, dst, go_send.at[source_id], go_recv.at[source_id], device)

    def send_go(j, none):
        e = (me + j) % experts
        remote(outgoing.at[e], arrived.at[me], go_send.at[e], go_recv.at[me], (e, t)).start()
        return none

    lax.fori_loop(1, experts, send_go, 0)
    own = pltpu.make_async_copy(outgoing.at[me], arrived.at[me], go_recv.at[me])
    own.start()

    def take_arrived(k):
        def wait_one(j, none):
            s = k * per + j

            @pl.when(s == me)
            def _():
                own.wait()

            @pl.when(s != me)
            def _():
                remote(outgoing.at[s], arrived.at[s], go_send.at[s], go_recv.at[s], (s, t)).wait_recv()

            return none

        lax.fori_loop(0, per, wait_one, 0)
        row = lax.broadcasted_iota(jnp.int32, (block, per * SLOT_ROWS), 0)
        col = lax.broadcasted_iota(jnp.int32, (block, per * SLOT_ROWS), 1)
        pick = (col == row // cap * SLOT_ROWS + row % cap).astype(jnp.bfloat16)
        padded = arrived[pl.ds(k * per, per)].astype(jnp.float32).reshape(per * SLOT_ROWS, width)
        rows[k, z, c] = jnp.dot(
            pick, padded.astype(jnp.bfloat16), preferred_element_type=jnp.float32
        ).astype(jnp.bfloat16)

    def ring_rows(k, d, i, p, device):
        at = (z - i if d == 0 else z + i) % chips if isinstance(i, int) else lax.rem((z - i if d == 0 else z + i) + chips, chips)
        ref = rows.at[k, at, c, :, piece[p]]
        return remote(ref, ref, ag_send.at[k, d, i, p], ag_recv.at[k, d, i, p], device)

    def to_partner(k, at, p):
        ref = rows.at[k, at, c, :, piece[p]]
        return remote(ref, ref, pair_send.at[k, at, p], pair_recv.at[k, at, p], partner)

    def start_own(k):
        for p in range(2):
            for d in range(2):
                ring_rows(k, d, 0, p if d == 0 else 1 - p, ahead[d]).start()
        for p in range(2):
            to_partner(k, z, p).start()

    def from_ring(k, d, i, p):
        at = lax.rem((z - i - 1 if d == 0 else z + i + 1) + chips, chips)
        ref = rows.at[k, at, c, :, piece[p]]
        return at, remote(ref, ref, ag_send.at[k, d, i, p], ag_recv.at[k, d, i, p], ahead[d])

    def gather_step(k, i):
        for order in range(2):
            for d in range(2):
                p = d if order == 0 else 1 - d

                def handle(d=d, p=p, last=(order == 1)):
                    at, copy = from_ring(k, d, i, p)
                    copy.wait_recv()

                    @pl.when(i + 1 < (far - 1 if last else far))
                    def _():
                        ref = rows.at[k, at, c, :, piece[p]]
                        remote(ref, ref, ag_send.at[k, d, i + 1, p], ag_recv.at[k, d, i + 1, p], ahead[d]).start()

                    to_partner(k, at, p).start()

                if order == 0:
                    handle()
                else:
                    pl.when(i < far - 1)(handle)

    def wait_partner_rows(k):
        def wait_one(at, none):
            for p in range(2):
                ref = rows.at[k, at, 1 - c, :, piece[p]]
                remote(ref, ref, pair_send.at[k, at, p], pair_recv.at[k, at, p], partner).wait_recv()
            return none

        lax.fori_loop(0, chips, wait_one, 0)

    group = chips // far

    def experts_on(k, i):
        at = pl.ds(i * group, group)
        x = rows[k, at].reshape(group * 2 * block, width)
        across = (((1,), (1,)), ((), ()))
        gate = lax.dot_general(x, gate_w[...], across, preferred_element_type=jnp.float32)
        up = lax.dot_general(x, up_w[...], across, preferred_element_type=jnp.float32)
        hidden = (gate / (1.0 + jnp.exp(-gate)) * up).astype(jnp.bfloat16)
        product = jnp.dot(hidden, down_w[...], preferred_element_type=jnp.float32)
        part[k, at] = product.astype(jnp.bfloat16).reshape(group, 2, block, width)
        for j in range(group):
            pin(k, i * group + j).start()

    def pin(k, at):
        return remote(
            part.at[k, at, 1 - c], partner_part.at[k, at], pin_send.at[k, at], pin_recv.at[k, at], partner
        )

    def wait_pins(k):
        def wait_one(at, none):
            pin(k, at).wait_recv()
            return none

        lax.fori_loop(0, chips, wait_one, 0)

    def ring_step(k, i):
        for order in range(2):
            for d in range(2):
                p = d if order == 0 else 1 - d

                def handle(d=d, p=p, first=(order == 0)):
                    at = lax.rem((z + (far - i) if d == 0 else z - (far - i)) + chips, chips)
                    own_sum = part[k, at, c, :, piece[p]].astype(jnp.float32) + partner_part[
                        k, at, :, piece[p]
                    ].astype(jnp.float32)

                    @pl.when(i == 0)
                    def _():
                        part[k, at, c, :, piece[p]] = own_sum.astype(jnp.bfloat16)

                    @pl.when(i > 0)
                    def _():
                        before = jnp.maximum(i - 1, 0)
                        if first:
                            from_sum(k, d, before, p).wait_recv()
                        else:
                            pl.when(i > 1)(lambda: from_sum(k, d, before, p).wait_recv())
                        total = own_sum + ring_sum[k, d, before, :, piece[p]].astype(jnp.float32)
                        part[k, at, c, :, piece[p]] = total.astype(jnp.bfloat16)

                    remote(
                        part.at[k, at, c, :, piece[p]],
                        ring_sum.at[k, d, i, :, piece[p]],
                        rs_send.at[k, d, i, p],
                        rs_recv.at[k, d, i, p],
                        ahead[d],
                    ).start()

                if order == 0:
                    handle()
                else:
                    pl.when(i > 0)(handle)

    def from_sum(k, d, i, p):
        ref = ring_sum.at[k, d, i, :, piece[p]]
        return remote(ref, ref, rs_send.at[k, d, i, p], rs_recv.at[k, d, i, p], ahead[d])

    def send_back(k):
        for p in range(2):
            for d in range(2):
                from_sum(k, d, far - 1, p).wait_recv()
        total = (
            part[k, z, c].astype(jnp.float32)
            + partner_part[k, z].astype(jnp.float32)
            + ring_sum[k, 0, far - 1].astype(jnp.float32)
            + ring_sum[k, 1, far - 1].astype(jnp.float32)
        ).astype(jnp.bfloat16)
        row = lax.broadcasted_iota(jnp.int32, (per * SLOT_ROWS, block), 0)
        col = lax.broadcasted_iota(jnp.int32, (per * SLOT_ROWS, block), 1)
        spread = ((row % SLOT_ROWS < cap) & (col == row // SLOT_ROWS * cap + row % SLOT_ROWS)).astype(jnp.bfloat16)
        back[pl.ds(k * per, per)] = (
            jnp.dot(spread, total, preferred_element_type=jnp.float32)
            .reshape(per, SLOT_ROWS, width)
            .astype(jnp.bfloat16)
        )

        def send_one(j, none):
            s = k * per + j

            @pl.when(s != me)
            def _():
                remote(back.at[s], returned.at[me], back_send.at[s], back_recv.at[me], (s, t)).start()

            @pl.when(s == me)
            def _():
                pltpu.make_async_copy(back.at[s], returned.at[me], back_recv.at[me]).start()

            return none

        lax.fori_loop(0, per, send_one, 0)

    def steps(body):
        def one(i, none):
            body(i)
            return none

        lax.fori_loop(0, far, one, 0)

    take_arrived(0)
    start_own(0)
    take_arrived(1)
    steps(lambda i: gather_step(0, i))
    start_own(1)
    for load in loads:
        load.wait()
    wait_partner_rows(0)

    def gather_and_compute(i):
        gather_step(1, i)
        experts_on(0, i)

    steps(gather_and_compute)
    wait_partner_rows(1)
    wait_pins(0)

    def sum_and_compute(i):
        ring_step(0, i)
        experts_on(1, i)

    steps(sum_and_compute)
    wait_pins(1)
    steps(lambda i: (pl.when(i == 1)(lambda: send_back(0)), ring_step(1, i)))
    send_back(1)

    def wait_back(e, none):
        @pl.when(e == me)
        def _():
            pltpu.make_async_copy(back.at[e], returned.at[e], back_recv.at[e]).wait()

        @pl.when(e != me)
        def _():
            remote(back.at[e], returned.at[e], back_send.at[e], back_recv.at[e], (e, t)).wait_recv()

        return none

    lax.fori_loop(0, experts, wait_back, 0)
    picked = returned[...].astype(jnp.float32).reshape(experts * SLOT_ROWS, width).astype(jnp.bfloat16)
    combined = stream_ref[...].astype(jnp.float32)
    for n in reversed(range(3)):
        combined = combined + lax.dot_general(
            weight_ref[n], picked, (((0,), (0,)), ((), ())), preferred_element_type=jnp.float32
        )
    out_ref[...] = combined.astype(jnp.bfloat16)

    def drain_sp(j, none):
        e = (me + j) % experts
        remote(outgoing.at[e], arrived.at[me], go_send.at[e], go_recv.at[me], (e, t)).wait_send()
        remote(back.at[e], returned.at[me], back_send.at[e], back_recv.at[me], (e, t)).wait_send()
        return none

    lax.fori_loop(1, experts, drain_sp, 0)

    def drain_pair(at, none):
        for k in range(chunks):
            for p in range(2):
                to_partner(k, at, p).wait_send()
            pin(k, at).wait_send()
        return none

    lax.fori_loop(0, chips, drain_pair, 0)

    def drain_ring(i, none):
        for k in range(chunks):
            for d in range(2):
                for p in range(2):

                    def sent(k=k, d=d, p=p):
                        ref = rows.at[k, 0, c, :, piece[p]]
                        remote(ref, ref, ag_send.at[k, d, i, p], ag_recv.at[k, d, i, p], ahead[d]).wait_send()

                    def summed(k=k, d=d, p=p):
                        ref = rows.at[k, 0, c, :, piece[p]]
                        remote(ref, ref, rs_send.at[k, d, i, p], rs_recv.at[k, d, i, p], ahead[d]).wait_send()

                    if p == d:
                        sent()
                        summed()
                    else:
                        pl.when(i < far - 1)(sent)
                        pl.when(i > 0)(summed)
        return none

    lax.fori_loop(0, far, drain_ring, 0)


def layer_kernel(
    chips_y, cap, q_hbm, k_hbm, v_hbm, bias_hbm, gain_hbm, w_hbm, residual_hbm, norm_hbm, choice_hbm, share_hbm,
    gate_hbm, up_hbm, down_hbm, out_ref, q, k, v, bias, gain, w, residual, norm, choice, share, gate_w, up_w, down_w,
    load_sem, stream, normed, select, weight, *scratch,
):
    sources = (q_hbm, k_hbm, v_hbm, bias_hbm, gain_hbm, w_hbm, residual_hbm, norm_hbm, choice_hbm, share_hbm)
    sources += (gate_hbm.at[0], up_hbm.at[0], down_hbm.at[0])
    places = (q, k, v, bias, gain, w, residual, norm, choice, share, gate_w, up_w, down_w)
    loads = [pltpu.make_async_copy(src, dst, load_sem.at[i]) for i, (src, dst) in enumerate(zip(sources, places))]
    for load in loads:
        load.start()

    def route():
        for load in loads[8:10]:
            load.wait()
        slots, own_rows = select.shape
        slot = lax.broadcasted_iota(jnp.int32, (slots, own_rows), 0)
        expert, place = slot // SLOT_ROWS, slot % SLOT_ROWS
        first = choice[0:1, :] == expert
        named = first | (choice[1:2, :] == expert)
        earlier = lax.broadcasted_iota(jnp.int32, (own_rows, own_rows), 0) < lax.broadcasted_iota(
            jnp.int32, (own_rows, own_rows), 1
        )
        before = jnp.dot(
            named.astype(jnp.bfloat16), earlier.astype(jnp.bfloat16), preferred_element_type=jnp.float32
        )
        chosen = named & (before.astype(jnp.int32) == place)
        select[...] = chosen.astype(jnp.bfloat16)
        rest = jnp.where(chosen, jnp.where(first, share[0:1, :], share[1:2, :]), 0.0)
        for n in range(3):
            term = rest.astype(jnp.bfloat16)
            weight[n] = term
            rest = rest - term.astype(jnp.float32)

    attention_part(
        chips_y, loads[:8], route, q, k, v, bias, gain, w, residual, norm, stream, normed, *scratch[:ATTENTION_SCRATCH]
    )
    expert_part(cap, loads[10:], gate_w, up_w, down_w, stream, normed, select, weight, out_ref, *scratch[ATTENTION_SCRATCH:])


ATTENTION_SCRATCH = 30


def layer(
    queries, keys, values, key_bias, head_gain, out_weight, residual, norm_gain, gate_proj, up_proj, down_proj,
    expert_choice, expert_weights,
):
    rows, packed = queries.shape
    size, width, hidden = head_gain.shape[1], out_weight.shape[1], gate_proj.shape[2]
    blocks, chips, chips_y, chunks = lax.axis_size("sp"), lax.axis_size("tp") // 2, 4, 2
    chips_x, far, own = blocks // chips_y, chips // 2, residual.shape[0]
    cap = 4 * own // blocks
    block, slots = blocks // chunks * cap, blocks * SLOT_ROWS
    bf16, f32, dma = jnp.bfloat16, jnp.float32, pltpu.SemaphoreType.DMA
    arguments = (
        queries, keys, values, key_bias.T, head_gain, out_weight, residual, norm_gain.reshape(1, -1),
        expert_choice.T, expert_weights.T, gate_proj.swapaxes(1, 2), up_proj.swapaxes(1, 2), down_proj,
    )
    scratch = [pltpu.VMEM(a.shape[-2:], a.dtype) for a in arguments]
    scratch += [
        dma((len(arguments),)),
        pltpu.VMEM((own, width), bf16),
        pltpu.VMEM((own, width), bf16),
        pltpu.VMEM((slots, own), bf16),
        pltpu.VMEM((3, slots, own), bf16),
    ]
    attention_scratch = [
        pltpu.VMEM((2, rows + 16, packed), bf16),
        pltpu.VMEM((2, rows // 2, packed), bf16),
        pltpu.VMEM((blocks + 1, rows + 16, packed), bf16),
        pltpu.VMEM((2, rows // 2, packed), bf16),
        pltpu.VMEM((rows, packed), bf16),
        pltpu.VMEM((2, 2, size), f32),
        pltpu.VMEM((2, packed, width), bf16),
        pltpu.VMEM((rows, packed), f32),
        pltpu.VMEM((rows, 1), f32),
        pltpu.VMEM((2, 2, chips, own, size), bf16),
        pltpu.VMEM((chips_y, chips, own, size), bf16),
        pltpu.VMEM((chips, own, width), f32),
        pltpu.VMEM((2, far, own, width), bf16),
        pltpu.VMEM((2, far, own, width), bf16),
        dma((2,)),
        dma((2,)),
        dma((2,)),
        dma((2,)),
        dma((2, 3)),
        dma((2, 3)),
        dma((2, chips_x)),
        dma((2, chips_x)),
        dma((1,)),
        dma((1,)),
        dma((1,)),
        dma((1,)),
        dma((2, 2)),
        dma((chips_y,)),
        dma((2, far, 2)),
        dma((2, far, 2)),
    ]
    expert_scratch = [
        pltpu.VMEM((blocks, SLOT_ROWS, width), bf16),
        pltpu.VMEM((blocks, SLOT_ROWS, width), bf16),
        pltpu.VMEM((chunks, chips, 2, block, width), bf16),
        pltpu.VMEM((chunks, chips, 2, block, width), bf16),
        pltpu.VMEM((chunks, chips, block, width), bf16),
        pltpu.VMEM((chunks, 2, far, block, width), bf16),
        pltpu.VMEM((blocks, SLOT_ROWS, width), bf16),
        pltpu.VMEM((blocks, SLOT_ROWS, width), bf16),
        dma((blocks,)),
        dma((blocks,)),
        dma((chunks, 2, far, 2)),
        dma((chunks, 2, far, 2)),
        dma((chunks, chips, 2)),
        dma((chunks, chips, 2)),
        dma((chunks, chips)),
        dma((chunks, chips)),
        dma((chunks, 2, far, 2)),
        dma((chunks, 2, far, 2)),
        dma((blocks,)),
        dma((blocks,)),
    ]
    assert len(attention_scratch) == ATTENTION_SCRATCH
    return pl.pallas_call(
        functools.partial(layer_kernel, chips_y, cap),
        out_shape=jax.ShapeDtypeStruct(residual.shape, bf16),
        in_specs=[pl.BlockSpec(memory_space=pl.ANY)] * len(arguments),
        out_specs=pl.BlockSpec(memory_space=pltpu.VMEM),
        scratch_shapes=scratch + attention_scratch + expert_scratch,
        compiler_params=pltpu.CompilerParams(collective_id=1, has_side_effects=True, vmem_limit_bytes=60 << 20),
        name="layer",
    )(*arguments)


def solution(mesh):
    placed = (
        P("sp", "tp"),
        P("sp", "tp"),
        P("sp", "tp"),
        P("sp", "tp"),
        P("tp", None),
        P("tp", None),
        P(("sp", "tp"), None),
        P(),
        P("sp", None, "tp"),
        P("sp", None, "tp"),
        P("sp", "tp", None),
        P(("sp", "tp"), None),
        P(("sp", "tp"), None),
    )
    return jax.shard_map(
        layer, mesh=mesh, in_specs=placed, out_specs=P(("sp", "tp"), None), check_vma=False
    )
```

```python
import functools

import jax
import jax.numpy as jnp
from jax import lax
from jax.experimental import pallas as pl
from jax.experimental.pallas import tpu as pltpu
from jax.sharding import PartitionSpec as P

epsilon = 1e-06
CHUNK = 256
MESH = pl.DeviceIdType.MESH
SLOT_ROWS = 8


def remote(src, dst, send_sem, recv_sem, device):
    return pltpu.make_async_remote_copy(
        src_ref=src, dst_ref=dst, send_sem=send_sem, recv_sem=recv_sem, device_id=device, device_id_type=MESH
    )


def attention_part(
    chips_y, loads, route, q_ref, k_ref, v_ref, bias_ref, gain_ref, w_ref, residual_ref, norm_ref, stream_ref, normed_ref,
    kv_out, q_out, kv, q_in, q_wide, gains, weights, acc, carry, early, early_carry, att_out, att_in, part, part_out, ring_sum,
    kv_send, kv_recv, q_send, q_recv, pair_send, pair_recv, w_send, w_recv, g_send, g_recv,
    att_send, att_recv, rs_send, rs_recv,
):
    rows, packed = q_ref.shape
    size = packed // 2
    chips_x = lax.axis_size("sp") // chips_y
    chips = lax.axis_size("tp") // 2
    width = w_ref.shape[1]
    far, half = chips // 2, width // 2
    quarter = [pl.ds(n * half // 2, half // 2) for n in range(4)]
    me, t = lax.axis_index("sp"), lax.axis_index("tp")
    y, x, z, c = me // chips_x, me % chips_x, t // 2, t % 2

    def device(yy, xx, zz, cc):
        return (yy * chips_x + xx, 2 * zz + cc)

    def query_core(yy):
        return ((yy + 1) // 2) % 2

    partner = device(y, x, z, 1 - c)
    ahead = (device(y, x, (z + 1) % chips, c), device(y, x, (z + chips - 1) % chips, c))
    barrier = pltpu.get_barrier_semaphore()
    sources = lax.axis_size("sp")

    def greet(n, none):
        pl.semaphore_signal(barrier, inc=1, device_id=((me + n) % sources, t), device_id_type=MESH)
        return none

    lax.fori_loop(1, sources, greet, 0)
    others = [device((y + dy) % chips_y, x, z, 1 - c) for dy in range(chips_y)] + list(ahead)
    for other in others:
        pl.semaphore_signal(barrier, inc=1, device_id=other, device_id_type=MESH)
    for load in loads[:5]:
        load.wait()

    offsets = bias_ref[...].astype(jnp.float32)
    for h in range(2):
        lanes = slice(h * size, (h + 1) * size)
        kv_out[h, pl.ds(0, rows)] = jnp.concatenate([k_ref[:, lanes], v_ref[:, lanes]], axis=1)
        by_row = [offsets[h : h + 1, n * packed : (n + 1) * packed] for n in range(rows // packed)]
        by_row.append(jnp.zeros((16 - rows // packed, packed), jnp.float32))
        kv_out[h, pl.ds(rows, 16)] = jnp.concatenate(by_row, axis=0).astype(jnp.bfloat16)
        q_neg = q_ref[:, lanes] * jnp.bfloat16(-(size ** -0.5))
        q_out[h] = jnp.concatenate([q_neg[: rows // 2], q_neg[rows // 2 :]], axis=1)
    gains[c] = gain_ref[...]
    pl.semaphore_wait(barrier, sources - 1 + len(others))

    keeper = y // 2 == c
    asks_self = keeper & (query_core(y) == c)
    side, base = x % 2, x // 2 * 2
    other = (base + 2) % chips_x
    columns = (x, base + 1 - side, other + 1 - side, other + side)

    def to_column(h, n):
        return remote(
            kv_out.at[h], kv.at[me], kv_send.at[h, n], kv_recv.at[me], device(2 * c + h, columns[n], z, c)
        )

    for n in range(4):
        for h in range(2):
            if n > 0:
                to_column(h, n).start()
            else:
                pl.when(jnp.logical_not(2 * c + h == y))(lambda h=h: to_column(h, 0).start())

                @pl.when(2 * c + h == y)
                def _(h=h):
                    pltpu.make_async_copy(kv_out.at[h], kv.at[me], kv_recv.at[me]).start()

    for h in range(2):
        j = 2 * c + h

        @pl.when(jnp.logical_not(asks_self & (j == y)))
        def _(h=h, j=j):
            remote(q_out.at[h], q_in.at[y // 2], q_send.at[h], q_recv.at[y // 2], device(j, x, z, query_core(y))).start()

        @pl.when(asks_self & (j == y))
        def _(h=h):
            pltpu.make_async_copy(q_out.at[h], q_in.at[y // 2], q_recv.at[y // 2]).start()

    to_w = remote(w_ref, weights.at[c], w_send.at[0], w_recv.at[0], partner)
    to_g = remote(gain_ref, gains.at[c], g_send.at[0], g_recv.at[0], partner)
    to_g.start()
    route()

    def to_partner(s):
        return remote(kv.at[s], kv.at[s], pair_send.at[s], pair_recv.at[s], partner)

    def arrive(column):
        def one(yy, none):
            s = yy * chips_x + column

            @pl.when(keeper & (s == me))
            def _():
                pltpu.make_async_copy(kv_out.at[0], kv.at[s], kv_recv.at[s]).wait()

            @pl.when(keeper & (s != me))
            def _():
                remote(kv_out.at[0], kv.at[s], kv_send.at[0, 1], kv_recv.at[s], partner).wait_recv()

            pl.when(keeper)(lambda: to_partner(s).start())
            return none

        lax.fori_loop(0, chips_y, one, 0)

    def handed(column):
        def one(yy, none):
            pl.when(jnp.logical_not(keeper))(lambda: to_partner(yy * chips_x + column).wait_recv())
            return none

        lax.fori_loop(0, chips_y, one, 0)

    arrive(columns[0])
    arrive(columns[1])
    for load in loads[5:]:
        load.wait()
    to_w.start()
    weights[c] = w_ref[...]
    handed(columns[0])
    handed(columns[1])

    row = lax.broadcasted_iota(jnp.int32, (CHUNK, CHUNK), 0)
    col = lax.broadcasted_iota(jnp.int32, (CHUNK, CHUNK), 1)
    after = (row > col).astype(jnp.bfloat16)

    def pair_of_blocks(slot, older, masked, shift=0):
        def part_of(place, first, length):
            return kv[older + place, pl.ds(first, length)], kv[older + place, pl.ds(rows, 16)], first // 128, length // 128

        def chunk(sources, place):
            kv_part = jnp.concatenate([s[0] for s in sources], axis=0)
            offset = jnp.concatenate(
                [s[1][s[2] + n : s[2] + n + 1, :].astype(jnp.float32) for s in sources for n in range(s[3])], axis=1
            )
            minus = (
                lax.dot_general(
                    q_wide[slot], kv_part, (((1,), (1,)), ((), ())), preferred_element_type=jnp.float32
                )
                - offset
            )
            log_part = jnp.log(1.0 + jnp.exp(-jnp.abs(minus)))
            drop = jnp.minimum(minus, 0.0) - log_part
            own_log = drop - minus
            if masked:
                q_at = lax.broadcasted_iota(jnp.int32, (rows, CHUNK), 0) + (shift - place)
                earlier = lax.broadcasted_iota(jnp.int32, (rows, CHUNK), 1) < q_at
                drop = jnp.where(earlier, drop, 0.0)
            suffix = jnp.dot(drop.astype(jnp.bfloat16), after, preferred_element_type=jnp.float32)
            within = jnp.exp(own_log + suffix)
            if masked:
                within = jnp.where(earlier, within, 0.0)
            product = jnp.dot(within.astype(jnp.bfloat16), kv_part, preferred_element_type=jnp.float32)
            now = carry[...]
            acc[...] += jnp.exp(now) * product
            carry[...] = now + (suffix[:, :1] + drop[:, :1])

        chunk([part_of(1, 128, 256)], 512)
        chunk([part_of(0, 256, 128), part_of(1, 0, 128)], 256)
        chunk([part_of(0, 0, 256)], 0)

    def query_row(slot):
        return c if slot == 0 else 3 - c

    def begin(slot):
        from_y = query_row(slot)
        asked = asks_self & (from_y == y)

        @pl.when(asked)
        def _():
            pltpu.make_async_copy(q_out.at[0], q_in.at[slot], q_recv.at[slot]).wait()

        @pl.when(jnp.logical_not(asked))
        def _():
            remote(q_out.at[0], q_in.at[slot], q_send.at[0], q_recv.at[slot], partner).wait_recv()

        folded = q_in[slot]
        q_here = jnp.concatenate([folded[:, :size], folded[:, size:]], axis=0)
        q_wide[slot] = jnp.concatenate([q_here, jnp.zeros_like(q_here)], axis=1)

        def one(yy, masked):
            acc[...] = jnp.zeros_like(acc)
            carry[...] = jnp.zeros_like(carry)
            pair_of_blocks(slot, yy * chips_x + base, masked, side * rows)
            early[slot, yy] = acc[...]
            early_carry[slot, yy] = carry[...]

        def body(yy, none):
            one(yy, False)
            return none

        one(from_y, True)
        lax.fori_loop(0, from_y, body, 0)

    def attend(slot):
        from_y = query_row(slot)
        acc[...] = jnp.zeros_like(acc)
        carry[...] = jnp.zeros_like(carry)
        newest = from_y - (1 - base // 2)

        def body(n, none):
            now = carry[...]
            acc[...] += jnp.exp(now) * early[slot, from_y - n]
            carry[...] = now + early_carry[slot, from_y - n]

            @pl.when(n <= newest)
            def _():
                pair_of_blocks(slot, (newest - n) * chips_x + other, False)

            return none

        lax.fori_loop(0, from_y + 1, body, 0)
        mixture = acc[...][:, size:]
        scaled = mixture * lax.rsqrt(jnp.mean(mixture * mixture, axis=-1, keepdims=True) + epsilon)
        scaled = scaled * gains[y // 2, pl.ds(y % 2, 1), :]
        by_owner = scaled.reshape(chips, 2, rows // (2 * chips), size)
        for p in range(2):
            att_out[slot, p] = by_owner[:, p].astype(jnp.bfloat16)
            stays = (from_y == y) & (p == c)

            @pl.when(stays)
            def _(p=p):
                pltpu.make_async_copy(att_out.at[slot, p], att_in.at[y], att_recv.at[y]).start()

            @pl.when(jnp.logical_not(stays))
            def _(p=p):
                send_att(slot, p, from_y).start()

    def send_att(slot, p, from_y):
        return remote(
            att_out.at[slot, p], att_in.at[y], att_send.at[slot, p], att_recv.at[y], device(from_y, x, z, p)
        )

    begin(1)
    arrive(columns[2])
    arrive(columns[3])
    begin(0)
    handed(columns[2])
    handed(columns[3])
    to_g.wait_recv()
    attend(1)
    attend(0)

    for j in range(chips_y):
        stayed = (j == y) & (query_core(y) == c)

        @pl.when(stayed)
        def _(j=j):
            pltpu.make_async_copy(att_out.at[0, 0], att_in.at[j], att_recv.at[j]).wait()

        @pl.when(jnp.logical_not(stayed))
        def _(j=j):
            remote(att_out.at[0, 0], att_in.at[j], att_send.at[0, 0], att_recv.at[j], partner).wait_recv()

    to_w.wait_recv()
    heads = [att_in[j].astype(jnp.float32).reshape(rows // 2, size) for j in range(chips_y)]
    merged = jnp.concatenate(heads, axis=1).astype(jnp.bfloat16)
    share = jnp.dot(merged, weights[...].reshape(2 * packed, width), preferred_element_type=jnp.float32)
    part[...] = share.reshape(part.shape)

    def from_sum(d, i, p):
        ref = ring_sum.at[d, i, :, quarter[p]]
        return remote(ref, ref, rs_send.at[d, i, p], rs_recv.at[d, i, p], ahead[d])

    for i in range(far):
        for order in range(4 if i else 2):
            for d in range(2):
                p = order if d == 0 else (order + 2) % 4
                at = ((z + (far - i)) if d == 0 else (z - (far - i) + chips)) % chips
                total = part[at, :, quarter[p]]
                if i > 1 or (i == 1 and order < 2):
                    from_sum(d, i - 1, p).wait_recv()
                    total = total + ring_sum[d, i - 1, :, quarter[p]].astype(jnp.float32)
                part_out[d, i, :, quarter[p]] = total.astype(jnp.bfloat16)
                remote(
                    part_out.at[d, i, :, quarter[p]],
                    ring_sum.at[d, i, :, quarter[p]],
                    rs_send.at[d, i, p],
                    rs_recv.at[d, i, p],
                    ahead[d],
                ).start()
    for d in range(2):
        for p in range(4):
            from_sum(d, far - 1, p).wait_recv()
    projected = part[z] + ring_sum[0, far - 1].astype(jnp.float32) + ring_sum[1, far - 1].astype(jnp.float32)
    stream = (residual_ref[...].astype(jnp.float32) + projected).astype(jnp.bfloat16)
    stream_ref[...] = stream
    wide = stream.astype(jnp.float32)
    normed_ref[...] = (
        wide * lax.rsqrt(jnp.mean(wide * wide, axis=-1, keepdims=True) + epsilon) * norm_ref[...]
    ).astype(jnp.bfloat16)

    for h in range(2):
        j = 2 * c + h

        pl.when(jnp.logical_not(j == y))(lambda h=h: to_column(h, 0).wait_send())
        for n in range(1, 4):
            to_column(h, n).wait_send()

        @pl.when(jnp.logical_not(asks_self & (j == y)))
        def _(h=h):
            remote(q_out.at[h], q_in.at[0], q_send.at[h], q_recv.at[0], partner).wait_send()

    to_w.wait_send()
    to_g.wait_send()

    def drain_pair(s, none):
        pl.when(keeper)(lambda: to_partner(s).wait_send())
        return none

    lax.fori_loop(0, sources, drain_pair, 0)
    for slot in range(2):
        from_y = c if slot == 0 else 3 - c
        for p in range(2):

            @pl.when(jnp.logical_not((from_y == y) & (p == c)))
            def _(slot=slot, p=p, from_y=from_y):
                send_att(slot, p, from_y).wait_send()

    for d in range(2):
        for i in range(far):
            for order in range(4 if i else 2):
                from_sum(d, i, order if d == 0 else (order + 2) % 4).wait_send()


def expert_part(
    chips_y, cap, loads, gate_w, up_w, down_w, stream_ref, normed_ref, select_ref, weight_ref, out_ref,
    outgoing, arrived, rows, part, partner_part, ring_sum, back, returned, hidden,
    go_send, go_recv, ag_send, ag_recv, pair_send, pair_recv, pin_send, pin_recv,
    rs_send, rs_recv, back_send, back_recv,
):
    experts, _, width = outgoing.shape
    chunks, chips, _, block, _ = rows.shape
    far, half, per = chips // 2, width // 2, experts // chunks
    me, t = lax.axis_index("sp"), lax.axis_index("tp")
    z, c = t // 2, t % 2
    chips_x = experts // chips_y
    y, x = me // chips_x, me % chips_x
    moves = sorted(
        ((dy, dx) for dy in range(chips_y) for dx in range(chips_x)),
        key=lambda move: min(move[0], chips_y - move[0]) + min(move[1], chips_x - move[1]),
    )
    to_sp = [(y + dy) % chips_y * chips_x + (x + dx) % chips_x for dy, dx in moves]
    from_sp = [(y + chips_y - dy) % chips_y * chips_x + (x + chips_x - dx) % chips_x for dy, dx in moves]
    partner = (me, 2 * z + (1 - c))
    ahead = ((me, 2 * ((z + 1) % chips) + c), (me, 2 * ((z + chips - 1) % chips) + c))
    piece = (pl.ds(0, half), pl.ds(half, half))
    quarter = [pl.ds(n * half // 2, half // 2) for n in range(4)]

    chosen = jnp.dot(select_ref[...], normed_ref[...], preferred_element_type=jnp.float32)
    outgoing[...] = chosen.reshape(experts, SLOT_ROWS, width).astype(jnp.bfloat16)
    for k in range(chunks):
        for d in range(2):
            ring_sum[k, d, 0, :, piece[1 - d]] = jnp.zeros((block, half), jnp.bfloat16)

    def go(n):
        return remote(outgoing.at[to_sp[n]], arrived.at[n], go_send.at[n], go_recv.at[n], (to_sp[n], t))

    own = pltpu.make_async_copy(outgoing.at[me], arrived.at[0], go_recv.at[0])
    own.start()
    for n in range(1, experts):
        go(n).start()

    def take_arrived(k):
        for n in range(k * per, (k + 1) * per):
            (go(n).wait_recv if n else own.wait)()
        row = lax.broadcasted_iota(jnp.int32, (block, per * SLOT_ROWS), 0)
        col = lax.broadcasted_iota(jnp.int32, (block, per * SLOT_ROWS), 1)
        pick = (col == row // cap * SLOT_ROWS + row % cap).astype(jnp.bfloat16)
        padded = arrived[pl.ds(k * per, per)].astype(jnp.float32).reshape(per * SLOT_ROWS, width)
        rows[k, z, c] = jnp.dot(
            pick, padded.astype(jnp.bfloat16), preferred_element_type=jnp.float32
        ).astype(jnp.bfloat16)

    def far_first(d, order):
        return order if d == 0 else (order + 2) % 4

    def to_partner(k, at, p):
        ref = rows.at[k, at, c, :, piece[p]]
        return remote(ref, ref, pair_send.at[k, at, p], pair_recv.at[k, at, p], partner)

    def ring_rows(k, at, d, i, p):
        ref = rows.at[k, at, c, :, quarter[p]]
        return remote(ref, ref, ag_send.at[k, d, i, p], ag_recv.at[k, d, i, p], ahead[d])

    def start_own(k):
        for order in range(4):
            for d in range(2):
                ring_rows(k, z, d, 0, far_first(d, order)).start()
        for p in range(2):
            to_partner(k, z, p).start()

    def gather_half(k, i, second):
        for order in (2, 3) if second else (0, 1):
            for d in range(2):
                p = far_first(d, order)
                at = lax.rem((z - i - 1 if d == 0 else z + i + 1) + chips, chips)
                ring_rows(k, at, d, i, p).wait_recv()

                @pl.when(i + 1 < (far - 1 if second else far))
                def _(at=at, d=d, p=p):
                    ring_rows(k, at, d, i + 1, p).start()

                if order % 2 == 1:
                    to_partner(k, at, p // 2).start()

    def gather_step(k, i):
        gather_half(k, i, False)
        pl.when(i < far - 1)(lambda: gather_half(k, i, True))

    def wait_partner_rows(k):
        def wait_one(at, none):
            for p in range(2):
                ref = rows.at[k, at, 1 - c, :, piece[p]]
                remote(ref, ref, pair_send.at[k, at, p], pair_recv.at[k, at, p], partner).wait_recv()
            return none

        lax.fori_loop(0, chips, wait_one, 0)

    group = chips // far

    def gate_and_up(k, i):
        x = rows[k, pl.ds(i * group, group)].reshape(group * 2 * block, width)
        across = (((1,), (1,)), ((), ()))
        gate = lax.dot_general(x, gate_w[...], across, preferred_element_type=jnp.float32)
        up = lax.dot_general(x, up_w[...], across, preferred_element_type=jnp.float32)
        hidden[...] = (gate / (1.0 + jnp.exp(-gate)) * up).astype(jnp.bfloat16)

    def down(k, i):
        at = pl.ds(i * group, group)
        product = jnp.dot(hidden[...], down_w[...], preferred_element_type=jnp.float32)
        part[k, at] = product.astype(jnp.bfloat16).reshape(group, 2, block, width)
        for j in range(group):
            pin(k, i * group + j).start()

    def pin(k, at):
        return remote(
            part.at[k, at, 1 - c], partner_part.at[k, at], pin_send.at[k, at], pin_recv.at[k, at], partner
        )

    def wait_pins(k):
        def wait_one(at, none):
            pin(k, at).wait_recv()
            return none

        lax.fori_loop(0, chips, wait_one, 0)

    def from_sum(k, d, i, p):
        ref = ring_sum.at[k, d, i, :, quarter[p]]
        return remote(ref, ref, rs_send.at[k, d, i, p], rs_recv.at[k, d, i, p], ahead[d])

    def sum_half(k, i, second):
        for order in (2, 3) if second else (0, 1):
            for d in range(2):
                p = far_first(d, order)
                at = lax.rem((z + (far - i) if d == 0 else z - (far - i)) + chips, chips)
                total = part[k, at, c, :, quarter[p]].astype(jnp.float32) + partner_part[
                    k, at, :, quarter[p]
                ].astype(jnp.float32)
                if isinstance(i, int):
                    assert i == 0
                else:
                    wait = from_sum(k, d, i - 1, p).wait_recv
                    if second:
                        pl.when(i > 1)(wait)
                    else:
                        wait()
                    total = total + ring_sum[k, d, i - 1, :, quarter[p]].astype(jnp.float32)
                part[k, at, c, :, quarter[p]] = total.astype(jnp.bfloat16)
                remote(
                    part.at[k, at, c, :, quarter[p]],
                    ring_sum.at[k, d, i, :, quarter[p]],
                    rs_send.at[k, d, i, p],
                    rs_recv.at[k, d, i, p],
                    ahead[d],
                ).start()

    def send_back(k):
        for p in range(4):
            for d in range(2):
                from_sum(k, d, far - 1, p).wait_recv()
        total = (
            part[k, z, c].astype(jnp.float32)
            + partner_part[k, z].astype(jnp.float32)
            + ring_sum[k, 0, far - 1].astype(jnp.float32)
            + ring_sum[k, 1, far - 1].astype(jnp.float32)
        ).astype(jnp.bfloat16)
        row = lax.broadcasted_iota(jnp.int32, (per * SLOT_ROWS, block), 0)
        col = lax.broadcasted_iota(jnp.int32, (per * SLOT_ROWS, block), 1)
        spread = ((row % SLOT_ROWS < cap) & (col == row // SLOT_ROWS * cap + row % SLOT_ROWS)).astype(jnp.bfloat16)
        back[pl.ds(k * per, per)] = (
            jnp.dot(spread, total, preferred_element_type=jnp.float32)
            .reshape(per, SLOT_ROWS, width)
            .astype(jnp.bfloat16)
        )

        for n in range(k * per, (k + 1) * per):
            if n:
                send_home(n).start()
            else:
                pltpu.make_async_copy(back.at[0], returned.at[me], back_recv.at[me]).start()

    def send_home(n):
        return remote(back.at[n], returned.at[me], back_send.at[n], back_recv.at[me], (from_sp[n], t))

    def steps(first, last, body):
        def one(i, none):
            body(i)
            return none

        lax.fori_loop(first, last, one, 0)

    take_arrived(0)
    start_own(0)
    take_arrived(1)
    steps(0, far - 1, lambda i: gather_step(0, i))
    start_own(1)
    gather_step(0, far - 1)
    for load in loads:
        load.wait()
    wait_partner_rows(0)

    def gather_and_compute(i):
        gather_half(1, i, False)
        gate_and_up(0, i)
        gather_half(1, i, True)
        down(0, i)

    steps(0, far - 1, gather_and_compute)
    gate_and_up(0, far - 1)
    down(0, far - 1)
    wait_pins(0)
    sum_half(0, 0, False)
    gather_step(1, far - 1)
    wait_partner_rows(1)

    def sum_and_compute(i):
        sum_half(0, i, False)
        gate_and_up(1, i - 1)
        sum_half(0, i, True)
        down(1, i - 1)

    steps(1, far, sum_and_compute)
    gate_and_up(1, far - 1)
    down(1, far - 1)
    wait_pins(1)
    sum_half(1, 0, False)
    send_back(0)

    def only_sum(i):
        sum_half(1, i, False)
        sum_half(1, i, True)

    steps(1, far, only_sum)
    send_back(1)

    def wait_back(e, none):
        @pl.when(e == me)
        def _():
            pltpu.make_async_copy(back.at[e], returned.at[e], back_recv.at[e]).wait()

        @pl.when(e != me)
        def _():
            remote(back.at[e], returned.at[e], back_send.at[e], back_recv.at[e], (e, t)).wait_recv()

        return none

    lax.fori_loop(0, experts, wait_back, 0)
    picked = returned[...].astype(jnp.float32).reshape(experts * SLOT_ROWS, width).astype(jnp.bfloat16)
    combined = stream_ref[...].astype(jnp.float32)
    for n in reversed(range(3)):
        combined = combined + lax.dot_general(
            weight_ref[n], picked, (((0,), (0,)), ((), ())), preferred_element_type=jnp.float32
        )
    out_ref[...] = combined.astype(jnp.bfloat16)

    for n in range(1, experts):
        go(n).wait_send()
        send_home(n).wait_send()

    def drain_pair(at, none):
        for k in range(chunks):
            for p in range(2):
                to_partner(k, at, p).wait_send()
            pin(k, at).wait_send()
        return none

    lax.fori_loop(0, chips, drain_pair, 0)

    def drain_ring(i, none):
        for k in range(chunks):
            for d in range(2):
                for order in range(4):
                    p = far_first(d, order)
                    sent, summed = ring_rows(k, 0, d, i, p).wait_send, from_sum(k, d, i, p).wait_send
                    if order < 2:
                        sent()
                        summed()
                    else:
                        pl.when(i < far - 1)(sent)
                        pl.when(i > 0)(summed)
        return none

    lax.fori_loop(0, far, drain_ring, 0)


def layer_kernel(
    chips_y, cap, q_hbm, k_hbm, v_hbm, bias_hbm, gain_hbm, w_hbm, residual_hbm, norm_hbm, choice_hbm, share_hbm,
    gate_hbm, up_hbm, down_hbm, out_ref, q, k, v, bias, gain, w, residual, norm, choice, share, gate_w, up_w, down_w,
    load_sem, stream, normed, select, weight, *scratch,
):
    sources = (q_hbm, k_hbm, v_hbm, bias_hbm, gain_hbm, w_hbm, residual_hbm, norm_hbm, choice_hbm, share_hbm)
    sources += (gate_hbm.at[0], up_hbm.at[0], down_hbm.at[0])
    places = (q, k, v, bias, gain, w, residual, norm, choice, share, gate_w, up_w, down_w)
    loads = [pltpu.make_async_copy(src, dst, load_sem.at[i]) for i, (src, dst) in enumerate(zip(sources, places))]
    for load in loads:
        load.start()

    def route():
        for load in loads[8:10]:
            load.wait()
        slots, own_rows = select.shape
        slot = lax.broadcasted_iota(jnp.int32, (slots, own_rows), 0)
        expert, place = slot // SLOT_ROWS, slot % SLOT_ROWS
        first = choice[0:1, :] == expert
        named = first | (choice[1:2, :] == expert)
        earlier = lax.broadcasted_iota(jnp.int32, (own_rows, own_rows), 0) < lax.broadcasted_iota(
            jnp.int32, (own_rows, own_rows), 1
        )
        before = jnp.dot(
            named.astype(jnp.bfloat16), earlier.astype(jnp.bfloat16), preferred_element_type=jnp.float32
        )
        chosen = named & (before.astype(jnp.int32) == place)
        select[...] = chosen.astype(jnp.bfloat16)
        rest = jnp.where(chosen, jnp.where(first, share[0:1, :], share[1:2, :]), 0.0)
        for n in range(3):
            term = rest.astype(jnp.bfloat16)
            weight[n] = term
            rest = rest - term.astype(jnp.float32)

    attention_part(
        chips_y, loads[:8], route, q, k, v, bias, gain, w, residual, norm, stream, normed, *scratch[:ATTENTION_SCRATCH]
    )
    expert_part(chips_y, cap, loads[10:], gate_w, up_w, down_w, stream, normed, select, weight, out_ref, *scratch[ATTENTION_SCRATCH:])


ATTENTION_SCRATCH = 30


def layer(
    queries, keys, values, key_bias, head_gain, out_weight, residual, norm_gain, gate_proj, up_proj, down_proj,
    expert_choice, expert_weights,
):
    rows, packed = queries.shape
    size, width, hidden = head_gain.shape[1], out_weight.shape[1], gate_proj.shape[2]
    blocks, chips, chips_y, chunks = lax.axis_size("sp"), lax.axis_size("tp") // 2, 4, 2
    chips_x, far, own = blocks // chips_y, chips // 2, residual.shape[0]
    cap = 4 * own // blocks
    block, slots = blocks // chunks * cap, blocks * SLOT_ROWS
    bf16, f32, dma = jnp.bfloat16, jnp.float32, pltpu.SemaphoreType.DMA
    arguments = (
        queries, keys, values, key_bias.T, head_gain, out_weight, residual, norm_gain.reshape(1, -1),
        expert_choice.T, expert_weights.T, gate_proj.swapaxes(1, 2), up_proj.swapaxes(1, 2), down_proj,
    )
    scratch = [pltpu.VMEM(a.shape[-2:], a.dtype) for a in arguments]
    scratch += [
        dma((len(arguments),)),
        pltpu.VMEM((own, width), bf16),
        pltpu.VMEM((own, width), bf16),
        pltpu.VMEM((slots, own), bf16),
        pltpu.VMEM((3, slots, own), bf16),
    ]
    attention_scratch = [
        pltpu.VMEM((2, rows + 16, packed), bf16),
        pltpu.VMEM((2, rows // 2, packed), bf16),
        pltpu.VMEM((blocks, rows + 16, packed), bf16),
        pltpu.VMEM((2, rows // 2, packed), bf16),
        pltpu.VMEM((2, rows, packed), bf16),
        pltpu.VMEM((2, 2, size), f32),
        pltpu.VMEM((2, packed, width), bf16),
        pltpu.VMEM((rows, packed), f32),
        pltpu.VMEM((rows, 1), f32),
        pltpu.VMEM((2, chips_y, rows, packed), f32),
        pltpu.VMEM((2, chips_y, rows, 1), f32),
        pltpu.VMEM((2, 2, chips, own, size), bf16),
        pltpu.VMEM((chips_y, chips, own, size), bf16),
        pltpu.VMEM((chips, own, width), f32),
        pltpu.VMEM((2, far, own, width), bf16),
        pltpu.VMEM((2, far, own, width), bf16),
        dma((2, 4)),
        dma((blocks,)),
        dma((2,)),
        dma((2,)),
        dma((blocks,)),
        dma((blocks,)),
        dma((1,)),
        dma((1,)),
        dma((1,)),
        dma((1,)),
        dma((2, 2)),
        dma((chips_y,)),
        dma((2, far, 4)),
        dma((2, far, 4)),
    ]
    expert_scratch = [
        pltpu.VMEM((blocks, SLOT_ROWS, width), bf16),
        pltpu.VMEM((blocks, SLOT_ROWS, width), bf16),
        pltpu.VMEM((chunks, chips, 2, block, width), bf16),
        pltpu.VMEM((chunks, chips, 2, block, width), bf16),
        pltpu.VMEM((chunks, chips, block, width), bf16),
        pltpu.VMEM((chunks, 2, far, block, width), bf16),
        pltpu.VMEM((blocks, SLOT_ROWS, width), bf16),
        pltpu.VMEM((blocks, SLOT_ROWS, width), bf16),
        pltpu.VMEM((chips // far * 2 * block, hidden), bf16),
        dma((blocks,)),
        dma((blocks,)),
        dma((chunks, 2, far, 4)),
        dma((chunks, 2, far, 4)),
        dma((chunks, chips, 2)),
        dma((chunks, chips, 2)),
        dma((chunks, chips)),
        dma((chunks, chips)),
        dma((chunks, 2, far, 4)),
        dma((chunks, 2, far, 4)),
        dma((blocks,)),
        dma((blocks,)),
    ]
    assert len(attention_scratch) == ATTENTION_SCRATCH
    return pl.pallas_call(
        functools.partial(layer_kernel, chips_y, cap),
        out_shape=jax.ShapeDtypeStruct(residual.shape, bf16),
        in_specs=[pl.BlockSpec(memory_space=pl.ANY)] * len(arguments),
        out_specs=pl.BlockSpec(memory_space=pltpu.VMEM),
        scratch_shapes=scratch + attention_scratch + expert_scratch,
        compiler_params=pltpu.CompilerParams(collective_id=1, has_side_effects=True, vmem_limit_bytes=60 << 20),
        name="layer",
    )(*arguments)


def solution(mesh):
    placed = (
        P("sp", "tp"),
        P("sp", "tp"),
        P("sp", "tp"),
        P("sp", "tp"),
        P("tp", None),
        P("tp", None),
        P(("sp", "tp"), None),
        P(),
        P("sp", None, "tp"),
        P("sp", None, "tp"),
        P("sp", "tp", None),
        P(("sp", "tp"), None),
        P(("sp", "tp"), None),
    )
    return jax.shard_map(
        layer, mesh=mesh, in_specs=placed, out_specs=P(("sp", "tp"), None), check_vma=False
    )
```

```python
import functools

import jax
import jax.numpy as jnp
from jax import lax
from jax.experimental import pallas as pl
from jax.experimental.pallas import tpu as pltpu
from jax.sharding import PartitionSpec as P

epsilon = 1e-06
CHUNK = 256
MESH = pl.DeviceIdType.MESH
SLOT_ROWS = 8


def remote(src, dst, send_sem, recv_sem, device):
    return pltpu.make_async_remote_copy(
        src_ref=src, dst_ref=dst, send_sem=send_sem, recv_sem=recv_sem, device_id=device, device_id_type=MESH
    )


def attention_part(
    chips_y, loads, route, q_ref, k_ref, v_ref, bias_ref, gain_ref, w_ref, residual_ref, norm_ref, stream_ref, normed_ref,
    kv_out, q_out, kv, q_in, q_wide, gains, weights, acc, carry, early, early_carry, att_out, att_in, part, part_out, ring_sum,
    kv_send, kv_recv, q_send, q_recv, pair_send, pair_recv, w_send, w_recv, g_send, g_recv,
    att_send, att_recv, rs_send, rs_recv,
):
    rows, packed = q_ref.shape
    size = packed // 2
    chips_x = lax.axis_size("sp") // chips_y
    chips = lax.axis_size("tp") // 2
    width = w_ref.shape[1]
    far, half = chips // 2, width // 2
    quarter = [pl.ds(n * half // 2, half // 2) for n in range(4)]
    me, t = lax.axis_index("sp"), lax.axis_index("tp")
    y, x, z, c = me // chips_x, me % chips_x, t // 2, t % 2

    def device(yy, xx, zz, cc):
        return (yy * chips_x + xx, 2 * zz + cc)

    def query_core(yy):
        return ((yy + 1) // 2) % 2

    partner = device(y, x, z, 1 - c)
    ahead = (device(y, x, (z + 1) % chips, c), device(y, x, (z + chips - 1) % chips, c))
    barrier = pltpu.get_barrier_semaphore()
    sources = lax.axis_size("sp")

    def greet(n, none):
        pl.semaphore_signal(barrier, inc=1, device_id=((me + n) % sources, t), device_id_type=MESH)
        return none

    lax.fori_loop(1, sources, greet, 0)
    others = [device((y + dy) % chips_y, x, z, 1 - c) for dy in range(chips_y)] + list(ahead)
    for other in others:
        pl.semaphore_signal(barrier, inc=1, device_id=other, device_id_type=MESH)
    for load in loads[:5]:
        load.wait()

    offsets = bias_ref[...].astype(jnp.float32)
    for h in range(2):
        lanes = slice(h * size, (h + 1) * size)
        kv_out[h, pl.ds(0, rows)] = jnp.concatenate([k_ref[:, lanes], v_ref[:, lanes]], axis=1)
        by_row = [offsets[h : h + 1, n * packed : (n + 1) * packed] for n in range(rows // packed)]
        by_row.append(jnp.zeros((16 - rows // packed, packed), jnp.float32))
        kv_out[h, pl.ds(rows, 16)] = jnp.concatenate(by_row, axis=0).astype(jnp.bfloat16)
        q_neg = q_ref[:, lanes] * jnp.bfloat16(-(size ** -0.5))
        q_out[h] = jnp.concatenate([q_neg[: rows // 2], q_neg[rows // 2 :]], axis=1)
    gains[c] = gain_ref[...]
    pl.semaphore_wait(barrier, sources - 1 + len(others))

    keeper = y // 2 == c
    asks_self = keeper & (query_core(y) == c)
    side, base = x % 2, x // 2 * 2
    other = (base + 2) % chips_x
    columns = (x, base + 1 - side, other + 1 - side, other + side)

    def to_column(h, n):
        return remote(
            kv_out.at[h], kv.at[me], kv_send.at[h, n], kv_recv.at[me], device(2 * c + h, columns[n], z, c)
        )

    for n in range(4):
        for h in range(2):
            if n > 0:
                to_column(h, n).start()
            else:
                pl.when(jnp.logical_not(2 * c + h == y))(lambda h=h: to_column(h, 0).start())

                @pl.when(2 * c + h == y)
                def _(h=h):
                    pltpu.make_async_copy(kv_out.at[h], kv.at[me], kv_recv.at[me]).start()

    for h in range(2):
        j = 2 * c + h

        @pl.when(jnp.logical_not(asks_self & (j == y)))
        def _(h=h, j=j):
            remote(q_out.at[h], q_in.at[y // 2], q_send.at[h], q_recv.at[y // 2], device(j, x, z, query_core(y))).start()

        @pl.when(asks_self & (j == y))
        def _(h=h):
            pltpu.make_async_copy(q_out.at[h], q_in.at[y // 2], q_recv.at[y // 2]).start()

    to_w = remote(w_ref, weights.at[c], w_send.at[0], w_recv.at[0], partner)
    to_g = remote(gain_ref, gains.at[c], g_send.at[0], g_recv.at[0], partner)
    to_g.start()
    route()

    def to_partner(s):
        return remote(kv.at[s], kv.at[s], pair_send.at[s], pair_recv.at[s], partner)

    def arrive(column):
        def one(yy, none):
            s = yy * chips_x + column

            @pl.when(keeper & (s == me))
            def _():
                pltpu.make_async_copy(kv_out.at[0], kv.at[s], kv_recv.at[s]).wait()

            @pl.when(keeper & (s != me))
            def _():
                remote(kv_out.at[0], kv.at[s], kv_send.at[0, 1], kv_recv.at[s], partner).wait_recv()

            pl.when(keeper)(lambda: to_partner(s).start())
            return none

        lax.fori_loop(0, chips_y, one, 0)

    def handed(column):
        def one(yy, none):
            pl.when(jnp.logical_not(keeper))(lambda: to_partner(yy * chips_x + column).wait_recv())
            return none

        lax.fori_loop(0, chips_y, one, 0)

    arrive(columns[0])
    arrive(columns[1])
    for load in loads[5:]:
        load.wait()
    to_w.start()
    weights[c] = w_ref[...]
    handed(columns[0])
    handed(columns[1])

    row = lax.broadcasted_iota(jnp.int32, (CHUNK, CHUNK), 0)
    col = lax.broadcasted_iota(jnp.int32, (CHUNK, CHUNK), 1)
    after = (row > col).astype(jnp.bfloat16)

    def pair_of_blocks(slot, older, masked, shift=0):
        def part_of(place, first, length):
            return kv[older + place, pl.ds(first, length)], kv[older + place, pl.ds(rows, 16)], first // 128, length // 128

        def chunk(sources, place):
            kv_part = jnp.concatenate([s[0] for s in sources], axis=0)
            offset = jnp.concatenate(
                [s[1][s[2] + n : s[2] + n + 1, :].astype(jnp.float32) for s in sources for n in range(s[3])], axis=1
            )
            minus = (
                lax.dot_general(
                    q_wide[slot], kv_part, (((1,), (1,)), ((), ())), preferred_element_type=jnp.float32
                )
                - offset
            )
            log_part = jnp.log(1.0 + jnp.exp(-jnp.abs(minus)))
            drop = jnp.minimum(minus, 0.0) - log_part
            own_log = drop - minus
            if masked:
                q_at = lax.broadcasted_iota(jnp.int32, (rows, CHUNK), 0) + (shift - place)
                earlier = lax.broadcasted_iota(jnp.int32, (rows, CHUNK), 1) < q_at
                drop = jnp.where(earlier, drop, 0.0)
            suffix = jnp.dot(drop.astype(jnp.bfloat16), after, preferred_element_type=jnp.float32)
            within = jnp.exp(own_log + suffix)
            if masked:
                within = jnp.where(earlier, within, 0.0)
            product = jnp.dot(within.astype(jnp.bfloat16), kv_part, preferred_element_type=jnp.float32)
            now = carry[...]
            acc[...] += jnp.exp(now) * product
            carry[...] = now + (suffix[:, :1] + drop[:, :1])

        chunk([part_of(1, 128, 256)], 512)
        chunk([part_of(0, 256, 128), part_of(1, 0, 128)], 256)
        chunk([part_of(0, 0, 256)], 0)

    def query_row(slot):
        return c if slot == 0 else 3 - c

    def begin(slot):
        from_y = query_row(slot)
        asked = asks_self & (from_y == y)

        @pl.when(asked)
        def _():
            pltpu.make_async_copy(q_out.at[0], q_in.at[slot], q_recv.at[slot]).wait()

        @pl.when(jnp.logical_not(asked))
        def _():
            remote(q_out.at[0], q_in.at[slot], q_send.at[0], q_recv.at[slot], partner).wait_recv()

        folded = q_in[slot]
        q_here = jnp.concatenate([folded[:, :size], folded[:, size:]], axis=0)
        q_wide[slot] = jnp.concatenate([q_here, jnp.zeros_like(q_here)], axis=1)

        def one(yy, masked):
            acc[...] = jnp.zeros_like(acc)
            carry[...] = jnp.zeros_like(carry)
            pair_of_blocks(slot, yy * chips_x + base, masked, side * rows)
            early[slot, yy] = acc[...]
            early_carry[slot, yy] = carry[...]

        def body(yy, none):
            one(yy, False)
            return none

        one(from_y, True)
        lax.fori_loop(0, from_y, body, 0)

    def attend(slot):
        from_y = query_row(slot)
        acc[...] = jnp.zeros_like(acc)
        carry[...] = jnp.zeros_like(carry)
        newest = from_y - (1 - base // 2)

        def body(n, none):
            now = carry[...]
            acc[...] += jnp.exp(now) * early[slot, from_y - n]
            carry[...] = now + early_carry[slot, from_y - n]

            @pl.when(n <= newest)
            def _():
                pair_of_blocks(slot, (newest - n) * chips_x + other, False)

            return none

        lax.fori_loop(0, from_y + 1, body, 0)
        mixture = acc[...][:, size:]
        scaled = mixture * lax.rsqrt(jnp.mean(mixture * mixture, axis=-1, keepdims=True) + epsilon)
        scaled = scaled * gains[y // 2, pl.ds(y % 2, 1), :]
        by_owner = scaled.reshape(chips, 2, rows // (2 * chips), size)
        for p in range(2):
            att_out[slot, p] = by_owner[:, p].astype(jnp.bfloat16)
            stays = (from_y == y) & (p == c)

            @pl.when(stays)
            def _(p=p):
                pltpu.make_async_copy(att_out.at[slot, p], att_in.at[y], att_recv.at[y]).start()

            @pl.when(jnp.logical_not(stays))
            def _(p=p):
                send_att(slot, p, from_y).start()

    def send_att(slot, p, from_y):
        return remote(
            att_out.at[slot, p], att_in.at[y], att_send.at[slot, p], att_recv.at[y], device(from_y, x, z, p)
        )

    begin(1)
    arrive(columns[2])
    arrive(columns[3])
    begin(0)
    handed(columns[2])
    handed(columns[3])
    to_g.wait_recv()
    attend(1)
    attend(0)

    for j in range(chips_y):
        stayed = (j == y) & (query_core(y) == c)

        @pl.when(stayed)
        def _(j=j):
            pltpu.make_async_copy(att_out.at[0, 0], att_in.at[j], att_recv.at[j]).wait()

        @pl.when(jnp.logical_not(stayed))
        def _(j=j):
            remote(att_out.at[0, 0], att_in.at[j], att_send.at[0, 0], att_recv.at[j], partner).wait_recv()

    to_w.wait_recv()
    heads = [att_in[j].astype(jnp.float32).reshape(rows // 2, size) for j in range(chips_y)]
    merged = jnp.concatenate(heads, axis=1).astype(jnp.bfloat16)
    farthest = (z + far) % chips
    far_heads = [att_in[j, farthest].astype(jnp.float32) for j in range(chips_y)]
    far_merged = jnp.concatenate(far_heads, axis=1).astype(jnp.bfloat16)
    rows_of_w = weights[...].reshape(2 * packed, width)
    part[farthest] = jnp.dot(far_merged, rows_of_w, preferred_element_type=jnp.float32)

    def rest_of_part():
        share = jnp.dot(merged, rows_of_w, preferred_element_type=jnp.float32)
        part[...] = share.reshape(part.shape)

    def from_sum(d, i, p):
        ref = ring_sum.at[d, i, :, quarter[p]]
        return remote(ref, ref, rs_send.at[d, i, p], rs_recv.at[d, i, p], ahead[d])

    for i in range(far):
        if i == 1:
            rest_of_part()
        for order in range(4 if i else 2):
            for d in range(2):
                p = order if d == 0 else (order + 2) % 4
                at = ((z + (far - i)) if d == 0 else (z - (far - i) + chips)) % chips
                total = part[at, :, quarter[p]]
                if i > 1 or (i == 1 and order < 2):
                    from_sum(d, i - 1, p).wait_recv()
                    total = total + ring_sum[d, i - 1, :, quarter[p]].astype(jnp.float32)
                part_out[d, i, :, quarter[p]] = total.astype(jnp.bfloat16)
                remote(
                    part_out.at[d, i, :, quarter[p]],
                    ring_sum.at[d, i, :, quarter[p]],
                    rs_send.at[d, i, p],
                    rs_recv.at[d, i, p],
                    ahead[d],
                ).start()
    for d in range(2):
        for p in range(4):
            from_sum(d, far - 1, p).wait_recv()
    projected = part[z] + ring_sum[0, far - 1].astype(jnp.float32) + ring_sum[1, far - 1].astype(jnp.float32)
    stream = (residual_ref[...].astype(jnp.float32) + projected).astype(jnp.bfloat16)
    stream_ref[...] = stream
    wide = stream.astype(jnp.float32)
    normed_ref[...] = (
        wide * lax.rsqrt(jnp.mean(wide * wide, axis=-1, keepdims=True) + epsilon) * norm_ref[...]
    ).astype(jnp.bfloat16)

    for h in range(2):
        j = 2 * c + h

        pl.when(jnp.logical_not(j == y))(lambda h=h: to_column(h, 0).wait_send())
        for n in range(1, 4):
            to_column(h, n).wait_send()

        @pl.when(jnp.logical_not(asks_self & (j == y)))
        def _(h=h):
            remote(q_out.at[h], q_in.at[0], q_send.at[h], q_recv.at[0], partner).wait_send()

    to_w.wait_send()
    to_g.wait_send()

    def drain_pair(s, none):
        pl.when(keeper)(lambda: to_partner(s).wait_send())
        return none

    lax.fori_loop(0, sources, drain_pair, 0)
    for slot in range(2):
        from_y = c if slot == 0 else 3 - c
        for p in range(2):

            @pl.when(jnp.logical_not((from_y == y) & (p == c)))
            def _(slot=slot, p=p, from_y=from_y):
                send_att(slot, p, from_y).wait_send()

    for d in range(2):
        for i in range(far):
            for order in range(4 if i else 2):
                from_sum(d, i, order if d == 0 else (order + 2) % 4).wait_send()


def expert_part(
    chips_y, cap, loads, gate_w, up_w, down_w, stream_ref, normed_ref, select_ref, weight_ref, out_ref,
    outgoing, arrived, rows, part, partner_part, ring_sum, back, returned, hidden,
    go_send, go_recv, ag_send, ag_recv, pair_send, pair_recv, pin_send, pin_recv,
    rs_send, rs_recv, back_send, back_recv,
):
    experts, _, width = outgoing.shape
    chunks, chips, _, block, _ = rows.shape
    far, half, per = chips // 2, width // 2, experts // chunks
    me, t = lax.axis_index("sp"), lax.axis_index("tp")
    z, c = t // 2, t % 2
    chips_x = experts // chips_y
    y, x = me // chips_x, me % chips_x
    moves = sorted(
        ((dy, dx) for dy in range(chips_y) for dx in range(chips_x)),
        key=lambda move: min(move[0], chips_y - move[0]) + min(move[1], chips_x - move[1]),
    )
    to_sp = [(y + dy) % chips_y * chips_x + (x + dx) % chips_x for dy, dx in moves]
    from_sp = [(y + chips_y - dy) % chips_y * chips_x + (x + chips_x - dx) % chips_x for dy, dx in moves]
    partner = (me, 2 * z + (1 - c))
    ahead = ((me, 2 * ((z + 1) % chips) + c), (me, 2 * ((z + chips - 1) % chips) + c))
    piece = (pl.ds(0, half), pl.ds(half, half))
    quarter = [pl.ds(n * half // 2, half // 2) for n in range(4)]

    chosen = jnp.dot(select_ref[...], normed_ref[...], preferred_element_type=jnp.float32)
    outgoing[...] = chosen.reshape(experts, SLOT_ROWS, width).astype(jnp.bfloat16)
    for k in range(chunks):
        for d in range(2):
            ring_sum[k, d, 0, :, piece[1 - d]] = jnp.zeros((block, half), jnp.bfloat16)

    def go(n):
        return remote(outgoing.at[to_sp[n], pl.ds(0, cap)], arrived.at[n, pl.ds(0, cap)], go_send.at[n], go_recv.at[n], (to_sp[n], t))

    own = pltpu.make_async_copy(outgoing.at[me], arrived.at[0], go_recv.at[0])
    own.start()
    for n in range(1, experts):
        go(n).start()

    def take_arrived(k):
        for n in range(k * per, (k + 1) * per):
            (go(n).wait_recv if n else own.wait)()
        row = lax.broadcasted_iota(jnp.int32, (block, per * SLOT_ROWS), 0)
        col = lax.broadcasted_iota(jnp.int32, (block, per * SLOT_ROWS), 1)
        pick = (col == row // cap * SLOT_ROWS + row % cap).astype(jnp.bfloat16)
        padded = arrived[pl.ds(k * per, per)].astype(jnp.float32).reshape(per * SLOT_ROWS, width)
        rows[k, z, c] = jnp.dot(
            pick, padded.astype(jnp.bfloat16), preferred_element_type=jnp.float32
        ).astype(jnp.bfloat16)

    def far_first(d, order):
        return order if d == 0 else (order + 2) % 4

    def to_partner(k, at, p):
        ref = rows.at[k, at, c, :, piece[p]]
        return remote(ref, ref, pair_send.at[k, at, p], pair_recv.at[k, at, p], partner)

    def ring_rows(k, at, d, i, p):
        ref = rows.at[k, at, c, :, quarter[p]]
        return remote(ref, ref, ag_send.at[k, d, i, p], ag_recv.at[k, d, i, p], ahead[d])

    def start_own(k):
        for order in range(4):
            for d in range(2):
                ring_rows(k, z, d, 0, far_first(d, order)).start()
        for p in range(2):
            to_partner(k, z, p).start()

    def gather_half(k, i, second):
        for order in (2, 3) if second else (0, 1):
            for d in range(2):
                p = far_first(d, order)
                at = lax.rem((z - i - 1 if d == 0 else z + i + 1) + chips, chips)
                ring_rows(k, at, d, i, p).wait_recv()

                @pl.when(i + 1 < (far - 1 if second else far))
                def _(at=at, d=d, p=p):
                    ring_rows(k, at, d, i + 1, p).start()

                if order % 2 == 1:
                    to_partner(k, at, p // 2).start()

    def gather_step(k, i):
        gather_half(k, i, False)
        pl.when(i < far - 1)(lambda: gather_half(k, i, True))

    def wait_partner_rows(k):
        def wait_one(at, none):
            for p in range(2):
                ref = rows.at[k, at, 1 - c, :, piece[p]]
                remote(ref, ref, pair_send.at[k, at, p], pair_recv.at[k, at, p], partner).wait_recv()
            return none

        lax.fori_loop(0, chips, wait_one, 0)

    group = chips // far

    def gate_and_up(k, i):
        x = rows[k, pl.ds(i * group, group)].reshape(group * 2 * block, width)
        across = (((1,), (1,)), ((), ()))
        gate = lax.dot_general(x, gate_w[...], across, preferred_element_type=jnp.float32)
        up = lax.dot_general(x, up_w[...], across, preferred_element_type=jnp.float32)
        hidden[...] = (gate / (1.0 + jnp.exp(-gate)) * up).astype(jnp.bfloat16)

    def down(k, i):
        at = pl.ds(i * group, group)
        product = jnp.dot(hidden[...], down_w[...], preferred_element_type=jnp.float32)
        part[k, at] = product.astype(jnp.bfloat16).reshape(group, 2, block, width)
        for j in range(group):
            pin(k, i * group + j).start()

    def pin(k, at):
        return remote(
            part.at[k, at, 1 - c], partner_part.at[k, at], pin_send.at[k, at], pin_recv.at[k, at], partner
        )

    def wait_pins(k):
        def wait_one(at, none):
            pin(k, at).wait_recv()
            return none

        lax.fori_loop(0, chips, wait_one, 0)

    def from_sum(k, d, i, p):
        ref = ring_sum.at[k, d, i, :, quarter[p]]
        return remote(ref, ref, rs_send.at[k, d, i, p], rs_recv.at[k, d, i, p], ahead[d])

    def sum_half(k, i, second):
        for order in (2, 3) if second else (0, 1):
            for d in range(2):
                p = far_first(d, order)
                at = lax.rem((z + (far - i) if d == 0 else z - (far - i)) + chips, chips)
                total = part[k, at, c, :, quarter[p]].astype(jnp.float32) + partner_part[
                    k, at, :, quarter[p]
                ].astype(jnp.float32)
                if isinstance(i, int):
                    assert i == 0
                else:
                    wait = from_sum(k, d, i - 1, p).wait_recv
                    if second:
                        pl.when(i > 1)(wait)
                    else:
                        wait()
                    total = total + ring_sum[k, d, i - 1, :, quarter[p]].astype(jnp.float32)
                part[k, at, c, :, quarter[p]] = total.astype(jnp.bfloat16)
                remote(
                    part.at[k, at, c, :, quarter[p]],
                    ring_sum.at[k, d, i, :, quarter[p]],
                    rs_send.at[k, d, i, p],
                    rs_recv.at[k, d, i, p],
                    ahead[d],
                ).start()

    def send_back(k):
        for p in range(4):
            for d in range(2):
                from_sum(k, d, far - 1, p).wait_recv()
        total = (
            part[k, z, c].astype(jnp.float32)
            + partner_part[k, z].astype(jnp.float32)
            + ring_sum[k, 0, far - 1].astype(jnp.float32)
            + ring_sum[k, 1, far - 1].astype(jnp.float32)
        ).astype(jnp.bfloat16)
        row = lax.broadcasted_iota(jnp.int32, (per * SLOT_ROWS, block), 0)
        col = lax.broadcasted_iota(jnp.int32, (per * SLOT_ROWS, block), 1)
        spread = ((row % SLOT_ROWS < cap) & (col == row // SLOT_ROWS * cap + row % SLOT_ROWS)).astype(jnp.bfloat16)
        back[pl.ds(k * per, per)] = (
            jnp.dot(spread, total, preferred_element_type=jnp.float32)
            .reshape(per, SLOT_ROWS, width)
            .astype(jnp.bfloat16)
        )

        for n in range(k * per, (k + 1) * per):
            if n:
                send_home(n).start()
            else:
                pltpu.make_async_copy(back.at[0], returned.at[me], back_recv.at[me]).start()

    def send_home(n):
        return remote(
            back.at[n, pl.ds(0, cap)], returned.at[me, pl.ds(0, cap)], back_send.at[n], back_recv.at[me], (from_sp[n], t)
        )

    def steps(first, last, body):
        def one(i, none):
            body(i)
            return none

        lax.fori_loop(first, last, one, 0)

    take_arrived(0)
    start_own(0)
    gather_step(0, 0)
    take_arrived(1)
    steps(1, far - 1, lambda i: gather_step(0, i))
    start_own(1)
    gather_step(0, far - 1)
    for load in loads:
        load.wait()
    wait_partner_rows(0)

    def gather_and_compute(i):
        gather_half(1, i, False)
        gate_and_up(0, i)
        gather_half(1, i, True)
        down(0, i)

    steps(0, far - 1, gather_and_compute)
    gate_and_up(0, far - 1)
    down(0, far - 1)
    wait_pins(0)
    sum_half(0, 0, False)
    gather_step(1, far - 1)
    wait_partner_rows(1)

    def sum_and_compute(i):
        sum_half(0, i, False)
        gate_and_up(1, i - 1)
        sum_half(0, i, True)
        down(1, i - 1)

    steps(1, far, sum_and_compute)
    gate_and_up(1, far - 1)
    down(1, far - 1)
    wait_pins(1)
    sum_half(1, 0, False)
    send_back(0)

    def only_sum(i):
        sum_half(1, i, False)
        sum_half(1, i, True)

    steps(1, far, only_sum)
    send_back(1)

    def wait_back(e, none):
        @pl.when(e == me)
        def _():
            pltpu.make_async_copy(back.at[e], returned.at[e], back_recv.at[e]).wait()

        @pl.when(e != me)
        def _():
            kept = returned.at[e, pl.ds(0, cap)]
            remote(kept, kept, back_send.at[e], back_recv.at[e], (e, t)).wait_recv()

        return none

    lax.fori_loop(0, experts, wait_back, 0)
    picked = returned[...].astype(jnp.float32).reshape(experts * SLOT_ROWS, width).astype(jnp.bfloat16)
    combined = stream_ref[...].astype(jnp.float32)
    for n in reversed(range(3)):
        combined = combined + lax.dot_general(
            weight_ref[n], picked, (((0,), (0,)), ((), ())), preferred_element_type=jnp.float32
        )
    out_ref[...] = combined.astype(jnp.bfloat16)

    for n in range(1, experts):
        go(n).wait_send()
        send_home(n).wait_send()

    def drain_pair(at, none):
        for k in range(chunks):
            for p in range(2):
                to_partner(k, at, p).wait_send()
            pin(k, at).wait_send()
        return none

    lax.fori_loop(0, chips, drain_pair, 0)

    def drain_ring(i, none):
        for k in range(chunks):
            for d in range(2):
                for order in range(4):
                    p = far_first(d, order)
                    sent, summed = ring_rows(k, 0, d, i, p).wait_send, from_sum(k, d, i, p).wait_send
                    if order < 2:
                        sent()
                        summed()
                    else:
                        pl.when(i < far - 1)(sent)
                        pl.when(i > 0)(summed)
        return none

    lax.fori_loop(0, far, drain_ring, 0)


def layer_kernel(
    chips_y, cap, q_hbm, k_hbm, v_hbm, bias_hbm, gain_hbm, w_hbm, residual_hbm, norm_hbm, choice_hbm, share_hbm,
    gate_hbm, up_hbm, down_hbm, out_ref, q, k, v, bias, gain, w, residual, norm, choice, share, gate_w, up_w, down_w,
    load_sem, stream, normed, select, weight, *scratch,
):
    sources = (q_hbm, k_hbm, v_hbm, bias_hbm, gain_hbm, w_hbm, residual_hbm, norm_hbm, choice_hbm, share_hbm)
    sources += (gate_hbm.at[0], up_hbm.at[0], down_hbm.at[0])
    places = (q, k, v, bias, gain, w, residual, norm, choice, share, gate_w, up_w, down_w)
    loads = [pltpu.make_async_copy(src, dst, load_sem.at[i]) for i, (src, dst) in enumerate(zip(sources, places))]
    for load in loads[:5]:
        load.start()
    for landing in (scratch[ATTENTION_SCRATCH + 1], scratch[ATTENTION_SCRATCH + 7]):
        landing[...] = jnp.zeros_like(landing)

    def route():
        for load in loads[5:]:
            load.start()
        for load in loads[8:10]:
            load.wait()
        slots, own_rows = select.shape
        slot = lax.broadcasted_iota(jnp.int32, (slots, own_rows), 0)
        expert, place = slot // SLOT_ROWS, slot % SLOT_ROWS
        first = choice[0:1, :] == expert
        named = first | (choice[1:2, :] == expert)
        earlier = lax.broadcasted_iota(jnp.int32, (own_rows, own_rows), 0) < lax.broadcasted_iota(
            jnp.int32, (own_rows, own_rows), 1
        )
        before = jnp.dot(
            named.astype(jnp.bfloat16), earlier.astype(jnp.bfloat16), preferred_element_type=jnp.float32
        )
        chosen = named & (before.astype(jnp.int32) == place)
        select[...] = chosen.astype(jnp.bfloat16)
        rest = jnp.where(chosen, jnp.where(first, share[0:1, :], share[1:2, :]), 0.0)
        for n in range(3):
            term = rest.astype(jnp.bfloat16)
            weight[n] = term
            rest = rest - term.astype(jnp.float32)

    attention_part(
        chips_y, loads[:8], route, q, k, v, bias, gain, w, residual, norm, stream, normed, *scratch[:ATTENTION_SCRATCH]
    )
    expert_part(chips_y, cap, loads[10:], gate_w, up_w, down_w, stream, normed, select, weight, out_ref, *scratch[ATTENTION_SCRATCH:])


ATTENTION_SCRATCH = 30


def layer(
    queries, keys, values, key_bias, head_gain, out_weight, residual, norm_gain, gate_proj, up_proj, down_proj,
    expert_choice, expert_weights,
):
    rows, packed = queries.shape
    size, width, hidden = head_gain.shape[1], out_weight.shape[1], gate_proj.shape[2]
    blocks, chips, chips_y, chunks = lax.axis_size("sp"), lax.axis_size("tp") // 2, 4, 2
    chips_x, far, own = blocks // chips_y, chips // 2, residual.shape[0]
    cap = 4 * own // blocks
    block, slots = blocks // chunks * cap, blocks * SLOT_ROWS
    bf16, f32, dma = jnp.bfloat16, jnp.float32, pltpu.SemaphoreType.DMA
    arguments = (
        queries, keys, values, key_bias.T, head_gain, out_weight, residual, norm_gain.reshape(1, -1),
        expert_choice.T, expert_weights.T, gate_proj.swapaxes(1, 2), up_proj.swapaxes(1, 2), down_proj,
    )
    scratch = [pltpu.VMEM(a.shape[-2:], a.dtype) for a in arguments]
    scratch += [
        dma((len(arguments),)),
        pltpu.VMEM((own, width), bf16),
        pltpu.VMEM((own, width), bf16),
        pltpu.VMEM((slots, own), bf16),
        pltpu.VMEM((3, slots, own), bf16),
    ]
    attention_scratch = [
        pltpu.VMEM((2, rows + 16, packed), bf16),
        pltpu.VMEM((2, rows // 2, packed), bf16),
        pltpu.VMEM((blocks, rows + 16, packed), bf16),
        pltpu.VMEM((2, rows // 2, packed), bf16),
        pltpu.VMEM((2, rows, packed), bf16),
        pltpu.VMEM((2, 2, size), f32),
        pltpu.VMEM((2, packed, width), bf16),
        pltpu.VMEM((rows, packed), f32),
        pltpu.VMEM((rows, 1), f32),
        pltpu.VMEM((2, chips_y, rows, packed), f32),
        pltpu.VMEM((2, chips_y, rows, 1), f32),
        pltpu.VMEM((2, 2, chips, own, size), bf16),
        pltpu.VMEM((chips_y, chips, own, size), bf16),
        pltpu.VMEM((chips, own, width), f32),
        pltpu.VMEM((2, far, own, width), bf16),
        pltpu.VMEM((2, far, own, width), bf16),
        dma((2, 4)),
        dma((blocks,)),
        dma((2,)),
        dma((2,)),
        dma((blocks,)),
        dma((blocks,)),
        dma((1,)),
        dma((1,)),
        dma((1,)),
        dma((1,)),
        dma((2, 2)),
        dma((chips_y,)),
        dma((2, far, 4)),
        dma((2, far, 4)),
    ]
    expert_scratch = [
        pltpu.VMEM((blocks, SLOT_ROWS, width), bf16),
        pltpu.VMEM((blocks, SLOT_ROWS, width), bf16),
        pltpu.VMEM((chunks, chips, 2, block, width), bf16),
        pltpu.VMEM((chunks, chips, 2, block, width), bf16),
        pltpu.VMEM((chunks, chips, block, width), bf16),
        pltpu.VMEM((chunks, 2, far, block, width), bf16),
        pltpu.VMEM((blocks, SLOT_ROWS, width), bf16),
        pltpu.VMEM((blocks, SLOT_ROWS, width), bf16),
        pltpu.VMEM((chips // far * 2 * block, hidden), bf16),
        dma((blocks,)),
        dma((blocks,)),
        dma((chunks, 2, far, 4)),
        dma((chunks, 2, far, 4)),
        dma((chunks, chips, 2)),
        dma((chunks, chips, 2)),
        dma((chunks, chips)),
        dma((chunks, chips)),
        dma((chunks, 2, far, 4)),
        dma((chunks, 2, far, 4)),
        dma((blocks,)),
        dma((blocks,)),
    ]
    assert len(attention_scratch) == ATTENTION_SCRATCH
    return pl.pallas_call(
        functools.partial(layer_kernel, chips_y, cap),
        out_shape=jax.ShapeDtypeStruct(residual.shape, bf16),
        in_specs=[pl.BlockSpec(memory_space=pl.ANY)] * len(arguments),
        out_specs=pl.BlockSpec(memory_space=pltpu.VMEM),
        scratch_shapes=scratch + attention_scratch + expert_scratch,
        compiler_params=pltpu.CompilerParams(collective_id=1, has_side_effects=True, vmem_limit_bytes=60 << 20),
        name="layer",
    )(*arguments)


def solution(mesh):
    placed = (
        P("sp", "tp"),
        P("sp", "tp"),
        P("sp", "tp"),
        P("sp", "tp"),
        P("tp", None),
        P("tp", None),
        P(("sp", "tp"), None),
        P(),
        P("sp", None, "tp"),
        P("sp", None, "tp"),
        P("sp", "tp", None),
        P(("sp", "tp"), None),
        P(("sp", "tp"), None),
    )
    return jax.shard_map(
        layer, mesh=mesh, in_specs=placed, out_specs=P(("sp", "tp"), None), check_vma=False
    )
```

```python
import functools

import jax
import jax.numpy as jnp
from jax import lax
from jax.experimental import pallas as pl
from jax.experimental.pallas import tpu as pltpu
from jax.sharding import PartitionSpec as P

epsilon = 1e-06
CHUNK = 256
MESH = pl.DeviceIdType.MESH
SLOT_ROWS = 8


def remote(src, dst, send_sem, recv_sem, device):
    return pltpu.make_async_remote_copy(
        src_ref=src, dst_ref=dst, send_sem=send_sem, recv_sem=recv_sem, device_id=device, device_id_type=MESH
    )


def attention_part(
    chips_y, loads, route, q_ref, k_ref, v_ref, bias_ref, gain_ref, w_ref, residual_ref, norm_ref, stream_ref, normed_ref,
    kv_out, q_out, kv, q_in, q_wide, gains, weights, acc, carry, early, early_carry, att_out, att_in, part, part_out, ring_sum,
    kv_send, kv_recv, q_send, q_recv, pair_send, pair_recv, w_send, w_recv, g_send, g_recv,
    att_send, att_recv, rs_send, rs_recv,
):
    rows, packed = q_ref.shape
    size = packed // 2
    chips_x = lax.axis_size("sp") // chips_y
    chips = lax.axis_size("tp") // 2
    width = w_ref.shape[1]
    far, half = chips // 2, width // 2
    quarter = [pl.ds(n * half // 2, half // 2) for n in range(4)]
    me, t = lax.axis_index("sp"), lax.axis_index("tp")
    y, x, z, c = me // chips_x, me % chips_x, t // 2, t % 2

    def device(yy, xx, zz, cc):
        return (yy * chips_x + xx, 2 * zz + cc)

    def query_core(yy):
        return ((yy + 1) // 2) % 2

    partner = device(y, x, z, 1 - c)
    ahead = (device(y, x, (z + 1) % chips, c), device(y, x, (z + chips - 1) % chips, c))
    barrier = pltpu.get_barrier_semaphore()
    sources = lax.axis_size("sp")

    def greet(n, none):
        pl.semaphore_signal(barrier, inc=1, device_id=((me + n) % sources, t), device_id_type=MESH)
        return none

    lax.fori_loop(1, sources, greet, 0)
    others = [device((y + dy) % chips_y, x, z, 1 - c) for dy in range(chips_y)] + list(ahead)
    for other in others:
        pl.semaphore_signal(barrier, inc=1, device_id=other, device_id_type=MESH)
    for load in loads[:5]:
        load.wait()

    offsets = bias_ref[...].astype(jnp.float32)
    for h in range(2):
        lanes = slice(h * size, (h + 1) * size)
        kv_out[h, pl.ds(0, rows)] = jnp.concatenate([k_ref[:, lanes], v_ref[:, lanes]], axis=1)
        by_row = [offsets[h : h + 1, n * packed : (n + 1) * packed] for n in range(rows // packed)]
        by_row.append(jnp.zeros((16 - rows // packed, packed), jnp.float32))
        kv_out[h, pl.ds(rows, 16)] = jnp.concatenate(by_row, axis=0).astype(jnp.bfloat16)
        q_neg = q_ref[:, lanes] * jnp.bfloat16(-(size ** -0.5))
        q_out[h] = jnp.concatenate([q_neg[: rows // 2], q_neg[rows // 2 :]], axis=1)
    gains[c] = gain_ref[...]
    pl.semaphore_wait(barrier, sources - 1 + len(others))

    keeper = y // 2 == c
    asks_self = keeper & (query_core(y) == c)
    side, base = x % 2, x // 2 * 2
    other = (base + 2) % chips_x
    columns = (x, base + 1 - side, other + 1 - side, other + side)

    def to_column(h, n):
        return remote(
            kv_out.at[h], kv.at[me], kv_send.at[h, n], kv_recv.at[me], device(2 * c + h, columns[n], z, c)
        )

    for n in range(4):
        for h in range(2):
            if n > 0:
                to_column(h, n).start()
            else:
                pl.when(jnp.logical_not(2 * c + h == y))(lambda h=h: to_column(h, 0).start())

                @pl.when(2 * c + h == y)
                def _(h=h):
                    pltpu.make_async_copy(kv_out.at[h], kv.at[me], kv_recv.at[me]).start()

    for h in range(2):
        j = 2 * c + h

        @pl.when(jnp.logical_not(asks_self & (j == y)))
        def _(h=h, j=j):
            remote(q_out.at[h], q_in.at[y // 2], q_send.at[h], q_recv.at[y // 2], device(j, x, z, query_core(y))).start()

        @pl.when(asks_self & (j == y))
        def _(h=h):
            pltpu.make_async_copy(q_out.at[h], q_in.at[y // 2], q_recv.at[y // 2]).start()

    to_w = remote(w_ref, weights.at[c], w_send.at[0], w_recv.at[0], partner)
    to_g = remote(gain_ref, gains.at[c], g_send.at[0], g_recv.at[0], partner)
    to_g.start()
    route()

    def to_partner(s):
        return remote(kv.at[s], kv.at[s], pair_send.at[s], pair_recv.at[s], partner)

    def arrive(column):
        def one(yy, none):
            s = yy * chips_x + column

            @pl.when(keeper & (s == me))
            def _():
                pltpu.make_async_copy(kv_out.at[0], kv.at[s], kv_recv.at[s]).wait()

            @pl.when(keeper & (s != me))
            def _():
                remote(kv_out.at[0], kv.at[s], kv_send.at[0, 1], kv_recv.at[s], partner).wait_recv()

            pl.when(keeper)(lambda: to_partner(s).start())
            return none

        lax.fori_loop(0, chips_y, one, 0)

    def handed(column):
        def one(yy, none):
            pl.when(jnp.logical_not(keeper))(lambda: to_partner(yy * chips_x + column).wait_recv())
            return none

        lax.fori_loop(0, chips_y, one, 0)

    arrive(columns[0])
    arrive(columns[1])
    for load in loads[5:]:
        load.wait()
    to_w.start()
    weights[c] = w_ref[...]
    handed(columns[0])
    handed(columns[1])

    row = lax.broadcasted_iota(jnp.int32, (CHUNK, CHUNK), 0)
    col = lax.broadcasted_iota(jnp.int32, (CHUNK, CHUNK), 1)
    after = (row > col).astype(jnp.bfloat16)

    def pair_of_blocks(slot, older, masked, shift=0):
        def part_of(place, first, length):
            return kv[older + place, pl.ds(first, length)], kv[older + place, pl.ds(rows, 16)], first // 128, length // 128

        def chunk(sources, place):
            kv_part = jnp.concatenate([s[0] for s in sources], axis=0)
            offset = jnp.concatenate(
                [s[1][s[2] + n : s[2] + n + 1, :].astype(jnp.float32) for s in sources for n in range(s[3])], axis=1
            )
            minus = (
                lax.dot_general(
                    q_wide[slot], kv_part, (((1,), (1,)), ((), ())), preferred_element_type=jnp.float32
                )
                - offset
            )
            log_part = jnp.log(1.0 + jnp.exp(-jnp.abs(minus)))
            drop = jnp.minimum(minus, 0.0) - log_part
            own_log = drop - minus
            if masked:
                q_at = lax.broadcasted_iota(jnp.int32, (rows, CHUNK), 0) + (shift - place)
                earlier = lax.broadcasted_iota(jnp.int32, (rows, CHUNK), 1) < q_at
                drop = jnp.where(earlier, drop, 0.0)
            suffix = jnp.dot(drop.astype(jnp.bfloat16), after, preferred_element_type=jnp.float32)
            within = jnp.exp(own_log + suffix)
            if masked:
                within = jnp.where(earlier, within, 0.0)
            product = jnp.dot(within.astype(jnp.bfloat16), kv_part, preferred_element_type=jnp.float32)
            now = carry[...]
            acc[...] += jnp.exp(now) * product
            carry[...] = now + (suffix[:, :1] + drop[:, :1])

        chunk([part_of(1, 128, 256)], 512)
        chunk([part_of(0, 256, 128), part_of(1, 0, 128)], 256)
        chunk([part_of(0, 0, 256)], 0)

    def query_row(slot):
        return c if slot == 0 else 3 - c

    def begin(slot):
        from_y = query_row(slot)
        asked = asks_self & (from_y == y)

        @pl.when(asked)
        def _():
            pltpu.make_async_copy(q_out.at[0], q_in.at[slot], q_recv.at[slot]).wait()

        @pl.when(jnp.logical_not(asked))
        def _():
            remote(q_out.at[0], q_in.at[slot], q_send.at[0], q_recv.at[slot], partner).wait_recv()

        folded = q_in[slot]
        q_here = jnp.concatenate([folded[:, :size], folded[:, size:]], axis=0)
        q_wide[slot] = jnp.concatenate([q_here, jnp.zeros_like(q_here)], axis=1)

        def one(yy, masked):
            acc[...] = jnp.zeros_like(acc)
            carry[...] = jnp.zeros_like(carry)
            pair_of_blocks(slot, yy * chips_x + base, masked, side * rows)
            early[slot, yy] = acc[...]
            early_carry[slot, yy] = carry[...]

        def body(yy, none):
            one(yy, False)
            return none

        one(from_y, True)
        lax.fori_loop(0, from_y, body, 0)

    def attend(slot):
        from_y = query_row(slot)
        acc[...] = jnp.zeros_like(acc)
        carry[...] = jnp.zeros_like(carry)
        newest = from_y - (1 - base // 2)

        def body(n, none):
            now = carry[...]
            acc[...] += jnp.exp(now) * early[slot, from_y - n]
            carry[...] = now + early_carry[slot, from_y - n]

            @pl.when(n <= newest)
            def _():
                pair_of_blocks(slot, (newest - n) * chips_x + other, False)

            return none

        lax.fori_loop(0, from_y + 1, body, 0)
        mixture = acc[...][:, size:]
        scaled = mixture * lax.rsqrt(jnp.mean(mixture * mixture, axis=-1, keepdims=True) + epsilon)
        scaled = scaled * gains[y // 2, pl.ds(y % 2, 1), :]
        by_owner = scaled.reshape(chips, 2, rows // (2 * chips), size)
        for p in range(2):
            att_out[slot, p] = by_owner[:, p].astype(jnp.bfloat16)
            stays = (from_y == y) & (p == c)

            @pl.when(stays)
            def _(p=p):
                pltpu.make_async_copy(att_out.at[slot, p], att_in.at[y], att_recv.at[y]).start()

            @pl.when(jnp.logical_not(stays))
            def _(p=p):
                send_att(slot, p, from_y).start()

    def send_att(slot, p, from_y):
        return remote(
            att_out.at[slot, p], att_in.at[y], att_send.at[slot, p], att_recv.at[y], device(from_y, x, z, p)
        )

    begin(0)
    arrive(columns[2])
    arrive(columns[3])
    begin(1)
    handed(columns[2])
    handed(columns[3])
    to_g.wait_recv()
    attend(1)
    attend(0)

    for j in range(chips_y):
        stayed = (j == y) & (query_core(y) == c)

        @pl.when(stayed)
        def _(j=j):
            pltpu.make_async_copy(att_out.at[0, 0], att_in.at[j], att_recv.at[j]).wait()

        @pl.when(jnp.logical_not(stayed))
        def _(j=j):
            remote(att_out.at[0, 0], att_in.at[j], att_send.at[0, 0], att_recv.at[j], partner).wait_recv()

    to_w.wait_recv()
    heads = [att_in[j].astype(jnp.float32).reshape(rows // 2, size) for j in range(chips_y)]
    merged = jnp.concatenate(heads, axis=1).astype(jnp.bfloat16)
    farthest = (z + far) % chips
    far_heads = [att_in[j, farthest].astype(jnp.float32) for j in range(chips_y)]
    far_merged = jnp.concatenate(far_heads, axis=1).astype(jnp.bfloat16)
    rows_of_w = weights[...].reshape(2 * packed, width)
    part[farthest] = jnp.dot(far_merged, rows_of_w, preferred_element_type=jnp.float32)

    def rest_of_part():
        share = jnp.dot(merged, rows_of_w, preferred_element_type=jnp.float32)
        part[...] = share.reshape(part.shape)

    def from_sum(d, i, p):
        ref = ring_sum.at[d, i, :, quarter[p]]
        return remote(ref, ref, rs_send.at[d, i, p], rs_recv.at[d, i, p], ahead[d])

    for i in range(far):
        if i == 1:
            rest_of_part()
        for order in range(4 if i else 2):
            for d in range(2):
                p = order if d == 0 else (order + 2) % 4
                at = ((z + (far - i)) if d == 0 else (z - (far - i) + chips)) % chips
                total = part[at, :, quarter[p]]
                if i > 1 or (i == 1 and order < 2):
                    from_sum(d, i - 1, p).wait_recv()
                    total = total + ring_sum[d, i - 1, :, quarter[p]].astype(jnp.float32)
                part_out[d, i, :, quarter[p]] = total.astype(jnp.bfloat16)
                remote(
                    part_out.at[d, i, :, quarter[p]],
                    ring_sum.at[d, i, :, quarter[p]],
                    rs_send.at[d, i, p],
                    rs_recv.at[d, i, p],
                    ahead[d],
                ).start()
    for d in range(2):
        for p in range(4):
            from_sum(d, far - 1, p).wait_recv()
    projected = part[z] + ring_sum[0, far - 1].astype(jnp.float32) + ring_sum[1, far - 1].astype(jnp.float32)
    stream = (residual_ref[...].astype(jnp.float32) + projected).astype(jnp.bfloat16)
    stream_ref[...] = stream
    wide = stream.astype(jnp.float32)
    normed_ref[...] = (
        wide * lax.rsqrt(jnp.mean(wide * wide, axis=-1, keepdims=True) + epsilon) * norm_ref[...]
    ).astype(jnp.bfloat16)

    for h in range(2):
        j = 2 * c + h

        pl.when(jnp.logical_not(j == y))(lambda h=h: to_column(h, 0).wait_send())
        for n in range(1, 4):
            to_column(h, n).wait_send()

        @pl.when(jnp.logical_not(asks_self & (j == y)))
        def _(h=h):
            remote(q_out.at[h], q_in.at[0], q_send.at[h], q_recv.at[0], partner).wait_send()

    to_w.wait_send()
    to_g.wait_send()

    def drain_pair(s, none):
        pl.when(keeper)(lambda: to_partner(s).wait_send())
        return none

    lax.fori_loop(0, sources, drain_pair, 0)
    for slot in range(2):
        from_y = c if slot == 0 else 3 - c
        for p in range(2):

            @pl.when(jnp.logical_not((from_y == y) & (p == c)))
            def _(slot=slot, p=p, from_y=from_y):
                send_att(slot, p, from_y).wait_send()

    for d in range(2):
        for i in range(far):
            for order in range(4 if i else 2):
                from_sum(d, i, order if d == 0 else (order + 2) % 4).wait_send()


def expert_part(
    chips_y, cap, loads, gate_w, up_w, down_w, stream_ref, normed_ref, select_ref, weight_ref, out_ref,
    outgoing, arrived, rows, part, partner_part, ring_sum, back, returned, hidden,
    go_send, go_recv, ag_send, ag_recv, pair_send, pair_recv, pin_send, pin_recv,
    rs_send, rs_recv, back_send, back_recv,
):
    experts, _, width = outgoing.shape
    chunks, chips, _, block, _ = rows.shape
    far, half, per = chips // 2, width // 2, experts // chunks
    me, t = lax.axis_index("sp"), lax.axis_index("tp")
    z, c = t // 2, t % 2
    chips_x = experts // chips_y
    y, x = me // chips_x, me % chips_x
    moves = sorted(
        ((dy, dx) for dy in range(chips_y) for dx in range(chips_x)),
        key=lambda move: min(move[0], chips_y - move[0]) + min(move[1], chips_x - move[1]),
    )
    to_sp = [(y + dy) % chips_y * chips_x + (x + dx) % chips_x for dy, dx in moves]
    from_sp = [(y + chips_y - dy) % chips_y * chips_x + (x + chips_x - dx) % chips_x for dy, dx in moves]
    partner = (me, 2 * z + (1 - c))
    ahead = ((me, 2 * ((z + 1) % chips) + c), (me, 2 * ((z + chips - 1) % chips) + c))
    piece = (pl.ds(0, half), pl.ds(half, half))
    quarter = [pl.ds(n * half // 2, half // 2) for n in range(4)]

    chosen = jnp.dot(select_ref[...], normed_ref[...], preferred_element_type=jnp.float32)
    outgoing[...] = chosen.reshape(experts, SLOT_ROWS, width).astype(jnp.bfloat16)
    for k in range(chunks):
        for d in range(2):
            ring_sum[k, d, 0, :, piece[1 - d]] = jnp.zeros((block, half), jnp.bfloat16)

    def go(n):
        return remote(outgoing.at[to_sp[n], pl.ds(0, cap)], arrived.at[n, pl.ds(0, cap)], go_send.at[n], go_recv.at[n], (to_sp[n], t))

    own = pltpu.make_async_copy(outgoing.at[me], arrived.at[0], go_recv.at[0])
    own.start()
    for n in range(1, experts):
        go(n).start()

    def take_arrived(k):
        for n in range(k * per, (k + 1) * per):
            (go(n).wait_recv if n else own.wait)()
        row = lax.broadcasted_iota(jnp.int32, (block, per * SLOT_ROWS), 0)
        col = lax.broadcasted_iota(jnp.int32, (block, per * SLOT_ROWS), 1)
        pick = (col == row // cap * SLOT_ROWS + row % cap).astype(jnp.bfloat16)
        padded = arrived[pl.ds(k * per, per)].astype(jnp.float32).reshape(per * SLOT_ROWS, width)
        rows[k, z, c] = jnp.dot(
            pick, padded.astype(jnp.bfloat16), preferred_element_type=jnp.float32
        ).astype(jnp.bfloat16)

    def far_first(d, order):
        return order if d == 0 else (order + 2) % 4

    def to_partner(k, at, p):
        ref = rows.at[k, at, c, :, piece[p]]
        return remote(ref, ref, pair_send.at[k, at, p], pair_recv.at[k, at, p], partner)

    def ring_rows(k, at, d, i, p):
        ref = rows.at[k, at, c, :, quarter[p]]
        return remote(ref, ref, ag_send.at[k, d, i, p], ag_recv.at[k, d, i, p], ahead[d])

    def start_own(k):
        for order in range(4):
            for d in range(2):
                ring_rows(k, z, d, 0, far_first(d, order)).start()
        for p in range(2):
            to_partner(k, z, p).start()

    def gather_half(k, i, second):
        for order in (2, 3) if second else (0, 1):
            for d in range(2):
                p = far_first(d, order)
                at = lax.rem((z - i - 1 if d == 0 else z + i + 1) + chips, chips)
                ring_rows(k, at, d, i, p).wait_recv()

                @pl.when(i + 1 < (far - 1 if second else far))
                def _(at=at, d=d, p=p):
                    ring_rows(k, at, d, i + 1, p).start()

                if order % 2 == 1:
                    to_partner(k, at, p // 2).start()

    def gather_step(k, i):
        gather_half(k, i, False)
        pl.when(i < far - 1)(lambda: gather_half(k, i, True))

    def wait_partner_rows(k):
        def wait_one(at, none):
            for p in range(2):
                ref = rows.at[k, at, 1 - c, :, piece[p]]
                remote(ref, ref, pair_send.at[k, at, p], pair_recv.at[k, at, p], partner).wait_recv()
            return none

        lax.fori_loop(0, chips, wait_one, 0)

    group = chips // far

    def gate_and_up(k, i):
        x = rows[k, pl.ds(i * group, group)].reshape(group * 2 * block, width)
        across = (((1,), (1,)), ((), ()))
        gate = lax.dot_general(x, gate_w[...], across, preferred_element_type=jnp.float32)
        up = lax.dot_general(x, up_w[...], across, preferred_element_type=jnp.float32)
        hidden[...] = (gate / (1.0 + jnp.exp(-gate)) * up).astype(jnp.bfloat16)

    def down(k, i):
        at = pl.ds(i * group, group)
        product = jnp.dot(hidden[...], down_w[...], preferred_element_type=jnp.float32)
        part[k, at] = product.astype(jnp.bfloat16).reshape(group, 2, block, width)
        for j in range(group):
            pin(k, i * group + j).start()

    def pin(k, at):
        return remote(
            part.at[k, at, 1 - c], partner_part.at[k, at], pin_send.at[k, at], pin_recv.at[k, at], partner
        )

    def wait_pins(k):
        def wait_one(at, none):
            pin(k, at).wait_recv()
            return none

        lax.fori_loop(0, chips, wait_one, 0)

    def from_sum(k, d, i, p):
        ref = ring_sum.at[k, d, i, :, quarter[p]]
        return remote(ref, ref, rs_send.at[k, d, i, p], rs_recv.at[k, d, i, p], ahead[d])

    def sum_half(k, i, second):
        for order in (2, 3) if second else (0, 1):
            for d in range(2):
                p = far_first(d, order)
                at = lax.rem((z + (far - i) if d == 0 else z - (far - i)) + chips, chips)
                total = part[k, at, c, :, quarter[p]].astype(jnp.float32) + partner_part[
                    k, at, :, quarter[p]
                ].astype(jnp.float32)
                if isinstance(i, int):
                    assert i == 0
                else:
                    wait = from_sum(k, d, i - 1, p).wait_recv
                    if second:
                        pl.when(i > 1)(wait)
                    else:
                        wait()
                    total = total + ring_sum[k, d, i - 1, :, quarter[p]].astype(jnp.float32)
                part[k, at, c, :, quarter[p]] = total.astype(jnp.bfloat16)
                remote(
                    part.at[k, at, c, :, quarter[p]],
                    ring_sum.at[k, d, i, :, quarter[p]],
                    rs_send.at[k, d, i, p],
                    rs_recv.at[k, d, i, p],
                    ahead[d],
                ).start()

    def send_back(k):
        for p in range(4):
            for d in range(2):
                from_sum(k, d, far - 1, p).wait_recv()
        total = (
            part[k, z, c].astype(jnp.float32)
            + partner_part[k, z].astype(jnp.float32)
            + ring_sum[k, 0, far - 1].astype(jnp.float32)
            + ring_sum[k, 1, far - 1].astype(jnp.float32)
        ).astype(jnp.bfloat16)
        row = lax.broadcasted_iota(jnp.int32, (per * SLOT_ROWS, block), 0)
        col = lax.broadcasted_iota(jnp.int32, (per * SLOT_ROWS, block), 1)
        spread = ((row % SLOT_ROWS < cap) & (col == row // SLOT_ROWS * cap + row % SLOT_ROWS)).astype(jnp.bfloat16)
        back[pl.ds(k * per, per)] = (
            jnp.dot(spread, total, preferred_element_type=jnp.float32)
            .reshape(per, SLOT_ROWS, width)
            .astype(jnp.bfloat16)
        )

        for n in range(k * per, (k + 1) * per):
            if n:
                send_home(n).start()
            else:
                pltpu.make_async_copy(back.at[0], returned.at[me], back_recv.at[me]).start()

    def send_home(n):
        return remote(
            back.at[n, pl.ds(0, cap)], returned.at[me, pl.ds(0, cap)], back_send.at[n], back_recv.at[me], (from_sp[n], t)
        )

    def steps(first, last, body):
        def one(i, none):
            body(i)
            return none

        lax.fori_loop(first, last, one, 0)

    take_arrived(0)
    start_own(0)
    gather_step(0, 0)
    take_arrived(1)
    steps(1, far - 1, lambda i: gather_step(0, i))
    start_own(1)
    gather_step(0, far - 1)
    for load in loads:
        load.wait()
    wait_partner_rows(0)

    def gather_and_compute(i):
        gather_half(1, i, False)
        gate_and_up(0, i)
        gather_half(1, i, True)
        down(0, i)

    steps(0, far - 1, gather_and_compute)
    gate_and_up(0, far - 1)
    down(0, far - 1)
    wait_pins(0)
    sum_half(0, 0, False)
    gather_step(1, far - 1)
    wait_partner_rows(1)

    def sum_and_compute(i):
        sum_half(0, i, False)
        gate_and_up(1, i - 1)
        sum_half(0, i, True)
        down(1, i - 1)

    steps(1, far, sum_and_compute)
    gate_and_up(1, far - 1)
    down(1, far - 1)
    wait_pins(1)
    sum_half(1, 0, False)
    send_back(0)

    def only_sum(i):
        sum_half(1, i, False)
        sum_half(1, i, True)

    steps(1, far, only_sum)
    send_back(1)

    def wait_back(e, none):
        @pl.when(e == me)
        def _():
            pltpu.make_async_copy(back.at[e], returned.at[e], back_recv.at[e]).wait()

        @pl.when(e != me)
        def _():
            kept = returned.at[e, pl.ds(0, cap)]
            remote(kept, kept, back_send.at[e], back_recv.at[e], (e, t)).wait_recv()

        return none

    lax.fori_loop(0, experts, wait_back, 0)
    picked = returned[...].astype(jnp.float32).reshape(experts * SLOT_ROWS, width).astype(jnp.bfloat16)
    combined = stream_ref[...].astype(jnp.float32)
    for n in reversed(range(3)):
        combined = combined + lax.dot_general(
            weight_ref[n], picked, (((0,), (0,)), ((), ())), preferred_element_type=jnp.float32
        )
    out_ref[...] = combined.astype(jnp.bfloat16)

    for n in range(1, experts):
        go(n).wait_send()
        send_home(n).wait_send()

    def drain_pair(at, none):
        for k in range(chunks):
            for p in range(2):
                to_partner(k, at, p).wait_send()
            pin(k, at).wait_send()
        return none

    lax.fori_loop(0, chips, drain_pair, 0)

    def drain_ring(i, none):
        for k in range(chunks):
            for d in range(2):
                for order in range(4):
                    p = far_first(d, order)
                    sent, summed = ring_rows(k, 0, d, i, p).wait_send, from_sum(k, d, i, p).wait_send
                    if order < 2:
                        sent()
                        summed()
                    else:
                        pl.when(i < far - 1)(sent)
                        pl.when(i > 0)(summed)
        return none

    lax.fori_loop(0, far, drain_ring, 0)


def layer_kernel(
    chips_y, cap, q_hbm, k_hbm, v_hbm, bias_hbm, gain_hbm, w_hbm, residual_hbm, norm_hbm, choice_hbm, share_hbm,
    gate_hbm, up_hbm, down_hbm, out_ref, q, k, v, bias, gain, w, residual, norm, choice, share, gate_w, up_w, down_w,
    load_sem, stream, normed, select, weight, *scratch,
):
    sources = (q_hbm, k_hbm, v_hbm, bias_hbm, gain_hbm, w_hbm, residual_hbm, norm_hbm, choice_hbm, share_hbm)
    sources += (gate_hbm.at[0], up_hbm.at[0], down_hbm.at[0])
    places = (q, k, v, bias, gain, w, residual, norm, choice, share, gate_w, up_w, down_w)
    loads = [pltpu.make_async_copy(src, dst, load_sem.at[i]) for i, (src, dst) in enumerate(zip(sources, places))]
    for load in loads[:5]:
        load.start()
    for landing in (scratch[ATTENTION_SCRATCH + 1], scratch[ATTENTION_SCRATCH + 7]):
        landing[...] = jnp.zeros_like(landing)

    def route():
        for load in loads[5:]:
            load.start()
        for load in loads[8:10]:
            load.wait()
        slots, own_rows = select.shape
        slot = lax.broadcasted_iota(jnp.int32, (slots, own_rows), 0)
        expert, place = slot // SLOT_ROWS, slot % SLOT_ROWS
        first = choice[0:1, :] == expert
        named = first | (choice[1:2, :] == expert)
        earlier = lax.broadcasted_iota(jnp.int32, (own_rows, own_rows), 0) < lax.broadcasted_iota(
            jnp.int32, (own_rows, own_rows), 1
        )
        before = jnp.dot(
            named.astype(jnp.bfloat16), earlier.astype(jnp.bfloat16), preferred_element_type=jnp.float32
        )
        chosen = named & (before.astype(jnp.int32) == place)
        select[...] = chosen.astype(jnp.bfloat16)
        rest = jnp.where(chosen, jnp.where(first, share[0:1, :], share[1:2, :]), 0.0)
        for n in range(3):
            term = rest.astype(jnp.bfloat16)
            weight[n] = term
            rest = rest - term.astype(jnp.float32)

    attention_part(
        chips_y, loads[:8], route, q, k, v, bias, gain, w, residual, norm, stream, normed, *scratch[:ATTENTION_SCRATCH]
    )
    expert_part(chips_y, cap, loads[10:], gate_w, up_w, down_w, stream, normed, select, weight, out_ref, *scratch[ATTENTION_SCRATCH:])


ATTENTION_SCRATCH = 30


def layer(
    queries, keys, values, key_bias, head_gain, out_weight, residual, norm_gain, gate_proj, up_proj, down_proj,
    expert_choice, expert_weights,
):
    rows, packed = queries.shape
    size, width, hidden = head_gain.shape[1], out_weight.shape[1], gate_proj.shape[2]
    blocks, chips, chips_y, chunks = lax.axis_size("sp"), lax.axis_size("tp") // 2, 4, 2
    chips_x, far, own = blocks // chips_y, chips // 2, residual.shape[0]
    cap = 4 * own // blocks
    block, slots = blocks // chunks * cap, blocks * SLOT_ROWS
    bf16, f32, dma = jnp.bfloat16, jnp.float32, pltpu.SemaphoreType.DMA
    arguments = (
        queries, keys, values, key_bias.T, head_gain, out_weight, residual, norm_gain.reshape(1, -1),
        expert_choice.T, expert_weights.T, gate_proj.swapaxes(1, 2), up_proj.swapaxes(1, 2), down_proj,
    )
    scratch = [pltpu.VMEM(a.shape[-2:], a.dtype) for a in arguments]
    scratch += [
        dma((len(arguments),)),
        pltpu.VMEM((own, width), bf16),
        pltpu.VMEM((own, width), bf16),
        pltpu.VMEM((slots, own), bf16),
        pltpu.VMEM((3, slots, own), bf16),
    ]
    attention_scratch = [
        pltpu.VMEM((2, rows + 16, packed), bf16),
        pltpu.VMEM((2, rows // 2, packed), bf16),
        pltpu.VMEM((blocks, rows + 16, packed), bf16),
        pltpu.VMEM((2, rows // 2, packed), bf16),
        pltpu.VMEM((2, rows, packed), bf16),
        pltpu.VMEM((2, 2, size), f32),
        pltpu.VMEM((2, packed, width), bf16),
        pltpu.VMEM((rows, packed), f32),
        pltpu.VMEM((rows, 1), f32),
        pltpu.VMEM((2, chips_y, rows, packed), f32),
        pltpu.VMEM((2, chips_y, rows, 1), f32),
        pltpu.VMEM((2, 2, chips, own, size), bf16),
        pltpu.VMEM((chips_y, chips, own, size), bf16),
        pltpu.VMEM((chips, own, width), f32),
        pltpu.VMEM((2, far, own, width), bf16),
        pltpu.VMEM((2, far, own, width), bf16),
        dma((2, 4)),
        dma((blocks,)),
        dma((2,)),
        dma((2,)),
        dma((blocks,)),
        dma((blocks,)),
        dma((1,)),
        dma((1,)),
        dma((1,)),
        dma((1,)),
        dma((2, 2)),
        dma((chips_y,)),
        dma((2, far, 4)),
        dma((2, far, 4)),
    ]
    expert_scratch = [
        pltpu.VMEM((blocks, SLOT_ROWS, width), bf16),
        pltpu.VMEM((blocks, SLOT_ROWS, width), bf16),
        pltpu.VMEM((chunks, chips, 2, block, width), bf16),
        pltpu.VMEM((chunks, chips, 2, block, width), bf16),
        pltpu.VMEM((chunks, chips, block, width), bf16),
        pltpu.VMEM((chunks, 2, far, block, width), bf16),
        pltpu.VMEM((blocks, SLOT_ROWS, width), bf16),
        pltpu.VMEM((blocks, SLOT_ROWS, width), bf16),
        pltpu.VMEM((chips // far * 2 * block, hidden), bf16),
        dma((blocks,)),
        dma((blocks,)),
        dma((chunks, 2, far, 4)),
        dma((chunks, 2, far, 4)),
        dma((chunks, chips, 2)),
        dma((chunks, chips, 2)),
        dma((chunks, chips)),
        dma((chunks, chips)),
        dma((chunks, 2, far, 4)),
        dma((chunks, 2, far, 4)),
        dma((blocks,)),
        dma((blocks,)),
    ]
    assert len(attention_scratch) == ATTENTION_SCRATCH
    return pl.pallas_call(
        functools.partial(layer_kernel, chips_y, cap),
        out_shape=jax.ShapeDtypeStruct(residual.shape, bf16),
        in_specs=[pl.BlockSpec(memory_space=pl.ANY)] * len(arguments),
        out_specs=pl.BlockSpec(memory_space=pltpu.VMEM),
        scratch_shapes=scratch + attention_scratch + expert_scratch,
        compiler_params=pltpu.CompilerParams(collective_id=1, has_side_effects=True, vmem_limit_bytes=60 << 20),
        name="layer",
    )(*arguments)


def solution(mesh):
    placed = (
        P("sp", "tp"),
        P("sp", "tp"),
        P("sp", "tp"),
        P("sp", "tp"),
        P("tp", None),
        P("tp", None),
        P(("sp", "tp"), None),
        P(),
        P("sp", None, "tp"),
        P("sp", None, "tp"),
        P("sp", "tp", None),
        P(("sp", "tp"), None),
        P(("sp", "tp"), None),
    )
    return jax.shard_map(
        layer, mesh=mesh, in_specs=placed, out_specs=P(("sp", "tp"), None), check_vma=False
    )
```
